512 devices in a mesh: sp: 16 (over z), fs: 4 (over y), tp: 8 (over x, core).
Axes of the slice: x: 4, y: 4, z: 16, core: 2. Of those that a mesh axis runs over, the one named last changes fastest.
Arguments:
- inputs: bfloat16 [4, 4096, 4096], P('fs', 'sp', 'tp'), may hold values from -6 to 6
- norm_gain: float32 [4096], replicated, may hold values from 0.1 to 1.9
- conv_in_a: bfloat16 [4096, 1024], P(('sp', 'fs'), 'tp'), may hold values from -0.09375 to 0.09375
- conv_in_b: bfloat16 [4096, 1024], P(('sp', 'fs'), 'tp'), may hold values from -0.09375 to 0.09375
- query_w: bfloat16 [4096, 512], P(('sp', 'fs'), 'tp'), may hold values from -0.09375 to 0.09375
- key_w: bfloat16 [4096, 512], P(('sp', 'fs'), 'tp'), may hold values from -0.09375 to 0.09375
- value_w: bfloat16 [4096, 1024], P(('sp', 'fs'), 'tp'), may hold values from -0.09375 to 0.09375
- out_gate_w: bfloat16 [4096, 1024], P(('sp', 'fs'), 'tp'), may hold values from -0.09375 to 0.09375
- pointwise_w: bfloat16 [4096, 1024], P(('sp', 'fs'), 'tp'), may hold values from -0.1875 to 0.1875
- gla_out_w: bfloat16 [4096, 1024], P(('sp', 'fs'), 'tp'), may hold values from -0.1875 to 0.1875
- forget_first_factor: bfloat16 [4096, 64], replicated, may hold values from -0.09375 to 0.09375
- decay_w: bfloat16 [64, 512], replicated, may hold values from -0.75 to 0.75
- decay_bias: float32 [512], replicated, as said below
- decay_extra: float32 [4, 4096, 512], P('fs', 'sp', 'tp'), may hold values from -2.2 to 0, as said below
- conv_kernel: float32 [31, 1024], replicated, may hold values from -7 to 7
- conv_gain: float32 [1024], replicated, may hold values from 0.1 to 1.9
- head_gain: float32 [64], replicated, may hold values from 0.1 to 1.9
Outputs:
- mixed: bfloat16 [4, 4096, 4096], P('fs', 'sp', 'tp')
The draws below stay inside these ranges and needn't reach their ends.
Inputs may be any that keep to these rules, and one draw needn't show every extreme that they name: decay_bias is positive. decay_extra is never positive.
All inputs are finite; a program needn't handle non-finite values.
Results may differ from the reference program's by a relative error of at most 0.015.
Values may be sent and summed in bfloat16 or wider, within the bound.
A program may use at most 128 MiB of HBM per device.

```python
import math
import jax
import jax.numpy as jnp
from jax import lax

D = 4096
C = 1024
GLA_HEADS = 16
DK = 32
DV = 64
RANK = 64
CONV_WIDTH = 31
BLOCK = 64
TOK_DEV = 256
SEQS = 4
LENGTH = 4096
HK = 512
HV = 1024
N_TP = 8


def draw_decay_bias(key, part):
    first_key = jax.random.fold_in(key, 11)
    second_key = jax.random.fold_in(key, 12)
    third_key = jax.random.fold_in(key, 13)
    slow_share = 0.5
    slow_heads = jax.random.bernoulli(first_key, slow_share, (GLA_HEADS,))
    slow_channels = jnp.repeat(slow_heads, DK)
    slow_value = math.log(LENGTH / 16.0) + jax.random.uniform(second_key, (HK,), jnp.float32, 1.0, 1.5)
    fast_value = jax.random.uniform(third_key, (HK,), jnp.float32, 0.5, 1.7)
    return jnp.where(slow_channels, slow_value, fast_value).astype(jnp.float32)


def draw_decay_extra(key, part):
    rate_key = jax.random.fold_in(key, 21)
    spot_key = jax.random.fold_in(key, 22)
    depth_key = jax.random.fold_in(key, 23)
    segment_count = LENGTH // TOK_DEV
    log_rate = jax.random.uniform(rate_key, (SEQS, segment_count, 1, HK), jnp.float32, math.log(0.15), math.log(0.6))
    forget_factors = jnp.broadcast_to(jnp.exp(log_rate) / LENGTH, (SEQS, segment_count, TOK_DEV, HK)).reshape(SEQS, LENGTH, HK)
    spots = jax.random.randint(spot_key, (SEQS, 3), 0, LENGTH)
    tier_heights = jax.random.uniform(depth_key, (SEQS, 3, HK), jnp.float32, math.log(0.5), math.log(0.8))
    agreement_tally = (jnp.arange(LENGTH, dtype=jnp.int32)[None, :, None] == spots[:, None, :]).astype(jnp.float32)
    spurt_sizes_list = jnp.einsum('dqz,dzc->dqc', agreement_tally, tier_heights)
    return (spurt_sizes_list - forget_factors).astype(jnp.float32)


def draw_conv_kernel(key, part):
    base_key = jax.random.fold_in(key, 31)
    base = jax.random.truncated_normal(base_key, -4.0, 4.0, (CONV_WIDTH, C), jnp.float32) * CONV_WIDTH ** (-0.5)
    rising = 3.0 ** (jnp.arange(C, dtype=jnp.float32) / (C - 1))
    return (base * rising).astype(jnp.float32)


def shard_levels(own_key, dims, shards, low, largest):
    level, own = 1.0, jax.random.fold_in(own_key, 6)
    for axis_at, parts in shards:
        heights = jnp.exp(jax.random.uniform(jax.random.fold_in(own, axis_at), (parts,), jnp.float32, low / len(shards), largest / len(shards)))
        level = level * jnp.repeat(heights, dims[axis_at] // parts).reshape([-1 if axis == axis_at else 1 for axis in range(len(dims))])
    return level


def normal_values(rng, extent, scale, limit, split=(), held_as=jnp.bfloat16):
    result = scale * jax.random.normal(rng, extent, jnp.float32)
    if split:
        result = result * shard_levels(rng, extent, split, -0.22, 0.18)
    return jnp.clip(result, -limit, limit).astype(held_as)


def setup_inputs(seed: int = 0) -> dict:
    key_of = jax.random.split(jax.random.key(seed), 18)
    inputs = normal_values(key_of[0], (SEQS, LENGTH, D), 1.0, 6.0, ((0, 4), (1, 16), (2, 8)))
    norm_gain = jnp.clip(1.0 + 0.18 * jax.random.normal(key_of[1], (D,), jnp.float32), 0.1, 1.9)
    conv_in_a = normal_values(key_of[2], (D, C), D ** -0.5, 0.09375, ((0, 64), (1, 8)))
    conv_in_b = normal_values(key_of[3], (D, C), D ** -0.5, 0.09375, ((0, 64), (1, 8)))
    query_w = normal_values(key_of[4], (D, HK), D ** -0.5, 0.09375, ((0, 64), (1, 8)))
    key_w = normal_values(key_of[5], (D, HK), D ** -0.5, 0.09375, ((0, 64), (1, 8)))
    value_w = normal_values(key_of[6], (D, HV), D ** -0.5, 0.09375, ((0, 64), (1, 8)))
    out_gate_w = normal_values(key_of[7], (D, HV), D ** -0.5, 0.09375, ((0, 64), (1, 8)))
    pointwise_w = normal_values(key_of[8], (D, C), C ** -0.5, 0.1875, ((0, 64), (1, 8)))
    gla_out_w = normal_values(key_of[9], (D, HV), HV ** -0.5, 0.1875, ((0, 64), (1, 8)))
    forget_first_factor = normal_values(key_of[10], (D, RANK), D ** -0.5, 0.09375)
    decay_w = normal_values(key_of[11], (RANK, HK), RANK ** -0.5, 0.75)
    decay_bias = draw_decay_bias(jax.random.fold_in(key_of[17], 71), 0)
    decay_extra = draw_decay_extra(jax.random.fold_in(key_of[17], 71), 0)
    conv_kernel = draw_conv_kernel(jax.random.fold_in(key_of[17], 71), 0)
    conv_gain = jnp.clip(1.0 + 0.18 * jax.random.normal(key_of[15], (C,), jnp.float32), 0.1, 1.9)
    head_gain = jnp.clip(1.0 + 0.18 * jax.random.normal(key_of[16], (DV,), jnp.float32), 0.1, 1.9)
    return dict(inputs=inputs, norm_gain=norm_gain, conv_in_a=conv_in_a, conv_in_b=conv_in_b, query_w=query_w, key_w=key_w, value_w=value_w, out_gate_w=out_gate_w, pointwise_w=pointwise_w, gla_out_w=gla_out_w, forget_first_factor=forget_first_factor, decay_w=decay_w, decay_bias=decay_bias, decay_extra=decay_extra, conv_kernel=conv_kernel, conv_gain=conv_gain, head_gain=head_gain)


def reference(inputs, norm_gain, conv_in_a, conv_in_b, query_w, key_w, value_w, out_gate_w, pointwise_w, gla_out_w, forget_first_factor, decay_w, decay_bias, decay_extra, conv_kernel, conv_gain, head_gain):
    position_count = SEQS * LENGTH
    flat_rows = inputs.reshape(position_count, D).astype(jnp.float32)
    row_scale = lax.rsqrt(lax.optimization_barrier(jnp.mean(flat_rows * flat_rows, axis=1, keepdims=True)) + 1e-06)
    scaled = (flat_rows * norm_gain).astype(jnp.bfloat16)

    def project(weight):
        product = jnp.dot(scaled, weight, preferred_element_type=jnp.float32)
        return (product * row_scale).astype(jnp.bfloat16)
    conv_a, conv_b, queries, keys, values, out_gate, low_rank = [project(weight) for weight in (conv_in_a, conv_in_b, query_w, key_w, value_w, out_gate_w, forget_first_factor)]
    gated = (conv_a.astype(jnp.float32) * jax.nn.sigmoid(conv_b.astype(jnp.float32))).astype(jnp.bfloat16)
    padded = jnp.pad(gated.reshape(SEQS, LENGTH, C).astype(jnp.float32), ((0, 0), (CONV_WIDTH - 1, 0), (0, 0)))
    convolved = jnp.zeros((SEQS, LENGTH, C), jnp.float32)
    for offset in range(CONV_WIDTH):
        convolved = convolved + conv_kernel[offset] * padded[:, offset:offset + LENGTH]
    average = lax.optimization_barrier(jnp.mean(convolved, axis=-1, keepdims=True))
    spread_squared_mean = lax.optimization_barrier(jnp.mean(jnp.square(convolved - average), axis=-1, keepdims=True))
    normed = (convolved - average) * lax.rsqrt(spread_squared_mean + 1e-05) * conv_gain
    conv_act = jax.nn.silu(normed).astype(jnp.bfloat16).reshape(position_count, C)
    pre_decay = jnp.dot(low_rank, decay_w, preferred_element_type=jnp.float32) + decay_bias
    log_decay = jax.nn.log_sigmoid(pre_decay) / 16.0 + decay_extra.reshape(position_count, HK)
    block_count = LENGTH // BLOCK

    def split_blocks(array_operand, width):
        return array_operand.reshape(SEQS, block_count, BLOCK, GLA_HEADS, width).transpose(1, 0, 3, 2, 4)
    q_blocks = split_blocks(queries.astype(jnp.float32), DK) * DK ** (-0.5)
    k_blocks = split_blocks(keys.astype(jnp.float32), DK)
    v_blocks = split_blocks(values.astype(jnp.float32), DV)
    cumulative_all = jnp.cumsum(split_blocks(log_decay, DK), axis=3)
    causal = jnp.tril(jnp.ones((BLOCK, BLOCK), dtype=bool))
    highest = lax.Precision.HIGHEST

    def advance(state, block_inputs):
        query_block, key_block, value_block, prefix_running_sum = block_inputs
        spread = prefix_running_sum[..., :, None, :] - prefix_running_sum[..., None, :, :]
        weights_in = jnp.exp(jnp.where(causal[:, :, None], spread, -jnp.inf))
        scores = jnp.einsum('shid,shjd,shijd->shij', query_block, key_block, weights_in, precision=highest)
        inner = jnp.einsum('shij,shjv->shiv', scores, value_block, precision=highest)
        outer = jnp.einsum('shid,shdv->shiv', query_block * jnp.exp(prefix_running_sum), state, precision=highest)
        last_total = prefix_running_sum[..., -1, :]
        added_share_term = jnp.einsum('shjd,shjv->shdv', key_block * jnp.exp(last_total[..., None, :] - prefix_running_sum), value_block, precision=highest)
        return (jnp.exp(last_total)[..., None] * state + added_share_term, inner + outer)
    start_state = jnp.zeros((SEQS, GLA_HEADS, DK, DV), jnp.float32)
    _, outputs = lax.scan(advance, start_state, (q_blocks, k_blocks, v_blocks, cumulative_all))
    outputs = outputs.transpose(1, 0, 3, 2, 4).reshape(position_count, GLA_HEADS, DV)
    normed_heads = outputs * lax.rsqrt(lax.optimization_barrier(jnp.mean(outputs * outputs, axis=-1, keepdims=True)) + 1e-06) * head_gain
    gla_act = (normed_heads.reshape(position_count, HV) * jax.nn.silu(out_gate.astype(jnp.float32))).astype(jnp.bfloat16)
    conv_group = C // N_TP
    head_group = HV // N_TP
    total = flat_rows
    for group_index in range(N_TP):
        convolution_window = slice(group_index * conv_group, (group_index + 1) * conv_group)
        head_slice = slice(group_index * head_group, (group_index + 1) * head_group)
        value_fraction = jnp.dot(conv_act[:, convolution_window], pointwise_w[:, convolution_window].T, preferred_element_type=jnp.float32)
        value_fraction = value_fraction + jnp.dot(gla_act[:, head_slice], gla_out_w[:, head_slice].T, preferred_element_type=jnp.float32)
        total = total + lax.optimization_barrier(value_fraction.astype(jnp.bfloat16)).astype(jnp.float32)
    return total.astype(jnp.bfloat16).reshape(SEQS, LENGTH, D)
```

```python
import functools

import jax
import jax.numpy as jnp
from jax import lax
from jax.experimental import pallas as pl
from jax.experimental.pallas import tpu as pltpu
from jax.sharding import PartitionSpec as P

MESH = pl.DeviceIdType.MESH
F32 = jnp.float32
BF16 = jnp.bfloat16
HIGHEST = lax.Precision.HIGHEST
NZ = 16
TOK = 256
NT = (((1,), (1,)), ((), ()))
TN = (((0,), (0,)), ((), ()))


def remote(src, dst, send, recv, device):
    return pltpu.make_async_remote_copy(
        src_ref=src,
        dst_ref=dst,
        send_sem=send,
        recv_sem=recv,
        device_id=device,
        device_id_type=MESH,
    )


def wrap(value, size):
    return lax.rem(value + size, size)


def rows(start, size):
    return pl.ds(pl.multiple_of(start, size), size)


def iota(shape, dim):
    return lax.broadcasted_iota(jnp.int32, shape, dim)


def sigmoid(value):
    return 1.0 / (1.0 + jnp.exp(-value))


def roll64(value):
    return pltpu.roll(value, 64, 1)


def body(
    xin,
    wsrc,
    owsrc,
    exsrc,
    dwt,
    bias,
    taps,
    cgain,
    hgain,
    out,
    xg,
    w,
    ow,
    acc_own,
    acc_send,
    acc_recv,
    mats,
    xors,
    scores,
    ext,
    exb,
    stats,
    tot_me,
    tots,
    st_me,
    sts,
    act_me,
    acts,
    po_send,
    po_recv,
    x_send1,
    x_send2,
    x_recv,
    wy_send,
    wy_recv,
    wz_send,
    wz_recv,
    ox_send,
    ox_recv,
    oz_send,
    oz_recv,
    oy_send,
    oy_recv,
    ex_send,
    ex_recv,
    d2d_send,
    d2d_recv,
    halo_send,
    halo_recv,
    stat_send,
    stat_recv,
    tot_send,
    tot_recv,
    st_send,
    st_recv,
    act_send,
    act_recv,
):
    z = lax.axis_index("sp")
    y = lax.axis_index("fs")
    t = lax.axis_index("tp")
    x = lax.div(t, 2)
    c = t - 2 * x
    y_half = lax.div(y, 2)
    y_low = y - 2 * y_half
    z_class = lax.rem(lax.div(z, 2), 2)
    partner = (z, y, 2 * x + 1 - c)

    def at(xx, yy, zz, cc):
        return (zz, yy, 2 * xx + cc)

    barrier = pltpu.get_barrier_semaphore()

    def greet_plane(k, carry):
        flat = lax.rem(y * 8 + t + k, 32)
        yy = lax.div(flat, 8)
        pl.semaphore_signal(
            barrier, inc=1, device_id=(z, yy, flat - 8 * yy), device_id_type=MESH
        )
        return carry

    lax.fori_loop(1, 32, greet_plane, 0)

    def greet_line(k, carry):
        pl.semaphore_signal(
            barrier, inc=1, device_id=(lax.rem(z + k, NZ), y, t), device_id_type=MESH
        )
        return carry

    lax.fori_loop(1, NZ, greet_line, 0)

    own_rows = y * TOK
    own_cols = pl.ds(pl.multiple_of(x * 512, 512), 512)
    xg[rows(own_rows, TOK), own_cols] = xin[...]
    pl.semaphore_wait(barrier, 31 + NZ - 1)

    finish = []

    def start(copy, cond=None):
        if cond is None:
            copy.start()
        else:
            pl.when(cond)(copy.start)
        finish.append((copy, cond))

    def w_at(zz, yy):
        at_row = lax.div(zz, 4) * 512 + lax.rem(zz, 2) * 256 + yy * 64
        return w.at[rows(at_row, 64), :]

    for j in range(2):
        mine = jnp.logical_and(2 * c + j == y, z_class == c)
        start(
            remote(
                wsrc.at[j],
                w_at(z, y),
                wy_send.at[j],
                wy_recv.at[y],
                at(x, 2 * c + j, z, z_class),
            ),
            jnp.logical_not(mine),
        )

        @pl.when(mine)
        def _():
            w_row = lax.div(z, 4) * 512 + lax.rem(z, 2) * 256 + y * 64
            w[rows(w_row, 64), :] = wsrc[j]

    x_up, x_down = wrap(x + 1, 4), wrap(x - 1, 4)
    y_up, y_down = wrap(y + 1, 4), wrap(y - 1, 4)
    z_up, z_down = wrap(z + 1, NZ), wrap(z - 1, NZ)
    streams = (
        (at(x_up, y, z, c), at(x, y_up, z, c), 1, True),
        (at(x_down, y, z, c), at(x, y_down, z, c), -1, True),
        (at(x, y_up, z, c), at(x_up, y, z, c), 1, False),
        (at(x, y_down, z, c), at(x_down, y, z, c), -1, False),
    )

    def x_hop(hop):
        for q, (first, second, sign, x_first) in enumerate(streams):
            for i in range(4):
                j = hop - i
                if j < 0 or j > 3:
                    continue
                dx, dy = (i, j) if x_first else (j, i)
                xx, yy = wrap(x - sign * dx, 4), wrap(y - sign * dy, 4)
                place = xg.at[
                    rows(yy * TOK + 64 * q, 64),
                    pl.ds(pl.multiple_of(xx * 512, 512), 512),
                ]
                source = xin.at[pl.ds(64 * q, 64), :] if hop == 0 else place
                if hop:
                    remote(
                        place, place, x_send2.at[q, 4 * i], x_recv.at[q, 4 * i + j], first
                    ).wait_recv()
                if j == 0 and i < 3:
                    start(
                        remote(
                            source, place, x_send1.at[q, i], x_recv.at[q, 4 * i + 4], first
                        )
                    )
                if j < 3:
                    start(
                        remote(
                            source,
                            place,
                            x_send2.at[q, 4 * i + j],
                            x_recv.at[q, 4 * i + j + 1],
                            second,
                        )
                    )

    x_hop(0)

    def ow_at(zz, xx):
        at_row = (4 * lax.rem(zz, 4) + y) * 64
        return ow.at[rows(at_row, 64), pl.ds(pl.multiple_of(xx * 256, 256), 256)]

    z_quarter = lax.div(z, 4)
    start(
        remote(owsrc, ow_at(z, x), ox_send, ox_recv.at[x], at(z_quarter, y, z, c)),
        x != z_quarter,
    )

    @pl.when(x == z_quarter)
    def _():
        ow[
            rows((4 * lax.rem(z, 4) + y) * 64, 64), pl.ds(pl.multiple_of(x * 256, 256), 256)
        ] = owsrc[...]

    for j in range(2):
        mine = jnp.logical_and(2 * c + j == y, y_half == c)
        start(
            remote(
                exsrc.at[j],
                exb.at[y_low],
                ex_send.at[j],
                ex_recv.at[y_low],
                at(x, 2 * c + j, z, y_half),
            ),
            jnp.logical_not(mine),
        )

        @pl.when(mine)
        def _():
            exb[y_low] = exsrc[j]

    up, down = (z_up, y, t), (z_down, y, t)

    def w_hop(d):
        if d == 0:
            mine = z_class == c
            for k in range(4):
                here = w_at(z, k)
                local = jnp.logical_and(y == k, y_half == c)

                @pl.when(jnp.logical_and(mine, jnp.logical_not(local)))
                def _():
                    remote(here, here, wy_send.at[0], wy_recv.at[k], up).wait_recv()

                start(remote(here, here, wz_send.at[0, 0, k], wz_recv.at[0, 1, k], up), mine)
                start(
                    remote(here, here, wz_send.at[1, 0, k], wz_recv.at[1, 1, k], down), mine
                )
            return
        for way, (target, far, last) in enumerate(((up, z - d, 8), (down, z + d, 7))):
            if d > last:
                continue
            origin = wrap(far, NZ)
            mine = lax.rem(lax.div(origin, 2), 2) == c
            for k in range(4):
                here = w_at(origin, k)
                copy = remote(
                    here, here, wz_send.at[way, d, k], wz_recv.at[way, d + 1, k], target
                )
                arrived = remote(
                    here, here, wz_send.at[way, d, k], wz_recv.at[way, d, k], target
                )
                pl.when(mine)(arrived.wait_recv)
                if d < last:
                    start(copy, mine)

    def ow_hop(d):
        if d == 0:
            mine = x == z_quarter
            for k in range(4):
                here = ow_at(z, k)

                @pl.when(jnp.logical_and(mine, x != k))
                def _():
                    remote(here, here, ox_send, ox_recv.at[k], up).wait_recv()

                start(remote(here, here, oz_send.at[0, 0, k], oz_recv.at[0, 1, k], up), mine)
                start(
                    remote(here, here, oz_send.at[1, 0, k], oz_recv.at[1, 1, k], down), mine
                )
            return
        for way, (target, far, last) in enumerate(((up, z - d, 8), (down, z + d, 7))):
            if d > last:
                continue
            origin = wrap(far, NZ)
            mine = lax.div(origin, 4) == x
            for k in range(4):
                here = ow_at(origin, k)
                copy = remote(
                    here, here, oz_send.at[way, d, k], oz_recv.at[way, d + 1, k], target
                )
                arrived = remote(
                    here, here, oz_send.at[way, d, k], oz_recv.at[way, d, k], target
                )
                pl.when(mine)(arrived.wait_recv)
                if d < last:
                    start(copy, mine)

    w_hop(0)
    ow_hop(0)

    lane = iota((TOK, TOK), 1)
    row = iota((TOK, TOK), 0)
    xors[...] = jnp.bitwise_xor(row, lane)
    one = jnp.ones((TOK, TOK), F32)
    nil = jnp.zeros((TOK, TOK), F32)

    def level_matrix(level, carry):
        half = lax.shift_left(jnp.int32(1), level)
        base = lane - jnp.bitwise_and(lane, 2 * half - 1)
        middle = base + half - 1
        low = jnp.minimum(lane, middle)
        high = jnp.maximum(lane, middle)
        mats[level] = jnp.where(
            jnp.logical_and(row > low, row <= high), one, nil
        ).astype(BF16)
        return carry

    lax.fori_loop(0, 8, level_matrix, 0)
    mats[8] = jnp.where(row <= lane, one, nil).astype(BF16)
    mats[9] = jnp.where(row > lane, one, nil).astype(BF16)

    for hop in range(1, 10):
        if hop <= 6:
            x_hop(hop)
        if hop <= 8:
            w_hop(hop)
        if hop >= 2:
            ow_hop(hop - 1)

    def project(half, target):
        def tile(s, carry):
            block = xg[rows((2 * half + s) * TOK, TOK), :]
            target[rows(s * TOK, TOK), :384] = jnp.dot(
                block, w[...], preferred_element_type=F32
            )
            squares = jnp.zeros((TOK, 128), F32)
            for k in range(16):
                piece = block[:, 128 * k : 128 * k + 128].astype(F32)
                squares = squares + piece * piece
            target[rows(s * TOK, TOK), 384:] = squares
            return carry

        lax.fori_loop(0, 2, tile, 0)

    project(1 - c, acc_send)
    swap = remote(acc_send, acc_recv, d2d_send.at[0], d2d_recv.at[0], partner)
    start(swap)
    project(c, acc_own)
    swap.wait_recv()

    low_lanes = iota((TOK, 128), 1) < 64

    def scaled(s):
        both = acc_own[rows(s * TOK, TOK), :] + acc_recv[rows(s * TOK, TOK), :]
        mean = jnp.sum(both[:, 384:], axis=1, keepdims=True) * (1.0 / 4096.0)
        factor = lax.rsqrt(mean + 1e-06)
        return (both[:, :384] * factor).astype(BF16).astype(F32)

    p0, p1 = scaled(0), scaled(1)

    first, second = p0[:, :128], p1[:, :128]
    left = jnp.where(low_lanes, first, roll64(second))
    right = jnp.where(low_lanes, roll64(first), second)
    ext[32:, :] = (left * sigmoid(right)).astype(BF16).astype(F32)
    start(
        remote(
            ext.at[pl.ds(TOK, 32), :], ext.at[pl.ds(0, 32), :], halo_send, halo_recv, up
        ),
        z < NZ - 1,
    )

    v0, v1 = p0[:, 128:256], p1[:, 128:256]
    gates = jnp.where(low_lanes, roll64(v0), v1)
    zero = jnp.zeros((TOK, 128), F32)
    v0 = jnp.where(low_lanes, v0, zero).astype(BF16)
    v1 = jnp.where(low_lanes, zero, roll64(v1)).astype(BF16)
    qt0, qt1 = p0[:, 256:].T, p1[:, 256:].T
    queries = jnp.concatenate([qt0[:32], qt1[:32]], axis=0) * (32.0 ** (-0.5))
    keys = jnp.concatenate([qt0[32:64], qt1[32:64]], axis=0)
    for s in range(2):
        local = jnp.logical_and(y_half == c, y_low == s)

        @pl.when(jnp.logical_not(local))
        def _():
            remote(exb.at[s], exb.at[s], ex_send.at[s], ex_recv.at[s], up).wait_recv()

    decays = []
    for s, qt in enumerate((qt0, qt1)):
        pre = (
            jnp.dot(dwt[...], qt[64:].astype(BF16), preferred_element_type=F32) + bias[...]
        )
        log_sig = jnp.minimum(pre, 0.0) - jnp.log1p(jnp.exp(-jnp.abs(pre)))
        decays.append(log_sig * (1.0 / 16.0) + exb[s])
    decay = jnp.concatenate(decays, axis=0)
    part0 = decay.astype(BF16)
    rest = decay - part0.astype(F32)
    part1 = rest.astype(BF16)
    part2 = (rest - part1.astype(F32)).astype(BF16)
    parts = jnp.concatenate([part0, part1, part2], axis=0)

    def decay_sums(which):
        sums = jnp.dot(parts, mats[which], preferred_element_type=F32)
        return jnp.exp(sums[:64] + sums[64:128] + sums[128:])

    tail_keys = (keys * decay_sums(9)).astype(BF16)
    st_me[...] = (
        jnp.dot(tail_keys[:32], v0, preferred_element_type=F32)
        + jnp.dot(tail_keys[32:], v1, preferred_element_type=F32)
    ).astype(BF16)
    wide = jnp.concatenate([decay, jnp.zeros((64, TOK), F32)], axis=0)
    tot_me[...] = lax.dot_general(
        jnp.ones((8, TOK), F32), wide, NT, precision=HIGHEST, preferred_element_type=F32
    )[:1]

    def tell(k, carry):
        @pl.when(z + k < NZ)
        def _():
            there = (z + k, y, t)
            remote(tot_me, tots.at[z], tot_send.at[k], tot_recv.at[z], there).start()
            remote(st_me, sts.at[z], st_send.at[k], st_recv.at[z], there).start()

        return carry

    lax.fori_loop(1, NZ, tell, 0)

    @pl.when(z == 0)
    def _():
        ext[:32, :] = jnp.zeros((32, 128), F32)

    @pl.when(z > 0)
    def _():
        halo = ext.at[pl.ds(0, 32), :]
        remote(halo, halo, halo_send, halo_recv, up).wait_recv()

    conv = jnp.zeros((TOK, 128), F32)
    for tap in range(31):
        conv = conv + taps[tap : tap + 1, :] * ext[2 + tap : 2 + tap + TOK, :]
    lane8, row8 = iota((8, 128), 1), iota((8, 128), 0)
    seq_of = lax.div(lane8, 64)
    pick_sum = jnp.where(row8 == seq_of, 1.0, 0.0).astype(F32)
    pick_square = jnp.where(row8 == seq_of + 2, 1.0, 0.0).astype(F32)
    me = 4 * x + y
    stats[me] = lax.dot_general(
        pick_sum, conv, NT, precision=HIGHEST, preferred_element_type=F32
    ) + lax.dot_general(
        pick_square, conv * conv, NT, precision=HIGHEST, preferred_element_type=F32
    )

    def stat_copy(k):
        other = lax.rem(me + k, 16)
        xx = lax.div(other, 4)
        return remote(
            stats.at[me],
            stats.at[me],
            stat_send.at[k],
            stat_recv.at[me],
            at(xx, other - 4 * xx, z, c),
        )

    def send_stat(k, carry):
        stat_copy(k).start()
        return carry

    lax.fori_loop(1, 16, send_stat, 0)

    y_next, y_prev = at(x, y_up, z, c), at(x, y_down, z, c)

    def oy_at(k, yy):
        return ow.at[rows((4 * k + yy) * 64, 64), :]

    for k in range(4):
        here = oy_at(k, y)
        start(remote(here, here, oy_send.at[0, k], oy_recv.at[0, k], y_next))
        start(remote(here, here, oy_send.at[1, k], oy_recv.at[1, k], y_prev))

    queries_low, keys_low = queries.astype(BF16), keys.astype(BF16)
    for s in range(2):
        own = lax.dot_general(
            queries_low[32 * s : 32 * s + 32],
            keys_low[32 * s : 32 * s + 32],
            TN,
            preferred_element_type=F32,
        )
        scores[s] = jnp.where(xors[...] == 0, own, 0.0)
    lane64 = iota((64, TOK), 1)

    def level_scores(level, carry):
        factor = decay_sums(level)
        upper = jnp.bitwise_and(lax.shift_right_logical(lane64, level), 1) == 1
        q_level = jnp.where(upper, queries * factor, 0.0).astype(BF16)
        k_level = jnp.where(upper, 0.0, keys * factor).astype(BF16)
        same = lax.shift_right_logical(xors[...], level + 1) == 0
        for s in range(2):
            pair = lax.dot_general(
                q_level[32 * s : 32 * s + 32],
                k_level[32 * s : 32 * s + 32],
                TN,
                preferred_element_type=F32,
            )
            scores[s] = scores[s] + jnp.where(same, pair, 0.0)
        return carry

    lax.fori_loop(0, 8, level_scores, 0)
    heads = jnp.dot(scores[0].astype(BF16), v0, preferred_element_type=F32) + jnp.dot(
        scores[1].astype(BF16), v1, preferred_element_type=F32
    )
    q_start = (queries * decay_sums(8)).astype(BF16)

    def wait_stat(k, carry):
        other = lax.rem(me + k, 16)
        there = stats.at[other]
        remote(there, there, stat_send.at[k], stat_recv.at[other], up).wait_recv()
        return carry

    lax.fori_loop(1, 16, wait_stat, 0)
    total = stats[0]
    for k in range(1, 16):
        total = total + stats[k]
    average = lax.dot_general(
        total, pick_sum * (1.0 / 1024.0), TN, precision=HIGHEST, preferred_element_type=F32
    )
    spread = lax.dot_general(
        total, pick_square * (1.0 / 1024.0), TN, precision=HIGHEST, preferred_element_type=F32
    )
    variance = jnp.maximum(spread - average * average, 0.0)
    normed = (conv - average) * lax.rsqrt(variance + 1e-05) * cgain[...]
    conv_act = normed * sigmoid(normed)

    for k in range(NZ - 1):

        @pl.when(k < z)
        def _():
            remote(
                tots.at[k], tots.at[k], tot_send.at[0], tot_recv.at[k], up
            ).wait_recv()
            remote(sts.at[k], sts.at[k], st_send.at[0], st_recv.at[k], up).wait_recv()

    row16 = iota((NZ, 128), 0)
    known = jnp.where(row16 < z, tots[:, 0, :], 0.0)
    from_row, to_row = iota((NZ, NZ), 0), iota((NZ, NZ), 1)
    between = jnp.where(
        jnp.logical_and(to_row > from_row, to_row < z), 1.0, 0.0
    ).astype(F32)
    exponent = jnp.dot(between, known, precision=HIGHEST, preferred_element_type=F32)
    reach = jnp.where(row16 < z, jnp.exp(exponent), 0.0)
    reach = jnp.concatenate([reach, jnp.zeros((128 - NZ, 128), F32)], axis=0).T
    low32 = iota((32, 128), 1) < 64
    entering = jnp.zeros((32, 128), F32)
    for k in range(NZ - 1):
        factor = jnp.where(low32, reach[:32, k : k + 1], reach[32:64, k : k + 1])
        state = jnp.where(z > k, sts[k].astype(F32), 0.0)
        entering = entering + factor * state
    heads = (
        heads
        + lax.dot_general(
            q_start[:32],
            jnp.where(low32, entering, 0.0).astype(BF16),
            TN,
            preferred_element_type=F32,
        )
        + lax.dot_general(
            q_start[32:],
            jnp.where(low32, 0.0, entering).astype(BF16),
            TN,
            preferred_element_type=F32,
        )
    )
    same_head = lax.div(iota((128, 128), 0), 64) == lax.div(iota((128, 128), 1), 64)
    mean_square = jnp.dot(
        heads * heads,
        jnp.where(same_head, 1.0 / 64.0, 0.0).astype(F32),
        precision=HIGHEST,
        preferred_element_type=F32,
    )
    gla_act = (
        heads * lax.rsqrt(mean_square + 1e-06) * hgain[...] * (gates * sigmoid(gates))
    )

    act_me[0] = jnp.where(low_lanes, conv_act, roll64(gla_act)).astype(BF16)
    act_me[1] = jnp.where(low_lanes, roll64(conv_act), gla_act).astype(BF16)
    act_cols = pl.ds(pl.multiple_of(x * 256 + y_low * 128, 128), 128)
    for s in range(2):
        for k in range(4):
            mine = (
                (x == k) & (2 * c + s == y) & (y_half == c)
            )
            start(
                remote(
                    act_me.at[s],
                    acts.at[:, act_cols],
                    act_send.at[s, k],
                    act_recv.at[2 * x + y_low],
                    at(k, 2 * c + s, z, y_half),
                ),
                jnp.logical_not(mine),
            )

            @pl.when(mine)
            def _():
                acts[:, act_cols] = act_me[s]

    def oy_wait(way, k, yy):
        here = oy_at(k, yy)
        remote(here, here, oy_send.at[0, 0], oy_recv.at[way, k], y_next).wait_recv()

    y_far = wrap(y + 2, 4)
    for k in range(2):
        oy_wait(0, k, y_down)
        here = oy_at(k, y_down)
        start(remote(here, here, oy_send.at[2, k], oy_recv.at[2, k], y_next))
        oy_wait(1, k + 2, y_up)
        here = oy_at(k + 2, y_up)
        start(remote(here, here, oy_send.at[2, k + 2], oy_recv.at[2, k + 2], y_prev))
    for k in range(2):
        oy_wait(0, k + 2, y_down)
        oy_wait(1, k, y_up)
    for k in range(4):
        oy_wait(2, k, y_far)

    for k in range(4):
        for j in range(2):
            local = (x == k) & (y_low == j) & (y_half == c)

            @pl.when(jnp.logical_not(local))
            def _():
                here = acts.at[:, pl.ds(256 * k + 128 * j, 128)]
                remote(
                    here, here, act_send.at[0, 0], act_recv.at[2 * k + j], up
                ).wait_recv()

    def output(half):
        return lax.dot_general(
            acts[...], ow[rows(half * 512, 512), :], NT, preferred_element_type=F32
        )

    po_send[...] = output(1 - c).astype(BF16)
    trade = remote(po_send, po_recv, d2d_send.at[1], d2d_recv.at[1], partner)
    start(trade)
    result = xin[...].astype(F32) + output(c)
    trade.wait_recv()
    out[...] = (result + po_recv[...].astype(F32)).astype(BF16)

    for copy, cond in finish:
        if cond is None:
            copy.wait_send()
        else:
            pl.when(cond)(copy.wait_send)

    def told(k, carry):
        @pl.when(z + k < NZ)
        def _():
            there = (z + k, y, t)
            remote(tot_me, tots.at[z], tot_send.at[k], tot_recv.at[z], there).wait_send()
            remote(st_me, sts.at[z], st_send.at[k], st_recv.at[z], there).wait_send()

        return carry

    lax.fori_loop(1, NZ, told, 0)

    def sent_stat(k, carry):
        stat_copy(k).wait_send()
        return carry

    lax.fori_loop(1, 16, sent_stat, 0)


def shards(
    inputs,
    norm_gain,
    conv_in_a,
    conv_in_b,
    query_w,
    key_w,
    value_w,
    out_gate_w,
    pointwise_w,
    gla_out_w,
    forget_first_factor,
    decay_w,
    decay_bias,
    decay_extra,
    conv_kernel,
    conv_gain,
    head_gain,
):
    z, y, t = lax.axis_index("sp"), lax.axis_index("fs"), lax.axis_index("tp")
    group = 4 * (t // 2) + y
    at_row = (4 * z + y) * 64
    gain = lax.dynamic_slice_in_dim(norm_gain, at_row, 64)[:, None, None]
    low_rank = lax.dynamic_slice_in_dim(forget_first_factor, at_row, 64)
    pieces = [
        a.reshape(64, 2, -1)
        for a in (conv_in_a, conv_in_b, value_w, out_gate_w, query_w, key_w)
    ]
    pieces.append(jnp.broadcast_to(low_rank[:, None, :], (64, 2, 64)))
    packed = jnp.concatenate(pieces, axis=2).astype(F32) * gain
    wsrc = packed.astype(BF16).transpose(1, 0, 2)
    owsrc = jnp.concatenate(
        [pointwise_w.reshape(64, 2, 64), gla_out_w.reshape(64, 2, 64)], axis=2
    ).reshape(64, 256)
    exsrc = decay_extra[0].T.reshape(2, 32, TOK)
    dwt = lax.dynamic_slice_in_dim(decay_w, group * 32, 32, 1).T
    bias = lax.dynamic_slice_in_dim(decay_bias, group * 32, 32)[:, None]
    taps = jnp.tile(lax.dynamic_slice_in_dim(conv_kernel, group * 64, 64, 1), (1, 2))
    cgain = jnp.tile(lax.dynamic_slice_in_dim(conv_gain, group * 64, 64), 2)[None]
    hgain = jnp.tile(head_gain, 2)[None]

    dma = pltpu.SemaphoreType.DMA
    vmem = pltpu.VMEM
    mixed = pl.pallas_call(
        body,
        out_shape=jax.ShapeDtypeStruct((TOK, 512), BF16),
        in_specs=[pl.BlockSpec(memory_space=vmem)] * 9,
        out_specs=pl.BlockSpec(memory_space=vmem),
        scratch_shapes=[
            vmem((4 * TOK, 2048), BF16),
            vmem((2048, 384), BF16),
            vmem((1024, 1024), BF16),
            vmem((512, 512), F32),
            vmem((512, 512), F32),
            vmem((512, 512), F32),
            vmem((10, TOK, TOK), BF16),
            vmem((TOK, TOK), jnp.int32),
            vmem((2, TOK, TOK), F32),
            vmem((TOK + 32, 128), F32),
            vmem((2, 32, TOK), F32),
            vmem((16, 8, TOK), F32),
            vmem((1, 128), F32),
            vmem((NZ, 1, 128), F32),
            vmem((32, 128), BF16),
            vmem((NZ, 32, 128), BF16),
            vmem((2, TOK, 128), BF16),
            vmem((TOK, 1024), BF16),
            vmem((TOK, 512), BF16),
            vmem((TOK, 512), BF16),
            dma((4, 4)),
            dma((4, 16)),
            dma((4, 16)),
            dma((2,)),
            dma((4,)),
            dma((2, 9, 4)),
            dma((2, 9, 4)),
            dma,
            dma((4,)),
            dma((2, 9, 4)),
            dma((2, 9, 4)),
            dma((3, 4)),
            dma((3, 4)),
            dma((2,)),
            dma((2,)),
            dma((2,)),
            dma((2,)),
            dma,
            dma,
            dma((16,)),
            dma((16,)),
            dma((16,)),
            dma((16,)),
            dma((16,)),
            dma((16,)),
            dma((2, 4)),
            dma((8,)),
        ],
        compiler_params=pltpu.CompilerParams(
            collective_id=0, has_side_effects=True, vmem_limit_bytes=48 * 1024 * 1024
        ),
        name="mixer",
    )(inputs[0], wsrc, owsrc, exsrc, dwt, bias, taps, cgain, hgain)
    return mixed[None]


def solution(mesh):
    weights = P(("sp", "fs"), "tp")
    return jax.shard_map(
        shards,
        mesh=mesh,
        in_specs=(
            P("fs", "sp", "tp"),
            P(),
            weights,
            weights,
            weights,
            weights,
            weights,
            weights,
            weights,
            weights,
            P(),
            P(),
            P(),
            P("fs", "sp", "tp"),
            P(),
            P(),
            P(),
        ),
        out_specs=P("fs", "sp", "tp"),
        check_vma=False,
    )
```

```python
import functools
import heapq

import jax
import jax.numpy as jnp
from jax import lax
from jax.experimental import pallas as pl
from jax.experimental.pallas import tpu as pltpu
from jax.sharding import PartitionSpec as P

MESH = pl.DeviceIdType.MESH
F32 = jnp.float32
BF16 = jnp.bfloat16
HIGHEST = lax.Precision.HIGHEST
NZ = 16
TOK = 256
NT = (((1,), (1,)), ((), ()))
TN = (((0,), (0,)), ((), ()))


def remote(src, dst, send, recv, device):
    return pltpu.make_async_remote_copy(
        src_ref=src,
        dst_ref=dst,
        send_sem=send,
        recv_sem=recv,
        device_id=device,
        device_id_type=MESH,
    )


def wrap(value, size):
    return lax.rem(value + size, size)


def rows(start, size):
    return pl.ds(pl.multiple_of(start, size), size)


def iota(shape, dim):
    return lax.broadcasted_iota(jnp.int32, shape, dim)


def sigmoid(value):
    return 1.0 / (1.0 + jnp.exp(-value))


def roll64(value):
    return pltpu.roll(value, 64, 1)


OFFSETS = (0, -1, 1, 2)
W_HOP = 2.2
OW_START, OW_HOP = 4.0, 3.0


def x_forwards(f, g, u):
    sends = []
    if g == 0:
        if f == 0:
            sends += [(0, 0, 1, 0), (0, 1, 2, 0)]
        elif f < 3 and u == f - 1:
            sends += [(0, u, 3, 0)]
        sends += [(1, 0, f, 1), (1, 1, f, 2)]
    elif g < 3 and u == g - 1:
        sends += [(1, u, f, 3)]
    return sends


def x_order():
    free, queue, done = {}, [], []

    def go(now, half, f, g, u):
        for which, way, ff, gg in x_forwards(f, g, u):
            link = ((which + half) % 2, way)
            free[link] = max(free.get(link, 0.0), now) + 1.4
            heapq.heappush(queue, (free[link] + 1.9, half, ff, gg, u))

    for u in range(2):
        for half in range(2):
            go(0.0, half, 0, 0, u)
    while queue:
        event = heapq.heappop(queue)
        done.append(event)
        go(*event)
    return done


def body(
    xin_hbm,
    gain_hbm,
    a_hbm,
    b_hbm,
    q_hbm,
    k_hbm,
    v_hbm,
    gate_hbm,
    point_hbm,
    gla_hbm,
    low_hbm,
    dw_hbm,
    bias_hbm,
    extra_hbm,
    kernel_hbm,
    cgain_hbm,
    hgain_hbm,
    out,
    gain_in,
    tiles_in,
    narrow_in,
    low_in,
    dw_in,
    bias_in,
    exsrc,
    taps_in,
    cgain_in,
    hgain_in,
    wsrc,
    owsrc,
    dwt,
    bias,
    taps,
    in_sem,
    xg,
    w,
    ow,
    acc_own,
    acc_send,
    acc_recv,
    mats,
    xors,
    scores,
    ext,
    exb,
    stats,
    tot_me,
    tots,
    st_me,
    sts,
    act_me,
    acts,
    po_send,
    po_recv,
    x_send,
    xd_send,
    xd_recv,
    own_send,
    ring_recv,
    wy_send,
    wy_recv,
    wz_send,
    wd_send,
    wd_recv,
    ox_send,
    ox_recv,
    oz_send,
    oz_recv,
    od_send,
    od_recv,
    oy_send,
    oy_recv,
    ex_send,
    ex_recv,
    d2d_send,
    d2d_recv,
    halo_send,
    halo_recv,
    stat_send,
    stat_recv,
    tot_send,
    tot_recv,
    st_send,
    st_recv,
    act_send,
    act_recv,
):
    scope = []

    def mark(name):
        if scope:
            scope.pop().__exit__(None, None, None)
        if name:
            scope.append(jax.named_scope(name))
            scope[0].__enter__()

    z = lax.axis_index("sp")
    y = lax.axis_index("fs")
    t = lax.axis_index("tp")
    x = lax.div(t, 2)
    c = t - 2 * x
    y_half = lax.div(y, 2)
    y_low = y - 2 * y_half
    z_class = lax.rem(lax.div(z, 2), 2)
    partner = (z, y, 2 * x + 1 - c)

    def at(xx, yy, zz, cc):
        return (zz, yy, 2 * xx + cc)

    mark("greet")
    group_pair = 2 * x + y_half

    def tile_of(index):
        return pl.ds(pl.multiple_of(index * 128, 128), 128)

    def feature_cols(xx, cc):
        return pl.ds(pl.multiple_of((2 * xx + cc) * 512, 512), 512)

    fetches = [
        pltpu.make_async_copy(source, target, in_sem.at[k])
        for k, (source, target) in enumerate(
            (
                (a_hbm, tiles_in.at[0]),
                (b_hbm, tiles_in.at[1]),
                (v_hbm, tiles_in.at[2]),
                (gate_hbm, tiles_in.at[3]),
                (point_hbm, tiles_in.at[4]),
                (gla_hbm, tiles_in.at[5]),
                (q_hbm, narrow_in.at[0]),
                (k_hbm, narrow_in.at[1]),
                (gain_hbm, gain_in),
                (low_hbm.at[:, tile_of(2 * z + y_half)], low_in),
                (xin_hbm, xg.at[rows(y * TOK, TOK), feature_cols(x, c)]),
                (extra_hbm, exsrc),
                (dw_hbm.at[:, tile_of(x)], dw_in),
                (bias_hbm, bias_in),
                (kernel_hbm.at[:, tile_of(group_pair)], taps_in),
                (cgain_hbm, cgain_in),
                (hgain_hbm, hgain_in),
            )
        )
    ]
    for fetch in fetches:
        fetch.start()

    barrier = pltpu.get_barrier_semaphore()

    def greet_plane(k, carry):
        flat = lax.rem(y * 8 + t + k, 32)
        yy = lax.div(flat, 8)
        pl.semaphore_signal(
            barrier, inc=1, device_id=(z, yy, flat - 8 * yy), device_id_type=MESH
        )
        return carry

    lax.fori_loop(1, 32, greet_plane, 0)

    for step in (1, NZ - 1):
        pl.semaphore_signal(
            barrier, inc=1, device_id=(lax.rem(z + step, NZ), y, t), device_id_type=MESH
        )

    mark("pack")
    low64 = iota((64, 128), 1) < 64
    lane64 = iota((64, 128), 1)
    y_even = y_low == 0

    def column(row_vector):
        return jnp.broadcast_to(row_vector, (128, 128)).T

    for fetch in fetches[:10]:
        fetch.wait()
    gain_all = column(gain_in[pl.ds(2 * z + y_half, 1), :])
    gain = jnp.where(y_even, gain_all[:64], gain_all[64:])

    def pair(k, scale):
        first = tiles_in[k].astype(F32) * scale
        second = tiles_in[k + 1].astype(F32) * scale
        return (
            jnp.where(low64, first, roll64(second)).astype(BF16),
            jnp.where(low64, roll64(first), second).astype(BF16),
        )

    for k in range(2):
        both = pair(2 * k, gain)
        for j in range(2):
            wsrc[j, :, 128 * k : 128 * k + 128] = both[j]
    both = pair(4, 1.0)
    for j in range(2):
        owsrc[:, 128 * j : 128 * j + 128] = both[j]
    narrow = jnp.concatenate([narrow_in[0], narrow_in[1]], axis=1).astype(F32)
    low_rows = low_in[...].astype(F32)
    low_rows = jnp.concatenate([low_rows, low_rows], axis=0).T
    low_rows = jnp.where(y_even, low_rows[:64], low_rows[64:])
    back32, back64 = pltpu.roll(narrow, 96, 1), roll64(narrow)
    mixed0 = jnp.where(low64, jnp.where(lane64 < 32, narrow, back32), low_rows)
    mixed1 = jnp.where(low64, jnp.where(lane64 < 32, back32, back64), low_rows)
    wsrc[0, :, 256:] = (mixed0 * gain).astype(BF16)
    wsrc[1, :, 256:] = (mixed1 * gain).astype(BF16)
    for fetch in fetches[10:12]:
        fetch.wait()
    mark("barrier_wait")
    pl.semaphore_wait(barrier, 31 + 2)

    finish = []

    def start(copy, cond=None):
        if cond is None:
            copy.start()
        else:
            pl.when(cond)(copy.start)
        finish.append((copy, cond))

    mark("first_sends")
    def w_at(zz, k):
        kind = lax.rem(lax.div(zz, 2), 2)
        begin = kind * 2048 + lax.div(zz, 4) * 512 + lax.rem(zz, 2) * 256 + k * 64
        return w.at[rows(begin, 64), :]

    for j in range(2):
        mine = jnp.logical_and(2 * c + j == y, c == 1)
        start(
            remote(
                wsrc.at[j], w_at(z, y), wy_send.at[j], wy_recv.at[y], at(x, 2 * c + j, z, 1)
            ),
            jnp.logical_not(mine),
        )

        @pl.when(mine)
        def _():
            w_at(z, y)[...] = wsrc[j]

    x_up, x_down = wrap(x + 1, 4), wrap(x - 1, 4)
    y_up, y_down = wrap(y + 1, 4), wrap(y - 1, 4)
    z_up, z_down = wrap(z + 1, NZ), wrap(z - 1, NZ)
    along_x = (at(x_up, y, z, c), at(x_down, y, z, c))
    along_y = (at(x, y_up, z, c), at(x, y_down, z, c))

    def x_rows(yy, half, u):
        return rows(yy * TOK + 128 * half + 64 * u, 64)

    def x_event(half, f, g, u):
        df, dg = OFFSETS[f], OFFSETS[g]
        xx, yy = (x + df, y + dg) if half == 0 else (x + dg, y + df)
        xx, yy = wrap(xx, 4), wrap(yy, 4)
        place = xg.at[
            x_rows(yy, half, u), pl.ds(pl.multiple_of(xx * 1024, 1024), 1024)
        ]
        others = xg.at[x_rows(yy, half, u), feature_cols(xx, 1)]
        slot = 32 * half + 8 * f + 2 * g + u
        if f == 0 and g == 0:
            remote(others, others, x_send, ring_recv.at[slot], partner).wait_recv()
        else:
            remote(place, place, x_send, ring_recv.at[slot], partner).wait_recv()
        first, second = (along_x, along_y) if half == 0 else (along_y, along_x)
        for which, way, ff, gg in x_forwards(f, g, u):
            remote(
                place,
                place,
                x_send,
                ring_recv.at[32 * half + 8 * ff + 2 * gg + u],
                (second if which else first)[way],
            ).start()
        if f or g:
            remote(others, others, xd_send, xd_recv, partner).start()

    @pl.when(c == 1)
    def _():
        for u in range(2):
            for half in range(2):
                mine = xg.at[x_rows(y, half, u), feature_cols(x, 1)]
                remote(
                    mine, mine, own_send, ring_recv.at[32 * half + u], partner
                ).start()

    def ow_rows(zz):
        return rows((4 * lax.rem(zz, 4) + y) * 64, 64)

    def ow_cols(xx):
        return pl.ds(pl.multiple_of(xx * 256, 256), 256)

    z_quarter = lax.div(z, 4)
    ow_mine = jnp.logical_and(x == z_quarter, c == 1)
    start(
        remote(
            owsrc,
            ow.at[c, ow_rows(z), ow_cols(x)],
            ox_send,
            ox_recv.at[c, x],
            at(z_quarter, y, z, 1),
        ),
        jnp.logical_not(ow_mine),
    )

    @pl.when(ow_mine)
    def _():
        ow[1, ow_rows(z), ow_cols(x)] = owsrc[...]

    for j in range(2):
        mine = jnp.logical_and(2 * c + j == y, y_half == c)
        start(
            remote(
                exsrc.at[j],
                exb.at[y_low],
                ex_send.at[j],
                ex_recv.at[y_low],
                at(x, 2 * c + j, z, y_half),
            ),
            jnp.logical_not(mine),
        )

        @pl.when(mine)
        def _():
            exb[y_low] = exsrc[j]

    up, down = (z_up, y, t), (z_down, y, t)

    ways = (up, down)

    def w_on(way, d, k, origin):
        here = w_at(origin, k)
        if d < 8 - way:
            remote(here, here, wz_send, ring_recv.at[4 * origin + k], ways[way]).start()
        if d == 0 and way == 0:
            return

        @pl.when(lax.rem(lax.div(origin, 2), 2) == 0)
        def _():
            remote(here, here, wd_send, wd_recv, partner).start()

    def w_start(k):
        here = w_at(z, k)

        @pl.when(jnp.logical_not(jnp.logical_and(y == k, y_half == 1)))
        def _():
            remote(here, here, wz_send, wy_recv.at[k], up).wait_recv()

        w_on(0, 0, k, z)
        w_on(1, 0, k, z)

    def w_event(way, d, k):
        origin = wrap(z - d if way == 0 else z + d, NZ)
        here = w_at(origin, k)
        remote(here, here, wz_send, ring_recv.at[4 * origin + k], up).wait_recv()
        w_on(way, d, k, origin)

    def ow_on(way, d, k, origin):
        here = ow.at[:, ow_rows(origin), ow_cols(k)]
        ours = ow.at[0, ow_rows(origin), ow_cols(k)]
        which = lax.rem(origin, 4)
        if d < 8 - way:
            remote(
                here, here, oz_send.at[way, which], oz_recv.at[which, k], ways[way]
            ).start()
        if d or way:
            remote(ours, ours, od_send, od_recv.at[which], partner).start()

    def ow_start(k):
        @pl.when(x == z_quarter)
        def _():
            for cc in range(2):
                part = ow.at[cc, ow_rows(z), ow_cols(k)]

                @pl.when(jnp.logical_not(jnp.logical_and(x == k, cc == 1)))
                def _():
                    remote(part, part, ox_send, ox_recv.at[cc, k], up).wait_recv()

            ow_on(0, 0, k, z)
            ow_on(1, 0, k, z)

    def ow_event(way, d, k):
        origin = wrap(z - d if way == 0 else z + d, NZ)

        @pl.when(lax.div(origin, 4) == x)
        def _():
            here = ow.at[:, ow_rows(origin), ow_cols(k)]
            remote(
                here, here, ox_send, oz_recv.at[lax.rem(origin, 4), k], up
            ).wait_recv()
            ow_on(way, d, k, origin)

    mark("params")
    for fetch in fetches[12:]:
        fetch.wait()
    dw_all = dw_in[...].astype(F32)
    dw_all = jnp.concatenate([dw_all, dw_all], axis=0).T
    dwt[...] = dw_all.astype(BF16)
    bias[...] = column(bias_in[pl.ds(x, 1), :])
    low31 = iota((31, 128), 1) < 64
    tap_rows = taps_in[...]
    tap_back = roll64(tap_rows)
    taps[:31, :] = jnp.where(low31 == y_even, tap_rows, tap_back)
    cgain_row = cgain_in[pl.ds(group_pair, 1), :]
    cgain = jnp.where(low31[:1] == y_even, cgain_row, roll64(cgain_row))
    hgain = jnp.concatenate([hgain_in[...], hgain_in[...]], axis=1)

    mark("constants")
    lane = iota((TOK, TOK), 1)
    row = iota((TOK, TOK), 0)
    xors[...] = jnp.bitwise_xor(row, lane)
    one = jnp.ones((TOK, TOK), F32)
    nil = jnp.zeros((TOK, TOK), F32)

    def level_matrix(level, carry):
        half = lax.shift_left(jnp.int32(1), level)
        base = lane - jnp.bitwise_and(lane, 2 * half - 1)
        middle = base + half - 1
        low = jnp.minimum(lane, middle)
        high = jnp.maximum(lane, middle)
        mats[level] = jnp.where(
            jnp.logical_and(row > low, row <= high), one, nil
        ).astype(BF16)
        return carry

    lax.fori_loop(0, 8, level_matrix, 0)
    mats[8] = jnp.where(row <= lane, one, nil).astype(BF16)
    mats[9] = jnp.where(row > lane, one, nil).astype(BF16)

    z_agenda = []
    for way in range(2):
        for d in range(1, 9 - way):
            for k in range(4):
                z_agenda.append((W_HOP * d + 0.5 * k, w_event, (way, d, k)))
                z_agenda.append((OW_START + OW_HOP * d + 0.5 * k, ow_event, (way, d, k)))
    z_agenda.sort(key=lambda entry: entry[0])
    needed = max(n for n, entry in enumerate(z_agenda) if entry[1] is w_event) + 1
    mark("gather")

    @pl.when(c == 0)
    def _():
        for u in range(2):
            for half in range(2):
                x_event(half, 0, 0, u)
        for n, (_, *event) in enumerate(x_order()):
            if n % 15 == 0:
                mark(f"x{n}")
            x_event(*event)
        mark("w_arrive")
        everything = w.at[pl.ds(0, 2048), :]
        remote(everything, everything, wd_send, wd_recv, partner).wait_recv()
        mark(None)

    @pl.when(c == 1)
    def _():
        for k in range(4):
            w_start(k)
        for k in range(4):
            ow_start(k)
        for n, (_, call, event) in enumerate(z_agenda[:needed]):
            if n % 24 == 0:
                mark(f"z{n}")
            call(*event)
        mark("x_arrive")
        everything = xg.at[pl.ds(0, 480), :]
        remote(everything, everything, xd_send, xd_recv, partner).wait_recv()
        mark(None)

    def oy_at(k, yy):
        return ow.at[c, rows((4 * k + yy) * 64, 64), :]

    def oy_own(k):
        for way in range(2):
            kk = (k + 2 * way) % 4
            here = oy_at(kk, y)
            remote(here, here, oy_send, oy_recv.at[way, kk], along_y[way]).start()

    def oy_wait(way, k, yy):
        here = oy_at(k, yy)
        remote(here, here, oy_send, oy_recv.at[way, k], partner).wait_recv()

    def oy_pass(k):
        for way, yy in enumerate((y_down, y_up)):
            kk = k + 2 * way
            oy_wait(way, kk, yy)
            here = oy_at(kk, yy)
            remote(here, here, oy_send, oy_recv.at[2, kk], along_y[way]).start()

    mark("project")
    def project(half, target):
        def tile(s, carry):
            blocks = [
                xg[rows((2 * half + s) * TOK, TOK), feature_cols(k, c)] for k in range(4)
            ]
            total = jnp.dot(blocks[0], w[rows(c * 2048, 512), :], preferred_element_type=F32)
            for k in range(1, 4):
                total = total + jnp.dot(
                    blocks[k],
                    w[rows(c * 2048 + 512 * k, 512), :],
                    preferred_element_type=F32,
                )
            target[rows(s * TOK, TOK), :384] = total
            squares = jnp.zeros((TOK, 128), F32)
            for k in range(16):
                piece = blocks[k // 4][:, 128 * (k % 4) : 128 * (k % 4) + 128].astype(F32)
                squares = squares + piece * piece
            target[rows(s * TOK, TOK), 384:] = squares
            return carry

        lax.fori_loop(0, 2, tile, 0)

    project(1 - c, acc_send)
    swap = remote(acc_send, acc_recv, d2d_send.at[0], d2d_recv.at[0], partner)
    start(swap)
    mark("late_weights")

    @pl.when(c == 1)
    def _():
        for _, call, event in z_agenda[needed:]:
            call(*event)

    @pl.when(c == 0)
    def _():
        for k in range(4):
            unit = oy_at(k, y)
            remote(unit, unit, od_send, od_recv.at[k], partner).wait_recv()

    oy_own(0)
    oy_own(1)
    mark("project2")
    project(c, acc_own)
    mark("swap_wait")
    oy_own(2)
    swap.wait_recv()

    mark("gating")
    low_lanes = iota((TOK, 128), 1) < 64

    def scaled(s):
        both = acc_own[rows(s * TOK, TOK), :] + acc_recv[rows(s * TOK, TOK), :]
        mean = jnp.sum(both[:, 384:], axis=1, keepdims=True) * (1.0 / 4096.0)
        factor = lax.rsqrt(mean + 1e-06)
        return (both[:, :384] * factor).astype(BF16).astype(F32)

    p0, p1 = scaled(0), scaled(1)

    first, second = p0[:, :128], p1[:, :128]
    left = jnp.where(low_lanes, first, roll64(second))
    right = jnp.where(low_lanes, roll64(first), second)
    ext[32:, :] = (left * sigmoid(right)).astype(BF16).astype(F32)
    start(
        remote(
            ext.at[pl.ds(TOK, 32), :], ext.at[pl.ds(0, 32), :], halo_send, halo_recv, up
        ),
        z < NZ - 1,
    )

    mark("decay")
    v0, v1 = p0[:, 128:256], p1[:, 128:256]
    gates = jnp.where(low_lanes, roll64(v0), v1)
    zero = jnp.zeros((TOK, 128), F32)
    v0 = jnp.where(low_lanes, v0, zero).astype(BF16)
    v1 = jnp.where(low_lanes, zero, roll64(v1)).astype(BF16)
    qt0, qt1 = p0[:, 256:].T, p1[:, 256:].T
    queries = jnp.concatenate([qt0[:32], qt1[:32]], axis=0) * (32.0 ** (-0.5))
    keys = jnp.concatenate([qt0[32:64], qt1[32:64]], axis=0)
    for s in range(2):
        local = jnp.logical_and(y_half == c, y_low == s)

        @pl.when(jnp.logical_not(local))
        def _():
            remote(exb.at[s], exb.at[s], ex_send.at[s], ex_recv.at[s], up).wait_recv()

    decays = []
    for s, qt in enumerate((qt0, qt1)):
        pre = (
            jnp.dot(
                dwt[rows(32 * y, 32), :][:, :64],
                qt[64:].astype(BF16),
                preferred_element_type=F32,
            )
            + bias[rows(32 * y, 32), :][:, :1]
        )
        log_sig = jnp.minimum(pre, 0.0) - jnp.log1p(jnp.exp(-jnp.abs(pre)))
        decays.append(log_sig * (1.0 / 16.0) + exb[s])
    decay = jnp.concatenate(decays, axis=0)
    part0 = decay.astype(BF16)
    rest = decay - part0.astype(F32)
    part1 = rest.astype(BF16)
    part2 = (rest - part1.astype(F32)).astype(BF16)
    parts = jnp.concatenate([part0, part1, part2], axis=0)

    def decay_sums(which):
        sums = jnp.dot(parts, mats[which], preferred_element_type=F32)
        return jnp.exp(sums[:64] + sums[64:128] + sums[128:])

    tail_keys = (keys * decay_sums(9)).astype(BF16)
    st_me[...] = (
        jnp.dot(tail_keys[:32], v0, preferred_element_type=F32)
        + jnp.dot(tail_keys[32:], v1, preferred_element_type=F32)
    ).astype(BF16)
    wide = jnp.concatenate([decay, jnp.zeros((64, TOK), F32)], axis=0)
    tot_me[...] = lax.dot_general(
        jnp.ones((8, TOK), F32), wide, NT, precision=HIGHEST, preferred_element_type=F32
    )[:1]

    def tell(k, carry):
        @pl.when(z + k < NZ)
        def _():
            there = (z + k, y, t)
            remote(tot_me, tots.at[z], tot_send.at[k], tot_recv.at[z], there).start()
            remote(st_me, sts.at[z], st_send.at[k], st_recv.at[z], there).start()

        return carry

    lax.fori_loop(1, NZ, tell, 0)

    oy_own(3)
    mark("attention")
    queries_low, keys_low = queries.astype(BF16), keys.astype(BF16)
    for s in range(2):
        own = lax.dot_general(
            queries_low[32 * s : 32 * s + 32],
            keys_low[32 * s : 32 * s + 32],
            TN,
            preferred_element_type=F32,
        )
        scores[s] = jnp.where(xors[...] == 0, own, 0.0)
    lane_of = iota((64, TOK), 1)

    def level_scores(level, carry):
        factor = decay_sums(level)
        upper = jnp.bitwise_and(lax.shift_right_logical(lane_of, level), 1) == 1
        q_level = jnp.where(upper, queries * factor, 0.0).astype(BF16)
        k_level = jnp.where(upper, 0.0, keys * factor).astype(BF16)
        same = lax.shift_right_logical(xors[...], level + 1) == 0
        for s in range(2):
            pair = lax.dot_general(
                q_level[32 * s : 32 * s + 32],
                k_level[32 * s : 32 * s + 32],
                TN,
                preferred_element_type=F32,
            )
            scores[s] = scores[s] + jnp.where(same, pair, 0.0)
        return carry

    lax.fori_loop(0, 4, level_scores, 0)

    mark("halo_wait")
    @pl.when(z == 0)
    def _():
        ext[:32, :] = jnp.zeros((32, 128), F32)

    @pl.when(z > 0)
    def _():
        halo = ext.at[pl.ds(0, 32), :]
        remote(halo, halo, halo_send, halo_recv, up).wait_recv()

    mark("conv")
    conv = jnp.zeros((TOK, 128), F32)
    for tap in range(31):
        conv = conv + taps[tap : tap + 1, :] * ext[2 + tap : 2 + tap + TOK, :]
    lane8, row8 = iota((8, 128), 1), iota((8, 128), 0)
    seq_of = lax.div(lane8, 64)
    pick_sum = jnp.where(row8 == seq_of, 1.0, 0.0).astype(F32)
    pick_square = jnp.where(row8 == seq_of + 2, 1.0, 0.0).astype(F32)
    me = 4 * x + y
    stats[me] = lax.dot_general(
        pick_sum, conv, NT, precision=HIGHEST, preferred_element_type=F32
    ) + lax.dot_general(
        pick_square, conv * conv, NT, precision=HIGHEST, preferred_element_type=F32
    )

    def stat_copy(k):
        other = lax.rem(me + k, 16)
        xx = lax.div(other, 4)
        return remote(
            stats.at[me],
            stats.at[me],
            stat_send,
            stat_recv,
            at(xx, other - 4 * xx, z, c),
        )

    def send_stat(k, carry):
        stat_copy(k).start()
        return carry

    lax.fori_loop(1, 16, send_stat, 0)

    oy_pass(0)

    mark("attention2")
    lax.fori_loop(4, 8, level_scores, 0)
    heads = jnp.dot(scores[0].astype(BF16), v0, preferred_element_type=F32) + jnp.dot(
        scores[1].astype(BF16), v1, preferred_element_type=F32
    )
    q_start = (queries * decay_sums(8)).astype(BF16)
    oy_pass(1)

    mark("stat_wait")
    others = stats.at[pl.ds(0, 15)]
    remote(others, others, stat_send, stat_recv, up).wait_recv()
    mark("norm")
    total = stats[0]
    for k in range(1, 16):
        total = total + stats[k]
    average = lax.dot_general(
        total, pick_sum * (1.0 / 1024.0), TN, precision=HIGHEST, preferred_element_type=F32
    )
    spread = lax.dot_general(
        total, pick_square * (1.0 / 1024.0), TN, precision=HIGHEST, preferred_element_type=F32
    )
    variance = jnp.maximum(spread - average * average, 0.0)
    normed = (conv - average) * lax.rsqrt(variance + 1e-05) * cgain
    conv_act = normed * sigmoid(normed)

    mark("state_wait")
    for k in range(NZ - 1):

        @pl.when(k < z)
        def _():
            remote(
                tots.at[k], tots.at[k], tot_send.at[0], tot_recv.at[k], up
            ).wait_recv()
            remote(sts.at[k], sts.at[k], st_send.at[0], st_recv.at[k], up).wait_recv()

    mark("heads")
    row16 = iota((NZ, 128), 0)
    known = jnp.where(row16 < z, tots[:, 0, :], 0.0)
    from_row, to_row = iota((NZ, NZ), 0), iota((NZ, NZ), 1)
    between = jnp.where(
        jnp.logical_and(to_row > from_row, to_row < z), 1.0, 0.0
    ).astype(F32)
    exponent = jnp.dot(between, known, precision=HIGHEST, preferred_element_type=F32)
    reach = jnp.where(row16 < z, jnp.exp(exponent), 0.0)
    reach = jnp.concatenate([reach, jnp.zeros((128 - NZ, 128), F32)], axis=0).T
    low32 = iota((32, 128), 1) < 64
    entering = jnp.zeros((32, 128), F32)
    for k in range(NZ - 1):
        factor = jnp.where(low32, reach[:32, k : k + 1], reach[32:64, k : k + 1])
        state = jnp.where(z > k, sts[k].astype(F32), 0.0)
        entering = entering + factor * state
    heads = (
        heads
        + lax.dot_general(
            q_start[:32],
            jnp.where(low32, entering, 0.0).astype(BF16),
            TN,
            preferred_element_type=F32,
        )
        + lax.dot_general(
            q_start[32:],
            jnp.where(low32, 0.0, entering).astype(BF16),
            TN,
            preferred_element_type=F32,
        )
    )
    same_head = lax.div(iota((128, 128), 0), 64) == lax.div(iota((128, 128), 1), 64)
    mean_square = jnp.dot(
        heads * heads,
        jnp.where(same_head, 1.0 / 64.0, 0.0).astype(F32),
        precision=HIGHEST,
        preferred_element_type=F32,
    )
    gla_act = (
        heads * lax.rsqrt(mean_square + 1e-06) * hgain * (gates * sigmoid(gates))
    )

    mark("act_send")
    act_me[0] = jnp.where(low_lanes, conv_act, roll64(gla_act)).astype(BF16)
    act_me[1] = jnp.where(low_lanes, roll64(conv_act), gla_act).astype(BF16)
    act_cols = pl.ds(pl.multiple_of(x * 256 + y_low * 128, 128), 128)
    for s in range(2):
        for k in range(4):
            mine = (
                (x == k) & (2 * c + s == y) & (y_half == c)
            )
            copy = remote(
                act_me.at[s],
                acts.at[:, act_cols],
                act_send,
                act_recv,
                at(k, 2 * c + s, z, y_half),
            )
            pl.when(jnp.logical_not(mine))(copy.start)

            @pl.when(mine)
            def _():
                acts[:, act_cols] = act_me[s]

    mark("oy_rest")
    y_far = wrap(y + 2, 4)
    for k in range(2):
        oy_wait(0, k + 2, y_down)
        oy_wait(1, k, y_up)
    for k in range(4):
        oy_wait(2, k, y_far)

    mark("act_wait")
    def act_bytes():
        return acts.at[:, pl.ds(0, 896)], acts

    for piece, cond in zip(act_bytes(), (y_half == c, y_half != c)):

        @pl.when(cond)
        def _():
            remote(piece, piece, act_send, act_recv, up).wait_recv()

    mark("output")
    def output(half):
        return lax.dot_general(
            acts[...], ow[c, rows(half * 512, 512), :], NT, preferred_element_type=F32
        )

    po_send[...] = output(1 - c).astype(BF16)
    trade = remote(po_send, po_recv, d2d_send.at[1], d2d_recv.at[1], partner)
    start(trade)
    residual = xg[rows(y * TOK, TOK), feature_cols(x, c)]
    result = residual.astype(F32) + output(c)
    mark("trade_wait")
    trade.wait_recv()
    out[...] = (result + po_recv[...].astype(F32)).astype(BF16)

    mark("drain")
    for copy, cond in finish:
        if cond is None:
            copy.wait_send()
        else:
            pl.when(cond)(copy.wait_send)

    def told(k, carry):
        @pl.when(z + k < NZ)
        def _():
            there = (z + k, y, t)
            remote(tot_me, tots.at[z], tot_send.at[k], tot_recv.at[z], there).wait_send()
            remote(st_me, sts.at[z], st_send.at[k], st_recv.at[z], there).wait_send()

        return carry

    lax.fori_loop(1, NZ, told, 0)

    def left(piece, semaphore, cond=None):
        copy = remote(piece, piece, semaphore, stat_recv, partner)
        if cond is None:
            copy.wait_send()
        else:
            pl.when(cond)(copy.wait_send)

    left(stats.at[pl.ds(0, 15)], stat_send)
    left(ow.at[c, pl.ds(0, 768), :], oy_send)
    for piece, cond in zip(act_bytes(), (y_half == c, y_half != c)):
        left(piece, act_send, cond)
    left(xg.at[pl.ds(0, 960), :], x_send, c == 0)
    left(xg.at[pl.ds(0, 480), :], xd_send, c == 0)
    left(xg.at[pl.ds(0, 32), :], own_send, c == 1)
    left(w.at[pl.ds(0, 3840), :], wz_send, c == 1)
    left(w.at[pl.ds(0, 2048), :], wd_send, c == 1)
    left(ow.at[0, pl.ds(0, 256), :], od_send, c == 1)
    for way in range(2):
        for k in range(4):
            origin = 4 * x + k
            hops = wrap(z - origin if way == 0 else origin - z, NZ)
            left(
                ow.at[:, pl.ds(0, 64), :],
                oz_send.at[way, k],
                jnp.logical_and(c == 1, hops < 8 - way),
            )
    mark(None)


def shards(
    inputs,
    norm_gain,
    conv_in_a,
    conv_in_b,
    query_w,
    key_w,
    value_w,
    out_gate_w,
    pointwise_w,
    gla_out_w,
    forget_first_factor,
    decay_w,
    decay_bias,
    decay_extra,
    conv_kernel,
    conv_gain,
    head_gain,
):
    dma = pltpu.SemaphoreType.DMA
    vmem = pltpu.VMEM
    mixed = pl.pallas_call(
        body,
        out_shape=jax.ShapeDtypeStruct((TOK, 512), BF16),
        in_specs=[pl.BlockSpec(memory_space=pltpu.HBM)] * 17,
        out_specs=pl.BlockSpec(memory_space=vmem),
        scratch_shapes=[
            vmem((32, 128), F32),
            vmem((6, 64, 128), BF16),
            vmem((2, 64, 64), BF16),
            vmem((64, 128), BF16),
            vmem((64, 128), BF16),
            vmem((4, 128), F32),
            vmem((2, 32, TOK), F32),
            vmem((31, 128), F32),
            vmem((8, 128), F32),
            vmem((1, 64), F32),
            vmem((2, 64, 384), BF16),
            vmem((64, 256), BF16),
            vmem((128, 128), BF16),
            vmem((128, 128), F32),
            vmem((32, 128), F32),
            dma((17,)),
            vmem((4 * TOK, 4096), BF16),
            vmem((4096, 384), BF16),
            vmem((2, 1024, 1024), BF16),
            vmem((512, 512), F32),
            vmem((512, 512), F32),
            vmem((512, 512), F32),
            vmem((10, TOK, TOK), BF16),
            vmem((TOK, TOK), jnp.int32),
            vmem((2, TOK, TOK), F32),
            vmem((TOK + 32, 128), F32),
            vmem((2, 32, TOK), F32),
            vmem((16, 8, TOK), F32),
            vmem((1, 128), F32),
            vmem((NZ, 1, 128), F32),
            vmem((32, 128), BF16),
            vmem((NZ, 32, 128), BF16),
            vmem((2, TOK, 128), BF16),
            vmem((TOK, 1024), BF16),
            vmem((TOK, 512), BF16),
            vmem((TOK, 512), BF16),
            dma,
            dma,
            dma,
            dma,
            dma((64,)),
            dma((2,)),
            dma((4,)),
            dma,
            dma,
            dma,
            dma,
            dma((2, 4)),
            dma((2, 4)),
            dma((4, 4)),
            dma,
            dma((4,)),
            dma,
            dma((3, 4)),
            dma((2,)),
            dma((2,)),
            dma((2,)),
            dma((2,)),
            dma,
            dma,
            dma,
            dma,
            dma((16,)),
            dma((16,)),
            dma((16,)),
            dma((16,)),
            dma,
            dma,
        ],
        compiler_params=pltpu.CompilerParams(
            collective_id=0, has_side_effects=True
        ),
        name="mixer",
    )(
        inputs[0],
        norm_gain.reshape(32, 128),
        conv_in_a,
        conv_in_b,
        query_w,
        key_w,
        value_w,
        out_gate_w,
        pointwise_w,
        gla_out_w,
        forget_first_factor.T,
        decay_w,
        decay_bias.reshape(4, 128),
        decay_extra[0].T.reshape(2, 32, TOK),
        conv_kernel,
        conv_gain.reshape(8, 128),
        head_gain.reshape(1, 64),
    )
    return mixed[None]


def solution(mesh):
    weights = P(("sp", "fs"), "tp")
    return jax.shard_map(
        shards,
        mesh=mesh,
        in_specs=(
            P("fs", "sp", "tp"),
            P(),
            weights,
            weights,
            weights,
            weights,
            weights,
            weights,
            weights,
            weights,
            P(),
            P(),
            P(),
            P("fs", "sp", "tp"),
            P(),
            P(),
            P(),
        ),
        out_specs=P("fs", "sp", "tp"),
        check_vma=False,
    )
```

```python
import functools
import heapq

import jax
import jax.numpy as jnp
from jax import lax
from jax.experimental import pallas as pl
from jax.experimental.pallas import tpu as pltpu
from jax.sharding import PartitionSpec as P

MESH = pl.DeviceIdType.MESH
F32 = jnp.float32
BF16 = jnp.bfloat16
HIGHEST = lax.Precision.HIGHEST
NZ = 16
TOK = 256
NT = (((1,), (1,)), ((), ()))
TN = (((0,), (0,)), ((), ()))


def remote(src, dst, send, recv, device):
    return pltpu.make_async_remote_copy(
        src_ref=src,
        dst_ref=dst,
        send_sem=send,
        recv_sem=recv,
        device_id=device,
        device_id_type=MESH,
    )


def wrap(value, size):
    return lax.rem(value + size, size)


def rows(start, size):
    return pl.ds(pl.multiple_of(start, size), size)


def iota(shape, dim):
    return lax.broadcasted_iota(jnp.int32, shape, dim)


def sigmoid(value):
    return 1.0 / (1.0 + jnp.exp(-value))


def roll64(value):
    return pltpu.roll(value, 64, 1)


OFFSETS = (0, -1, 1, 2)
UNIT = (64, 64)
W_HOP, W_PART = 2.7, 0.55


def x_forwards(f, g, u):
    sends = []
    if g == 0:
        if f == 0:
            sends += [(0, 0, 1, 0), (0, 1, 2, 0)]
        elif f < 3 and u == f - 1:
            sends += [(0, u, 3, 0)]
        sends += [(1, 0, f, 1), (1, 1, f, 2)]
    elif g < 3 and u == g - 1:
        sends += [(1, u, f, 3)]
    return sends


def x_order():
    free, queue, done = {}, [], []

    def go(now, half, f, g, u):
        for which, way, ff, gg in x_forwards(f, g, u):
            link = ((which + half) % 2, way)
            free[link] = max(free.get(link, 0.0), now) + 1.41 * UNIT[half] / 64
            heapq.heappush(queue, (free[link] + 2.5, half, ff, gg, u))

    for u in range(2):
        for half in range(2):
            go(0.0, half, 0, 0, u)
    while queue:
        event = heapq.heappop(queue)
        done.append(event)
        go(*event)
    return done


def body(
    xin_hbm,
    gain_hbm,
    a_hbm,
    b_hbm,
    q_hbm,
    k_hbm,
    v_hbm,
    gate_hbm,
    point_hbm,
    gla_hbm,
    low_hbm,
    dw_hbm,
    bias_hbm,
    extra_hbm,
    kernel_hbm,
    cgain_hbm,
    hgain_hbm,
    out,
    gain_in,
    tiles_in,
    narrow_in,
    low_in,
    dw_in,
    bias_in,
    exsrc,
    taps_in,
    cgain_in,
    hgain_in,
    wsrc,
    owsrc,
    dwt,
    bias,
    taps,
    in_sem,
    xg,
    w,
    ow,
    owz,
    acc_own,
    acc_send,
    acc_recv,
    mats,
    xors,
    scores,
    ext,
    exb,
    stats,
    tot_me,
    tots,
    st_me,
    sts,
    act_me,
    acts,
    po_send,
    po_recv,
    x_send,
    xd_send,
    xd_recv,
    own_send,
    ring_recv,
    wy_send,
    wy_recv,
    wz_send,
    wd_send,
    wd_recv,
    ox_recv,
    oz_send,
    oz_recv,
    od_send,
    od_recv,
    oy_send,
    oy_recv,
    ex_send,
    ex_recv,
    d2d_send,
    d2d_recv,
    halo_send,
    halo_recv,
    stat_send,
    stat_recv,
    tot_send,
    tot_recv,
    st_send,
    st_recv,
    act_send,
    act_recv,
    act2_send,
    act2_recv,
):
    scope = []

    def mark(name):
        if scope:
            scope.pop().__exit__(None, None, None)
        if name:
            scope.append(jax.named_scope(name))
            scope[0].__enter__()

    z = lax.axis_index("sp")
    y = lax.axis_index("fs")
    t = lax.axis_index("tp")
    x = lax.div(t, 2)
    c = t - 2 * x
    y_half = lax.div(y, 2)
    y_low = y - 2 * y_half
    z_class = lax.rem(lax.div(z, 2), 2)
    partner = (z, y, 2 * x + 1 - c)

    def at(xx, yy, zz, cc):
        return (zz, yy, 2 * xx + cc)

    mark("greet")
    barrier = pltpu.get_barrier_semaphore()

    def greet(zz, yy, tt):
        pl.semaphore_signal(barrier, inc=1, device_id=(zz, yy, tt), device_id_type=MESH)

    for step in (1, NZ - 1):
        greet(lax.rem(z + step, NZ), y, t)
    for step in range(1, 8):
        greet(z, y, lax.rem(t + step, 8))
    for step in range(1, 4):
        for cc in range(2):
            greet(z, lax.rem(y + step, 4), 2 * x + cc)

    group_pair = 2 * x + y_half

    def tile_of(index):
        return pl.ds(pl.multiple_of(index * 128, 128), 128)

    def feature_cols(xx, cc):
        return pl.ds(pl.multiple_of((2 * xx + cc) * 512, 512), 512)

    fetches = [
        pltpu.make_async_copy(source, target, in_sem.at[k])
        for k, (source, target) in enumerate(
            (
                (a_hbm, tiles_in.at[0]),
                (b_hbm, tiles_in.at[1]),
                (v_hbm, tiles_in.at[2]),
                (gate_hbm, tiles_in.at[3]),
                (point_hbm, tiles_in.at[4]),
                (gla_hbm, tiles_in.at[5]),
                (q_hbm, narrow_in.at[0]),
                (k_hbm, narrow_in.at[1]),
                (gain_hbm, gain_in),
                (low_hbm.at[:, tile_of(2 * z + y_half)], low_in),
                (xin_hbm, xg.at[rows(y * TOK, TOK), feature_cols(x, c)]),
                (extra_hbm, exsrc),
                (dw_hbm.at[:, tile_of(x)], dw_in),
                (bias_hbm, bias_in),
                (kernel_hbm.at[:, tile_of(group_pair)], taps_in),
                (cgain_hbm, cgain_in),
                (hgain_hbm, hgain_in),
            )
        )
    ]
    for fetch in fetches:
        fetch.start()

    mark("pack")
    low64 = iota((64, 128), 1) < 64
    lane64 = iota((64, 128), 1)
    y_even = y_low == 0

    def column(row_vector):
        return jnp.broadcast_to(row_vector, (128, 128)).T

    for fetch in fetches[:10]:
        fetch.wait()
    gain_all = column(gain_in[pl.ds(2 * z + y_half, 1), :])
    gain = jnp.where(y_even, gain_all[:64], gain_all[64:])

    def pair(k, scale):
        first = tiles_in[k].astype(F32) * scale
        second = tiles_in[k + 1].astype(F32) * scale
        return (
            jnp.where(low64, first, roll64(second)).astype(BF16),
            jnp.where(low64, roll64(first), second).astype(BF16),
        )

    for k in range(2):
        both = pair(2 * k, gain)
        for j in range(2):
            wsrc[j, :, 128 * k : 128 * k + 128] = both[j]
    both = pair(4, 1.0)
    for j in range(2):
        owsrc[:, 128 * j : 128 * j + 128] = both[j]
    narrow = jnp.concatenate([narrow_in[0], narrow_in[1]], axis=1).astype(F32)
    low_rows = low_in[...].astype(F32)
    low_rows = jnp.concatenate([low_rows, low_rows], axis=0).T
    low_rows = jnp.where(y_even, low_rows[:64], low_rows[64:])
    back32, back64 = pltpu.roll(narrow, 96, 1), roll64(narrow)
    mixed0 = jnp.where(low64, jnp.where(lane64 < 32, narrow, back32), low_rows)
    mixed1 = jnp.where(low64, jnp.where(lane64 < 32, back32, back64), low_rows)
    wsrc[0, :, 256:] = (mixed0 * gain).astype(BF16)
    wsrc[1, :, 256:] = (mixed1 * gain).astype(BF16)
    for fetch in fetches[10:12]:
        fetch.wait()
    mark("barrier_wait")
    pl.semaphore_wait(barrier, 2 + 7 + 6)

    finish = []

    def start(copy, cond=None):
        if cond is None:
            copy.start()
        else:
            pl.when(cond)(copy.start)
        finish.append((copy, cond))

    mark("first_sends")
    def w_at(zz, k):
        kind = lax.rem(lax.div(zz, 2), 2)
        begin = kind * 2048 + lax.div(zz, 4) * 512 + lax.rem(zz, 2) * 256 + k * 64
        return w.at[rows(begin, 64), :]

    for j in range(2):
        mine = jnp.logical_and(2 * c + j == y, c == 1)
        start(
            remote(
                wsrc.at[j], w_at(z, y), wy_send.at[j], wy_recv.at[y], at(x, 2 * c + j, z, 1)
            ),
            jnp.logical_not(mine),
        )

        @pl.when(mine)
        def _():
            w_at(z, y)[...] = wsrc[j]

    x_up, x_down = wrap(x + 1, 4), wrap(x - 1, 4)
    y_up, y_down = wrap(y + 1, 4), wrap(y - 1, 4)
    z_up, z_down = wrap(z + 1, NZ), wrap(z - 1, NZ)
    along_x = (at(x_up, y, z, 0), at(x_down, y, z, 0))
    along_y = (at(x, y_up, z, 0), at(x, y_down, z, 0))

    def x_rows(yy, half, u):
        begin = yy * TOK + 2 * UNIT[0] * half + UNIT[half] * u
        return pl.ds(pl.multiple_of(begin, 16), UNIT[half])

    def x_event(half, f, g, u):
        df, dg = OFFSETS[f], OFFSETS[g]
        xx, yy = (x + df, y + dg) if half == 0 else (x + dg, y + df)
        xx, yy = wrap(xx, 4), wrap(yy, 4)
        place = xg.at[
            x_rows(yy, half, u), pl.ds(pl.multiple_of(xx * 1024, 1024), 1024)
        ]
        others = xg.at[x_rows(yy, half, u), feature_cols(xx, 1)]
        slot = 32 * half + 8 * f + 2 * g + u
        if f == 0 and g == 0:
            place = xg.at[x_rows(yy, half, u), feature_cols(xx, c)]
        else:
            remote(place, place, x_send, ring_recv.at[slot], partner).wait_recv()
        first, second = (along_x, along_y) if half == 0 else (along_y, along_x)
        for which, way, ff, gg in x_forwards(f, g, u):
            remote(
                place,
                place,
                x_send,
                ring_recv.at[32 * half + 8 * ff + 2 * gg + u],
                (second if which else first)[way],
            ).start()
        if f or g:
            remote(others, others, xd_send, xd_recv, partner).start()

    for u in range(2):
        for half in range(2):
            x_event(half, 0, 0, u)

    @pl.when(c == 0)
    def _():
        remote(owsrc, owz.at[z, 0], own_send, ox_recv, partner).start()

    @pl.when(c == 1)
    def _():
        owz[z, 1] = owsrc[...]

    for j in range(2):
        mine = jnp.logical_and(2 * c + j == y, y_half == c)
        start(
            remote(
                exsrc.at[j],
                exb.at[y_low],
                ex_send.at[j],
                ex_recv.at[y_low],
                at(x, 2 * c + j, z, y_half),
            ),
            jnp.logical_not(mine),
        )

        @pl.when(mine)
        def _():
            exb[y_low] = exsrc[j]

    up, down = (z_up, y, t), (z_down, y, t)

    ways = (up, down)

    def w_on(way, d, k, origin):
        here = w_at(origin, k)
        if d < 8 - way:
            remote(here, here, wz_send, ring_recv.at[4 * origin + k], ways[way]).start()
        if d == 0 and way == 0:
            return

        @pl.when(lax.rem(lax.div(origin, 2), 2) == 0)
        def _():
            remote(here, here, wd_send, wd_recv, partner).start()

    def w_start(k):
        here = w_at(z, k)

        @pl.when(jnp.logical_not(jnp.logical_and(y == k, y_half == 1)))
        def _():
            remote(here, here, wz_send, wy_recv.at[k], up).wait_recv()

        w_on(0, 0, k, z)
        w_on(1, 0, k, z)

    def w_event(way, d, k):
        origin = wrap(z - d if way == 0 else z + d, NZ)
        here = w_at(origin, k)
        remote(here, here, wz_send, ring_recv.at[4 * origin + k], up).wait_recv()
        w_on(way, d, k, origin)

    def ow_cols(xx):
        return pl.ds(pl.multiple_of(xx * 256, 256), 256)

    def ow_at(zz):
        k = lax.rem(zz, 4)
        half = lax.div(k, 2)
        return ow.at[half, rows(y * 128 + (k - 2 * half) * 64, 64), ow_cols(x)]

    def ow_on(way, d, origin):
        here = owz.at[origin]
        if d < 8 - way:
            remote(here, here, oz_send, oz_recv.at[origin], ways[way]).start()

    def ow_give(n, carry):
        turn = lax.div(n, 4)
        ahead = jnp.where(turn == 2, 3, jnp.where(turn == 3, 2, turn))
        column = lax.rem(x + ahead, 4)
        origin = 4 * column + lax.rem(n, 4)
        behind = lax.rem(4 - ahead, 4)
        place = ow_at(origin)

        def give(cc):
            remote(
                owz.at[origin, cc], place, od_send, od_recv.at[behind], at(column, y, z, cc)
            ).start()

        give(0)
        pl.when(column != x)(functools.partial(give, 1))

        @pl.when(column == x)
        def _():
            place[...] = owz[origin, 1]

        return carry

    def ow_start():
        remote(owz.at[z, 0], owz.at[z, 0], oz_send, ox_recv, partner).wait_recv()
        ow_on(0, 0, z)
        ow_on(1, 0, z)

    def ow_event(way, d, k):
        origin = wrap(z - d if way == 0 else z + d, NZ)
        here = owz.at[origin]
        remote(here, here, oz_send, oz_recv.at[origin], up).wait_recv()
        ow_on(way, d, origin)

    mark("params")
    for fetch in fetches[12:]:
        fetch.wait()
    dw_all = dw_in[...].astype(F32)
    dw_all = jnp.concatenate([dw_all, dw_all], axis=0).T
    dwt[...] = dw_all.astype(BF16)
    bias[...] = column(bias_in[pl.ds(x, 1), :])
    low31 = iota((31, 128), 1) < 64
    tap_rows = taps_in[...]
    tap_back = roll64(tap_rows)
    taps[:31, :] = jnp.where(low31 == y_even, tap_rows, tap_back)
    cgain_row = cgain_in[pl.ds(group_pair, 1), :]
    cgain = jnp.where(low31[:1] == y_even, cgain_row, roll64(cgain_row))
    hgain = jnp.concatenate([hgain_in[...], hgain_in[...]], axis=1)

    mark("constants")
    lane = iota((TOK, TOK), 1)
    row = iota((TOK, TOK), 0)
    xors[...] = jnp.bitwise_xor(row, lane)
    one = jnp.ones((TOK, TOK), F32)
    nil = jnp.zeros((TOK, TOK), F32)

    def level_matrix(level, carry):
        half = lax.shift_left(jnp.int32(1), level)
        base = lane - jnp.bitwise_and(lane, 2 * half - 1)
        middle = base + half - 1
        low = jnp.minimum(lane, middle)
        high = jnp.maximum(lane, middle)
        mats[level] = jnp.where(
            jnp.logical_and(row > low, row <= high), one, nil
        ).astype(BF16)
        return carry

    lax.fori_loop(0, 8, level_matrix, 0)
    mats[8] = jnp.where(row <= lane, one, nil).astype(BF16)
    mats[9] = jnp.where(row > lane, one, nil).astype(BF16)

    z_agenda = []
    for way in range(2):
        for d in range(1, 9 - way):
            for k in range(5):
                call = ow_event if k == 4 else w_event
                z_agenda.append((W_HOP * d + W_PART * k, call, (way, d, k)))
    z_agenda.sort(key=lambda entry: entry[0])
    mark("gather")

    @pl.when(c == 0)
    def _():
        for n, (_, *event) in enumerate(x_order()):
            if n % 15 == 0:
                mark(f"x{n}")
            x_event(*event)
        mark("w_arrive")
        everything = w.at[pl.ds(0, 2048), :]
        remote(everything, everything, wd_send, wd_recv, partner).wait_recv()
        mark(None)

    @pl.when(c == 1)
    def _():
        for k in range(4):
            w_start(k)
        ow_start()
        for n, (_, call, event) in enumerate(z_agenda):
            if n % 24 == 0:
                mark(f"z{n}")
            call(*event)
        lax.fori_loop(0, 16, ow_give, 0)
        mark("x_arrive")
        everything = xg.at[pl.ds(0, 480), :]
        remote(everything, everything, xd_send, xd_recv, partner).wait_recv()
        mark(None)

    y_next = (at(x, y_up, z, c), at(x, y_down, z, c))
    y_from = (y_down, y_up)
    y_far = wrap(y + 2, 4)

    def oy_at(yy, ahead):
        return ow.at[:, rows(yy * 128, 128), ow_cols(lax.rem(x + ahead, 4))]

    def oy_own(way, ahead):
        here = oy_at(y, ahead)
        remote(here, here, oy_send, oy_recv.at[way, ahead], y_next[way]).start()

    def oy_wait(way, ahead, yy):
        here = oy_at(yy, ahead)
        remote(here, here, oy_send, oy_recv.at[way, ahead], partner).wait_recv()

    def oy_pass(way, ahead):
        oy_wait(way, ahead, y_from[way])
        here = oy_at(y_from[way], ahead)
        remote(here, here, oy_send, oy_recv.at[2, ahead], y_next[way]).start()

    mark("project")
    def swap_part(n):
        part = pl.ds(128, 384) if n == 0 else pl.ds(0, 128)
        return remote(
            acc_send.at[:, part], acc_recv.at[:, part], d2d_send.at[n], d2d_recv.at[n], partner
        )

    def project(half, target, n):
        begin, size = (128, 256) if n == 0 else (0, 128)
        for s in range(2):
            at_rows = pl.ds(s * TOK, TOK)
            blocks = [
                xg[rows((2 * half + s) * TOK, TOK), feature_cols(k, c)] for k in range(4)
            ]
            total = jnp.zeros((TOK, size), F32)
            for k in range(4):
                total = total + jnp.dot(
                    blocks[k],
                    w[rows(c * 2048 + 512 * k, 512), begin : begin + size],
                    preferred_element_type=F32,
                )
            target[at_rows, begin : begin + size] = total
            if n:
                continue
            squares = jnp.zeros((TOK, 128), F32)
            for k in range(16):
                piece = blocks[k // 4][:, 128 * (k % 4) : 128 * (k % 4) + 128].astype(F32)
                squares = squares + piece * piece
            target[at_rows, 384:] = squares

    def ow_wait(ahead):
        unit = ow.at[0, pl.ds(0, 64), :]
        copy = remote(unit, unit, od_send, od_recv.at[ahead], partner)
        if ahead:
            copy.wait_recv()
        else:
            pl.when(c == 0)(copy.wait_recv)

    project(1 - c, acc_send, 0)
    start(swap_part(0))
    ow_wait(0)
    oy_own(0, 0)
    oy_own(1, 0)
    mark("project2")
    project(c, acc_own, 0)
    mark("project3")
    project(1 - c, acc_send, 1)
    start(swap_part(1))
    mark("swap_wait")
    swap_part(0).wait_recv()

    low_lanes = iota((TOK, 128), 1) < 64

    def scaled(s):
        at_rows = pl.ds(s * TOK, TOK)
        both = acc_own[at_rows, 128:] + acc_recv[at_rows, 128:]
        mean = jnp.sum(both[:, 256:], axis=1, keepdims=True) * (1.0 / 4096.0)
        factor = lax.rsqrt(mean + 1e-06)
        return factor, (both[:, :256] * factor).astype(BF16).astype(F32)

    (factor0, p0), (factor1, p1) = scaled(0), scaled(1)

    mark("gating")
    project(c, acc_own, 1)
    swap_part(1).wait_recv()
    first, second = (
        ((acc_own[part, :128] + acc_recv[part, :128]) * factor).astype(BF16).astype(F32)
        for part, factor in ((pl.ds(0, TOK), factor0), (pl.ds(TOK, TOK), factor1))
    )
    left = jnp.where(low_lanes, first, roll64(second))
    right = jnp.where(low_lanes, roll64(first), second)
    ext[32:, :] = (left * sigmoid(right)).astype(BF16).astype(F32)
    start(
        remote(
            ext.at[pl.ds(TOK, 32), :], ext.at[pl.ds(0, 32), :], halo_send, halo_recv, up
        ),
        z < NZ - 1,
    )

    mark("decay")
    v0, v1 = p0[:, :128], p1[:, :128]
    gates = jnp.where(low_lanes, roll64(v0), v1)
    zero = jnp.zeros((TOK, 128), F32)
    v0 = jnp.where(low_lanes, v0, zero).astype(BF16)
    v1 = jnp.where(low_lanes, zero, roll64(v1)).astype(BF16)
    qt0, qt1 = p0[:, 128:].T, p1[:, 128:].T
    queries = jnp.concatenate([qt0[:32], qt1[:32]], axis=0) * (32.0 ** (-0.5))
    keys = jnp.concatenate([qt0[32:64], qt1[32:64]], axis=0)
    for s in range(2):
        local = jnp.logical_and(y_half == c, y_low == s)

        @pl.when(jnp.logical_not(local))
        def _():
            remote(exb.at[s], exb.at[s], ex_send.at[s], ex_recv.at[s], up).wait_recv()

    decays = []
    for s, qt in enumerate((qt0, qt1)):
        pre = (
            jnp.dot(
                dwt[rows(32 * y, 32), :][:, :64],
                qt[64:].astype(BF16),
                preferred_element_type=F32,
            )
            + bias[rows(32 * y, 32), :][:, :1]
        )
        log_sig = jnp.minimum(pre, 0.0) - jnp.log1p(jnp.exp(-jnp.abs(pre)))
        decays.append(log_sig * (1.0 / 16.0) + exb[s])
    decay = jnp.concatenate(decays, axis=0)
    part0 = decay.astype(BF16)
    rest = decay - part0.astype(F32)
    part1 = rest.astype(BF16)
    part2 = (rest - part1.astype(F32)).astype(BF16)
    parts = jnp.concatenate([part0, part1, part2], axis=0)

    def decay_sums(which):
        sums = jnp.dot(parts, mats[which], preferred_element_type=F32)
        return jnp.exp(sums[:64] + sums[64:128] + sums[128:])

    tail_keys = (keys * decay_sums(9)).astype(BF16)
    st_me[...] = (
        jnp.dot(tail_keys[:32], v0, preferred_element_type=F32)
        + jnp.dot(tail_keys[32:], v1, preferred_element_type=F32)
    ).astype(BF16)
    wide = jnp.concatenate([decay, jnp.zeros((64, TOK), F32)], axis=0)
    tot_me[...] = lax.dot_general(
        jnp.ones((8, TOK), F32), wide, NT, precision=HIGHEST, preferred_element_type=F32
    )[:1]

    def tell(n, carry):
        half = lax.div(n + 1, 2)
        k = jnp.where(lax.rem(n, 2) == 0, 8 - half, 8 + half)
        there = (lax.rem(z + k, NZ), y, t)
        remote(tot_me, tots.at[z], tot_send, tot_recv, there).start()
        remote(st_me, sts.at[z], st_send, st_recv, there).start()
        return carry

    lax.fori_loop(0, NZ - 1, tell, 0)

    ow_wait(1)
    oy_own(0, 1)
    ow_wait(3)
    oy_own(1, 3)
    mark("attention")
    queries_low, keys_low = queries.astype(BF16), keys.astype(BF16)
    for s in range(2):
        own = lax.dot_general(
            queries_low[32 * s : 32 * s + 32],
            keys_low[32 * s : 32 * s + 32],
            TN,
            preferred_element_type=F32,
        )
        scores[s] = jnp.where(xors[...] == 0, own, 0.0)
    lane_of = iota((64, TOK), 1)

    def level_scores(level, carry):
        factor = decay_sums(level)
        upper = jnp.bitwise_and(lax.shift_right_logical(lane_of, level), 1) == 1
        q_level = jnp.where(upper, queries * factor, 0.0).astype(BF16)
        k_level = jnp.where(upper, 0.0, keys * factor).astype(BF16)
        same = lax.shift_right_logical(xors[...], level + 1) == 0
        for s in range(2):
            pair = lax.dot_general(
                q_level[32 * s : 32 * s + 32],
                k_level[32 * s : 32 * s + 32],
                TN,
                preferred_element_type=F32,
            )
            scores[s] = scores[s] + jnp.where(same, pair, 0.0)
        return carry

    lax.fori_loop(0, 4, level_scores, 0)

    mark("halo_wait")
    @pl.when(z == 0)
    def _():
        ext[:32, :] = jnp.zeros((32, 128), F32)

    @pl.when(z > 0)
    def _():
        halo = ext.at[pl.ds(0, 32), :]
        remote(halo, halo, halo_send, halo_recv, up).wait_recv()

    mark("conv")
    conv = jnp.zeros((TOK, 128), F32)
    for tap in range(31):
        conv = conv + taps[tap : tap + 1, :] * ext[2 + tap : 2 + tap + TOK, :]
    lane8, row8 = iota((8, 128), 1), iota((8, 128), 0)
    seq_of = lax.div(lane8, 64)
    pick_sum = jnp.where(row8 == seq_of, 1.0, 0.0).astype(F32)
    pick_square = jnp.where(row8 == seq_of + 2, 1.0, 0.0).astype(F32)
    me = 4 * x + y
    stats[me] = lax.dot_general(
        pick_sum, conv, NT, precision=HIGHEST, preferred_element_type=F32
    ) + lax.dot_general(
        pick_square, conv * conv, NT, precision=HIGHEST, preferred_element_type=F32
    )

    def stat_copy(k):
        other = lax.rem(me + k, 16)
        xx = lax.div(other, 4)
        return remote(
            stats.at[me],
            stats.at[me],
            stat_send,
            stat_recv,
            at(xx, other - 4 * xx, z, c),
        )

    def send_stat(k, carry):
        stat_copy(k).start()
        return carry

    lax.fori_loop(1, 16, send_stat, 0)

    ow_wait(2)
    oy_own(0, 3)
    oy_own(1, 2)
    oy_own(0, 2)
    oy_own(1, 1)

    mark("attention2")
    lax.fori_loop(4, 8, level_scores, 0)
    heads = jnp.dot(scores[0].astype(BF16), v0, preferred_element_type=F32) + jnp.dot(
        scores[1].astype(BF16), v1, preferred_element_type=F32
    )
    q_start = (queries * decay_sums(8)).astype(BF16)

    mark("state_wait")
    others = tots.at[pl.ds(0, NZ - 1)]
    remote(others, others, tot_send, tot_recv, up).wait_recv()
    others = sts.at[pl.ds(0, NZ - 1)]
    remote(others, others, st_send, st_recv, up).wait_recv()
    mark("heads")
    row16 = iota((NZ, 128), 0)
    known = jnp.where(row16 < z, tots[:, 0, :], 0.0)
    from_row, to_row = iota((NZ, NZ), 0), iota((NZ, NZ), 1)
    between = jnp.where(
        jnp.logical_and(to_row > from_row, to_row < z), 1.0, 0.0
    ).astype(F32)
    exponent = jnp.dot(between, known, precision=HIGHEST, preferred_element_type=F32)
    reach = jnp.where(row16 < z, jnp.exp(exponent), 0.0)
    reach = jnp.concatenate([reach, jnp.zeros((128 - NZ, 128), F32)], axis=0).T
    low32 = iota((32, 128), 1) < 64
    entering = jnp.zeros((32, 128), F32)
    for k in range(NZ - 1):
        factor = jnp.where(low32, reach[:32, k : k + 1], reach[32:64, k : k + 1])
        state = jnp.where(z > k, sts[k].astype(F32), 0.0)
        entering = entering + factor * state
    heads = (
        heads
        + lax.dot_general(
            q_start[:32],
            jnp.where(low32, entering, 0.0).astype(BF16),
            TN,
            preferred_element_type=F32,
        )
        + lax.dot_general(
            q_start[32:],
            jnp.where(low32, 0.0, entering).astype(BF16),
            TN,
            preferred_element_type=F32,
        )
    )
    same_head = lax.div(iota((128, 128), 0), 64) == lax.div(iota((128, 128), 1), 64)
    mean_square = jnp.dot(
        heads * heads,
        jnp.where(same_head, 1.0 / 64.0, 0.0).astype(F32),
        precision=HIGHEST,
        preferred_element_type=F32,
    )
    gla_act = (
        heads * lax.rsqrt(mean_square + 1e-06) * hgain * (gates * sigmoid(gates))
    )

    mark("stat_wait")
    others = stats.at[pl.ds(0, 15)]
    remote(others, others, stat_send, stat_recv, up).wait_recv()
    mark("norm")
    total = stats[0]
    for k in range(1, 16):
        total = total + stats[k]
    average = lax.dot_general(
        total, pick_sum * (1.0 / 1024.0), TN, precision=HIGHEST, preferred_element_type=F32
    )
    spread = lax.dot_general(
        total, pick_square * (1.0 / 1024.0), TN, precision=HIGHEST, preferred_element_type=F32
    )
    variance = jnp.maximum(spread - average * average, 0.0)
    normed = (conv - average) * lax.rsqrt(variance + 1e-05) * cgain
    conv_act = normed * sigmoid(normed)

    mark("act_send")
    act_me[0] = jnp.where(low_lanes, conv_act, roll64(gla_act)).astype(BF16)
    act_me[1] = jnp.where(low_lanes, roll64(conv_act), gla_act).astype(BF16)
    def act_cols(j):
        return pl.ds(pl.multiple_of(x * 256 + j * 128, 128), 128)

    for s in range(2):
        mine = (2 * c + s == y) & (y_half == c)
        copy = remote(
            act_me.at[s],
            acts.at[:, act_cols(y_low)],
            act_send,
            act_recv.at[y_low],
            at(x, 2 * c + s, z, y_half),
        )
        pl.when(jnp.logical_not(mine))(copy.start)

        @pl.when(mine)
        def _():
            acts[:, act_cols(y_low)] = act_me[s]

    mark("act_pass")
    oy_pass(0, 0)
    oy_pass(1, 3)
    oy_pass(0, 1)
    oy_pass(1, 2)
    for n, j in enumerate((y_low, 1 - y_low)):
        block = acts.at[:, act_cols(j)]
        arrived = remote(block, block, act_send, act_recv.at[j], partner)
        if n == 0:
            pl.when(y_half != c)(arrived.wait_recv)
        else:
            arrived.wait_recv()
        for step in (2, 1, 3):
            there = at(lax.rem(x + step, 4), y, z, c)
            remote(block, block, act2_send, act2_recv, there).start()

    mark("oy_rest")
    for ahead in (3, 2):
        oy_wait(0, ahead, y_down)
    for ahead in (0, 1):
        oy_wait(1, ahead, y_up)
    for ahead in (0, 3, 1, 2):
        oy_wait(2, ahead, y_far)
    mark("act_wait")
    others = acts.at[:, pl.ds(0, 768)]
    remote(others, others, act2_send, act2_recv, partner).wait_recv()
    mark("output")
    def output(half):
        whole = lax.dot_general(acts[...], ow[half], NT, preferred_element_type=F32)
        parts = [whole[:, 128 * yy : 128 * yy + 128] for yy in range(4)]
        tiles = []
        for kk in range(2):
            for even, odd in ((parts[0], parts[1]), (parts[2], parts[3])):
                if kk == 0:
                    tiles.append(jnp.where(low_lanes, even, roll64(odd)))
                else:
                    tiles.append(jnp.where(low_lanes, roll64(even), odd))
        return jnp.concatenate(tiles, axis=1)

    po_send[...] = output(1 - c).astype(BF16)
    trade = remote(po_send, po_recv, d2d_send.at[2], d2d_recv.at[2], partner)
    start(trade)
    residual = xg[rows(y * TOK, TOK), feature_cols(x, c)]
    result = residual.astype(F32) + output(c)
    mark("trade_wait")
    trade.wait_recv()
    out[...] = (result + po_recv[...].astype(F32)).astype(BF16)

    mark("drain")
    for copy, cond in finish:
        if cond is None:
            copy.wait_send()
        else:
            pl.when(cond)(copy.wait_send)

    def left(piece, semaphore, cond=None):
        copy = remote(piece, piece, semaphore, stat_recv, partner)
        if cond is None:
            copy.wait_send()
        else:
            pl.when(cond)(copy.wait_send)

    left(stats.at[pl.ds(0, 15)], stat_send)
    left(tots.at[pl.ds(0, NZ - 1)], tot_send)
    left(sts.at[pl.ds(0, NZ - 1)], st_send)
    left(xg.at[pl.ds(0, 192), :], oy_send)
    left(acts.at[:, pl.ds(0, 128)], act_send, y_half == c)
    left(acts.at[:, pl.ds(0, 256)], act_send, y_half != c)
    left(acts.at[:, pl.ds(0, 768)], act2_send)
    left(xg.at[pl.ds(0, 832), :], x_send, c == 0)
    left(xg.at[pl.ds(0, 128), :], x_send, c == 1)
    left(xg.at[pl.ds(0, 480), :], xd_send, c == 0)
    left(owsrc, own_send, c == 0)
    left(w.at[pl.ds(0, 3840), :], wz_send, c == 1)
    left(w.at[pl.ds(0, 2048), :], wd_send, c == 1)
    left(ow.at[0, pl.ds(0, 448), :], od_send, c == 1)
    left(owz.at[pl.ds(0, 15)], oz_send, c == 1)
    mark(None)


def shards(
    inputs,
    norm_gain,
    conv_in_a,
    conv_in_b,
    query_w,
    key_w,
    value_w,
    out_gate_w,
    pointwise_w,
    gla_out_w,
    forget_first_factor,
    decay_w,
    decay_bias,
    decay_extra,
    conv_kernel,
    conv_gain,
    head_gain,
):
    dma = pltpu.SemaphoreType.DMA
    vmem = pltpu.VMEM
    mixed = pl.pallas_call(
        body,
        out_shape=jax.ShapeDtypeStruct((TOK, 512), BF16),
        in_specs=[pl.BlockSpec(memory_space=pltpu.HBM)] * 17,
        out_specs=pl.BlockSpec(memory_space=vmem),
        scratch_shapes=[
            vmem((32, 128), F32),
            vmem((6, 64, 128), BF16),
            vmem((2, 64, 64), BF16),
            vmem((64, 128), BF16),
            vmem((64, 128), BF16),
            vmem((4, 128), F32),
            vmem((2, 32, TOK), F32),
            vmem((31, 128), F32),
            vmem((8, 128), F32),
            vmem((1, 64), F32),
            vmem((2, 64, 384), BF16),
            vmem((64, 256), BF16),
            vmem((128, 128), BF16),
            vmem((128, 128), F32),
            vmem((32, 128), F32),
            dma((17,)),
            vmem((4 * TOK, 4096), BF16),
            vmem((4096, 384), BF16),
            vmem((2, 512, 1024), BF16),
            vmem((NZ, 2, 64, 256), BF16),
            vmem((512, 512), F32),
            vmem((512, 512), F32),
            vmem((512, 512), F32),
            vmem((10, TOK, TOK), BF16),
            vmem((TOK, TOK), jnp.int32),
            vmem((2, TOK, TOK), F32),
            vmem((TOK + 32, 128), F32),
            vmem((2, 32, TOK), F32),
            vmem((16, 8, TOK), F32),
            vmem((1, 128), F32),
            vmem((NZ, 1, 128), F32),
            vmem((32, 128), BF16),
            vmem((NZ, 32, 128), BF16),
            vmem((2, TOK, 128), BF16),
            vmem((TOK, 1024), BF16),
            vmem((TOK, 512), BF16),
            vmem((TOK, 512), BF16),
            dma,
            dma,
            dma,
            dma,
            dma((64,)),
            dma((2,)),
            dma((4,)),
            dma,
            dma,
            dma,
            dma,
            dma,
            dma((NZ,)),
            dma,
            dma((4,)),
            dma,
            dma((3, 4)),
            dma((2,)),
            dma((2,)),
            dma((3,)),
            dma((3,)),
            dma,
            dma,
            dma,
            dma,
            dma,
            dma,
            dma,
            dma,
            dma,
            dma((2,)),
            dma,
            dma,
        ],
        compiler_params=pltpu.CompilerParams(
            collective_id=0, has_side_effects=True
        ),
        name="mixer",
    )(
        inputs[0],
        norm_gain.reshape(32, 128),
        conv_in_a,
        conv_in_b,
        query_w,
        key_w,
        value_w,
        out_gate_w,
        pointwise_w,
        gla_out_w,
        forget_first_factor.T,
        decay_w,
        decay_bias.reshape(4, 128),
        decay_extra[0].T.reshape(2, 32, TOK),
        conv_kernel,
        conv_gain.reshape(8, 128),
        head_gain.reshape(1, 64),
    )
    return mixed[None]


def solution(mesh):
    weights = P(("sp", "fs"), "tp")
    return jax.shard_map(
        shards,
        mesh=mesh,
        in_specs=(
            P("fs", "sp", "tp"),
            P(),
            weights,
            weights,
            weights,
            weights,
            weights,
            weights,
            weights,
            weights,
            P(),
            P(),
            P(),
            P("fs", "sp", "tp"),
            P(),
            P(),
            P(),
        ),
        out_specs=P("fs", "sp", "tp"),
        check_vma=False,
    )
```

```python
import functools
import heapq

import jax
import jax.numpy as jnp
from jax import lax
from jax.experimental import pallas as pl
from jax.experimental.pallas import tpu as pltpu
from jax.sharding import PartitionSpec as P

MESH = pl.DeviceIdType.MESH
F32 = jnp.float32
BF16 = jnp.bfloat16
HIGHEST = lax.Precision.HIGHEST
NZ = 16
TOK = 256
NT = (((1,), (1,)), ((), ()))
TN = (((0,), (0,)), ((), ()))


def remote(src, dst, send, recv, device):
    return pltpu.make_async_remote_copy(
        src_ref=src,
        dst_ref=dst,
        send_sem=send,
        recv_sem=recv,
        device_id=device,
        device_id_type=MESH,
    )


def wrap(value, size):
    return lax.rem(value + size, size)


def rows(start, size):
    return pl.ds(pl.multiple_of(start, size), size)


def iota(shape, dim):
    return lax.broadcasted_iota(jnp.int32, shape, dim)


def sigmoid(value):
    return 1.0 / (1.0 + jnp.exp(-value))


def thirds(value):
    first = value.astype(BF16)
    rest = value - first.astype(F32)
    second = rest.astype(BF16)
    return first, second, (rest - second.astype(F32)).astype(BF16)


def roll64(value):
    return pltpu.roll(value, 64, 1)


OFFSETS = (0, -1, 1, 2)
UNIT = (64, 64)
W_HOP, W_PART = 2.7, 0.55


def x_forwards(f, g, u):
    sends = []
    if g == 0:
        if f == 0:
            sends += [(0, 0, 1, 0), (0, 1, 2, 0)]
        elif f < 3 and u == f - 1:
            sends += [(0, u, 3, 0)]
        sends += [(1, 0, f, 1), (1, 1, f, 2)]
    elif g < 3 and u == g - 1:
        sends += [(1, u, f, 3)]
    return sends


def x_order():
    free, queue, done = {}, [], []

    def go(now, half, f, g, u):
        for which, way, ff, gg in x_forwards(f, g, u):
            link = ((which + half) % 2, way)
            free[link] = max(free.get(link, 0.0), now) + 1.41 * UNIT[half] / 64
            heapq.heappush(queue, (free[link] + 2.5, half, ff, gg, u))

    for u in range(2):
        for half in range(2):
            go(0.0, half, 0, 0, u)
    while queue:
        event = heapq.heappop(queue)
        done.append(event)
        go(*event)
    return done


def body(
    xin_hbm,
    gain_hbm,
    a_hbm,
    b_hbm,
    q_hbm,
    k_hbm,
    v_hbm,
    gate_hbm,
    point_hbm,
    gla_hbm,
    low_hbm,
    dw_hbm,
    bias_hbm,
    extra_hbm,
    kernel_hbm,
    cgain_hbm,
    hgain_hbm,
    out,
    gain_in,
    tiles_in,
    narrow_in,
    low_in,
    dw_in,
    bias_in,
    exsrc,
    taps_in,
    cgain_in,
    hgain_in,
    wsrc,
    owsrc,
    dwt,
    bias,
    taps,
    in_sem,
    xg,
    w,
    ow,
    owz,
    acc_own,
    acc_send,
    acc_recv,
    mats,
    xors,
    scores,
    ext,
    exb,
    stats,
    tot_me,
    tots,
    st_me,
    sts,
    act_me,
    acts,
    po_send,
    po_recv,
    x_send,
    xd_send,
    xd_recv,
    own_send,
    ring_recv,
    wy_send,
    wy_recv,
    wz_send,
    wd_send,
    wd_recv,
    ox_recv,
    oz_send,
    oz_recv,
    od_send,
    od_recv,
    oy_send,
    oy_recv,
    ex_send,
    ex_recv,
    d2d_send,
    d2d_recv,
    halo_send,
    halo_recv,
    stat_send,
    stat_recv,
    tot_send,
    tot_recv,
    st_send,
    st_recv,
    act_send,
    act_recv,
    act2_send,
    act2_recv,
):
    scope = []

    def mark(name):
        if scope:
            scope.pop().__exit__(None, None, None)
        if name:
            scope.append(jax.named_scope(name))
            scope[0].__enter__()

    z = lax.axis_index("sp")
    y = lax.axis_index("fs")
    t = lax.axis_index("tp")
    x = lax.div(t, 2)
    c = t - 2 * x
    y_half = lax.div(y, 2)
    y_low = y - 2 * y_half
    z_class = lax.rem(lax.div(z, 2), 2)
    partner = (z, y, 2 * x + 1 - c)

    def at(xx, yy, zz, cc):
        return (zz, yy, 2 * xx + cc)

    mark("greet")
    barrier = pltpu.get_barrier_semaphore()

    def greet(zz, yy, tt):
        pl.semaphore_signal(barrier, inc=1, device_id=(zz, yy, tt), device_id_type=MESH)

    for step in (1, NZ - 1):
        greet(lax.rem(z + step, NZ), y, t)
    for step in range(1, 8):
        greet(z, y, lax.rem(t + step, 8))
    for step in range(1, 4):
        for cc in range(2):
            greet(z, lax.rem(y + step, 4), 2 * x + cc)

    group_pair = 2 * x + y_half

    def tile_of(index):
        return pl.ds(pl.multiple_of(index * 128, 128), 128)

    def feature_cols(xx, cc):
        return pl.ds(pl.multiple_of((2 * xx + cc) * 512, 512), 512)

    fetches = [
        pltpu.make_async_copy(source, target, in_sem.at[k])
        for k, (source, target) in enumerate(
            (
                (a_hbm, tiles_in.at[0]),
                (b_hbm, tiles_in.at[1]),
                (v_hbm, tiles_in.at[2]),
                (gate_hbm, tiles_in.at[3]),
                (point_hbm, tiles_in.at[4]),
                (gla_hbm, tiles_in.at[5]),
                (q_hbm, narrow_in.at[0]),
                (k_hbm, narrow_in.at[1]),
                (gain_hbm, gain_in),
                (low_hbm.at[:, tile_of(2 * z + y_half)], low_in),
                (xin_hbm, xg.at[rows(y * TOK, TOK), feature_cols(x, c)]),
                (extra_hbm, exsrc),
                (dw_hbm.at[:, tile_of(x)], dw_in),
                (bias_hbm, bias_in),
                (kernel_hbm.at[:, tile_of(group_pair)], taps_in),
                (cgain_hbm, cgain_in),
                (hgain_hbm, hgain_in),
            )
        )
    ]
    for fetch in fetches:
        fetch.start()

    mark("pack")
    low64 = iota((64, 128), 1) < 64
    lane64 = iota((64, 128), 1)
    y_even = y_low == 0

    def column(row_vector):
        return jnp.broadcast_to(row_vector, (128, 128)).T

    for fetch in fetches[:10]:
        fetch.wait()
    gain_all = column(gain_in[pl.ds(2 * z + y_half, 1), :])
    gain = jnp.where(y_even, gain_all[:64], gain_all[64:])

    def pair(k, scale):
        first = tiles_in[k].astype(F32) * scale
        second = tiles_in[k + 1].astype(F32) * scale
        return (
            jnp.where(low64, first, roll64(second)).astype(BF16),
            jnp.where(low64, roll64(first), second).astype(BF16),
        )

    for k in range(2):
        both = pair(2 * k, gain)
        for j in range(2):
            wsrc[j, :, 128 * k : 128 * k + 128] = both[j]
    both = pair(4, 1.0)
    for j in range(2):
        owsrc[:, 128 * j : 128 * j + 128] = both[j]
    narrow = jnp.concatenate([narrow_in[0], narrow_in[1]], axis=1).astype(F32)
    low_rows = low_in[...].astype(F32)
    low_rows = jnp.concatenate([low_rows, low_rows], axis=0).T
    low_rows = jnp.where(y_even, low_rows[:64], low_rows[64:])
    back32, back64 = pltpu.roll(narrow, 96, 1), roll64(narrow)
    mixed0 = jnp.where(low64, jnp.where(lane64 < 32, narrow, back32), low_rows)
    mixed1 = jnp.where(low64, jnp.where(lane64 < 32, back32, back64), low_rows)
    wsrc[0, :, 256:] = (mixed0 * gain).astype(BF16)
    wsrc[1, :, 256:] = (mixed1 * gain).astype(BF16)
    for fetch in fetches[10:12]:
        fetch.wait()
    mark("barrier_wait")
    pl.semaphore_wait(barrier, 2 + 7 + 6)

    finish = []

    def start(copy, cond=None):
        if cond is None:
            copy.start()
        else:
            pl.when(cond)(copy.start)
        finish.append((copy, cond))

    mark("first_sends")
    def w_at(zz, k):
        kind = lax.rem(lax.div(zz, 2), 2)
        begin = kind * 2048 + lax.div(zz, 4) * 512 + lax.rem(zz, 2) * 256 + k * 64
        return w.at[rows(begin, 64), :]

    for j in range(2):
        mine = jnp.logical_and(2 * c + j == y, c == 1)
        start(
            remote(
                wsrc.at[j], w_at(z, y), wy_send.at[j], wy_recv.at[y], at(x, 2 * c + j, z, 1)
            ),
            jnp.logical_not(mine),
        )

        @pl.when(mine)
        def _():
            w_at(z, y)[...] = wsrc[j]

    x_up, x_down = wrap(x + 1, 4), wrap(x - 1, 4)
    y_up, y_down = wrap(y + 1, 4), wrap(y - 1, 4)
    z_up, z_down = wrap(z + 1, NZ), wrap(z - 1, NZ)
    along_x = (at(x_up, y, z, 0), at(x_down, y, z, 0))
    along_y = (at(x, y_up, z, 0), at(x, y_down, z, 0))

    def x_rows(yy, half, u):
        begin = yy * TOK + 2 * UNIT[0] * half + UNIT[half] * u
        return pl.ds(pl.multiple_of(begin, 16), UNIT[half])

    def x_event(half, f, g, u):
        df, dg = OFFSETS[f], OFFSETS[g]
        xx, yy = (x + df, y + dg) if half == 0 else (x + dg, y + df)
        xx, yy = wrap(xx, 4), wrap(yy, 4)
        place = xg.at[
            x_rows(yy, half, u), pl.ds(pl.multiple_of(xx * 1024, 1024), 1024)
        ]
        others = xg.at[x_rows(yy, half, u), feature_cols(xx, 1)]
        slot = 32 * half + 8 * f + 2 * g + u
        if f == 0 and g == 0:
            place = xg.at[x_rows(yy, half, u), feature_cols(xx, c)]
        else:
            remote(place, place, x_send, ring_recv.at[slot], partner).wait_recv()
        first, second = (along_x, along_y) if half == 0 else (along_y, along_x)
        for which, way, ff, gg in x_forwards(f, g, u):
            remote(
                place,
                place,
                x_send,
                ring_recv.at[32 * half + 8 * ff + 2 * gg + u],
                (second if which else first)[way],
            ).start()
        if f or g:
            remote(others, others, xd_send, xd_recv, partner).start()

    for u in range(2):
        for half in range(2):
            x_event(half, 0, 0, u)

    @pl.when(c == 0)
    def _():
        remote(owsrc, owz.at[z, 0], own_send, ox_recv, partner).start()

    @pl.when(c == 1)
    def _():
        owz[z, 1] = owsrc[...]

    for j in range(2):
        mine = jnp.logical_and(2 * c + j == y, y_half == c)
        start(
            remote(
                exsrc.at[j],
                exb.at[y_low],
                ex_send.at[j],
                ex_recv.at[y_low],
                at(x, 2 * c + j, z, y_half),
            ),
            jnp.logical_not(mine),
        )

        @pl.when(mine)
        def _():
            exb[y_low] = exsrc[j]

    up, down = (z_up, y, t), (z_down, y, t)

    ways = (up, down)

    def w_on(way, d, k, origin):
        here = w_at(origin, k)
        if d < 8 - way:
            remote(here, here, wz_send, ring_recv.at[4 * origin + k], ways[way]).start()
        if d == 0 and way == 0:
            return

        @pl.when(lax.rem(lax.div(origin, 2), 2) == 0)
        def _():
            remote(here, here, wd_send, wd_recv, partner).start()

    def w_start(k):
        here = w_at(z, k)

        @pl.when(jnp.logical_not(jnp.logical_and(y == k, y_half == 1)))
        def _():
            remote(here, here, wz_send, wy_recv.at[k], up).wait_recv()

        w_on(0, 0, k, z)
        w_on(1, 0, k, z)

    def w_event(way, d, k):
        origin = wrap(z - d if way == 0 else z + d, NZ)
        here = w_at(origin, k)
        remote(here, here, wz_send, ring_recv.at[4 * origin + k], up).wait_recv()
        w_on(way, d, k, origin)

    def ow_cols(xx):
        return pl.ds(pl.multiple_of(xx * 256, 256), 256)

    def ow_at(zz):
        k = lax.rem(zz, 4)
        half = lax.div(k, 2)
        return ow.at[half, rows(y * 128 + (k - 2 * half) * 64, 64), ow_cols(x)]

    def ow_on(way, d, origin):
        here = owz.at[origin]
        if d < 8 - way:
            remote(here, here, oz_send, oz_recv.at[origin], ways[way]).start()

    def ow_give(n, carry):
        turn = lax.div(n, 4)
        ahead = jnp.where(turn == 2, 3, jnp.where(turn == 3, 2, turn))
        column = lax.rem(x + ahead, 4)
        origin = 4 * column + lax.rem(n, 4)
        behind = lax.rem(4 - ahead, 4)
        place = ow_at(origin)

        def give(cc):
            remote(
                owz.at[origin, cc], place, od_send, od_recv.at[behind], at(column, y, z, cc)
            ).start()

        give(0)
        pl.when(column != x)(functools.partial(give, 1))

        @pl.when(column == x)
        def _():
            place[...] = owz[origin, 1]

        return carry

    def ow_start():
        remote(owz.at[z, 0], owz.at[z, 0], oz_send, ox_recv, partner).wait_recv()
        ow_on(0, 0, z)
        ow_on(1, 0, z)

    def ow_event(way, d, k):
        origin = wrap(z - d if way == 0 else z + d, NZ)
        here = owz.at[origin]
        remote(here, here, oz_send, oz_recv.at[origin], up).wait_recv()
        ow_on(way, d, origin)

    mark("params")
    for fetch in fetches[12:]:
        fetch.wait()
    dw_all = dw_in[...].astype(F32)
    dw_all = jnp.concatenate([dw_all, dw_all], axis=0).T
    dwt[...] = dw_all.astype(BF16)
    bias[...] = column(bias_in[pl.ds(x, 1), :])
    low31 = iota((31, 128), 1) < 64
    tap_rows = taps_in[...]
    tap_back = roll64(tap_rows)
    taps[:31, :] = jnp.where(low31 == y_even, tap_rows, tap_back)
    cgain_row = cgain_in[pl.ds(group_pair, 1), :]
    cgain = jnp.where(low31[:1] == y_even, cgain_row, roll64(cgain_row))
    hgain = jnp.concatenate([hgain_in[...], hgain_in[...]], axis=1)

    mark("constants")
    lane = iota((TOK, TOK), 1)
    row = iota((TOK, TOK), 0)
    xors[...] = jnp.bitwise_xor(row, lane)
    one = jnp.ones((TOK, TOK), F32)
    nil = jnp.zeros((TOK, TOK), F32)

    def level_matrix(level, carry):
        half = lax.shift_left(jnp.int32(1), level)
        base = lane - jnp.bitwise_and(lane, 2 * half - 1)
        middle = base + half - 1
        low = jnp.minimum(lane, middle)
        high = jnp.maximum(lane, middle)
        mats[level] = jnp.where(
            jnp.logical_and(row > low, row <= high), one, nil
        ).astype(BF16)
        return carry

    lax.fori_loop(0, 8, level_matrix, 0)
    mats[8] = jnp.where(row <= lane, one, nil).astype(BF16)
    mats[9] = jnp.where(row > lane, one, nil).astype(BF16)

    z_agenda = []
    for way in range(2):
        for d in range(1, 9 - way):
            for k in range(5):
                call = ow_event if k == 4 else w_event
                z_agenda.append((W_HOP * d + W_PART * k, call, (way, d, k)))
    z_agenda.sort(key=lambda entry: entry[0])
    mark("gather")

    @pl.when(c == 0)
    def _():
        for n, (_, *event) in enumerate(x_order()):
            if n % 15 == 0:
                mark(f"x{n}")
            x_event(*event)
        mark("w_arrive")
        everything = w.at[pl.ds(0, 2048), :]
        remote(everything, everything, wd_send, wd_recv, partner).wait_recv()
        mark(None)

    @pl.when(c == 1)
    def _():
        for k in range(4):
            w_start(k)
        ow_start()
        for n, (_, call, event) in enumerate(z_agenda):
            if n % 24 == 0:
                mark(f"z{n}")
            call(*event)
        lax.fori_loop(0, 16, ow_give, 0)
        mark("x_arrive")
        everything = xg.at[pl.ds(0, 480), :]
        remote(everything, everything, xd_send, xd_recv, partner).wait_recv()
        mark(None)

    y_next = (at(x, y_up, z, c), at(x, y_down, z, c))
    y_from = (y_down, y_up)
    y_far = wrap(y + 2, 4)

    def oy_at(yy, ahead):
        return ow.at[:, rows(yy * 128, 128), ow_cols(lax.rem(x + ahead, 4))]

    def oy_own(way, ahead):
        here = oy_at(y, ahead)
        remote(here, here, oy_send, oy_recv.at[way, ahead], y_next[way]).start()

    def oy_wait(way, ahead, yy):
        here = oy_at(yy, ahead)
        remote(here, here, oy_send, oy_recv.at[way, ahead], partner).wait_recv()

    def oy_pass(way, ahead):
        oy_wait(way, ahead, y_from[way])
        here = oy_at(y_from[way], ahead)
        remote(here, here, oy_send, oy_recv.at[2, ahead], y_next[way]).start()

    mark("project")
    def swap_part(n):
        part = pl.ds(128, 384) if n == 0 else pl.ds(0, 128)
        return remote(
            acc_send.at[:, part], acc_recv.at[:, part], d2d_send.at[n], d2d_recv.at[n], partner
        )

    def project(half, target, n):
        begin, size = (128, 256) if n == 0 else (0, 128)
        for s in range(2):
            at_rows = pl.ds(s * TOK, TOK)
            blocks = [
                xg[rows((2 * half + s) * TOK, TOK), feature_cols(k, c)] for k in range(4)
            ]
            total = jnp.zeros((TOK, size), F32)
            for k in range(4):
                total = total + jnp.dot(
                    blocks[k],
                    w[rows(c * 2048 + 512 * k, 512), begin : begin + size],
                    preferred_element_type=F32,
                )
            target[at_rows, begin : begin + size] = total.astype(target.dtype)
            if n:
                continue
            squares = jnp.zeros((TOK, 128), F32)
            for k in range(16):
                piece = blocks[k // 4][:, 128 * (k % 4) : 128 * (k % 4) + 128].astype(F32)
                squares = squares + piece * piece
            target[at_rows, 384:] = squares.astype(target.dtype)

    def ow_wait(ahead):
        unit = ow.at[0, pl.ds(0, 64), :]
        copy = remote(unit, unit, od_send, od_recv.at[ahead], partner)
        if ahead:
            copy.wait_recv()
        else:
            pl.when(c == 0)(copy.wait_recv)

    project(1 - c, acc_send, 0)
    start(swap_part(0))
    ow_wait(0)
    oy_own(0, 0)
    oy_own(1, 0)
    mark("project2")
    project(c, acc_own, 0)
    mark("project3")
    project(1 - c, acc_send, 1)
    start(swap_part(1))
    mark("swap_wait")
    swap_part(0).wait_recv()

    low_lanes = iota((TOK, 128), 1) < 64

    def scaled(s):
        at_rows = pl.ds(s * TOK, TOK)
        both = acc_own[at_rows, 128:] + acc_recv[at_rows, 128:].astype(F32)
        mean = jnp.sum(both[:, 256:], axis=1, keepdims=True) * (1.0 / 4096.0)
        factor = lax.rsqrt(mean + 1e-06)
        return factor, (both[:, :256] * factor).astype(BF16).astype(F32)

    (factor0, p0), (factor1, p1) = scaled(0), scaled(1)

    mark("gating")
    project(c, acc_own, 1)
    swap_part(1).wait_recv()
    first, second = (
        ((acc_own[part, :128] + acc_recv[part, :128].astype(F32)) * factor).astype(BF16).astype(F32)
        for part, factor in ((pl.ds(0, TOK), factor0), (pl.ds(TOK, TOK), factor1))
    )
    left = jnp.where(low_lanes, first, roll64(second))
    right = jnp.where(low_lanes, roll64(first), second)
    ext[32:, :] = (left * sigmoid(right)).astype(BF16).astype(F32)
    start(
        remote(
            ext.at[pl.ds(TOK, 32), :], ext.at[pl.ds(0, 32), :], halo_send, halo_recv, up
        ),
        z < NZ - 1,
    )
    mark("decay")
    v0, v1 = p0[:, :128], p1[:, :128]
    gates = jnp.where(low_lanes, roll64(v0), v1)
    zero = jnp.zeros((TOK, 128), F32)
    v0 = jnp.where(low_lanes, v0, zero).astype(BF16)
    v1 = jnp.where(low_lanes, zero, roll64(v1)).astype(BF16)
    qt0, qt1 = p0[:, 128:].T, p1[:, 128:].T
    queries = jnp.concatenate([qt0[:32], qt1[:32]], axis=0) * (32.0 ** (-0.5))
    keys = jnp.concatenate([qt0[32:64], qt1[32:64]], axis=0)
    for s in range(2):
        local = jnp.logical_and(y_half == c, y_low == s)

        @pl.when(jnp.logical_not(local))
        def _():
            remote(exb.at[s], exb.at[s], ex_send.at[s], ex_recv.at[s], up).wait_recv()

    decays = []
    for s, qt in enumerate((qt0, qt1)):
        pre = (
            jnp.dot(
                dwt[rows(32 * y, 32), :][:, :64],
                qt[64:].astype(BF16),
                preferred_element_type=F32,
            )
            + bias[rows(32 * y, 32), :][:, :1]
        )
        log_sig = jnp.minimum(pre, 0.0) - jnp.log1p(jnp.exp(-jnp.abs(pre)))
        decays.append(log_sig * (1.0 / 16.0) + exb[s])
    decay = jnp.concatenate(decays, axis=0)
    parts = jnp.concatenate(thirds(decay), axis=0)

    def decay_sums(which):
        sums = jnp.dot(parts, mats[which], preferred_element_type=F32)
        return jnp.exp(sums[:64] + sums[64:128] + sums[128:])

    tail_keys = (keys * decay_sums(9)).astype(BF16)
    st_me[...] = (
        jnp.dot(tail_keys[:32], v0, preferred_element_type=F32)
        + jnp.dot(tail_keys[32:], v1, preferred_element_type=F32)
    ).astype(BF16)
    wide = jnp.concatenate([decay, jnp.zeros((64, TOK), F32)], axis=0)
    tot_me[...] = lax.dot_general(
        jnp.ones((8, TOK), F32), wide, NT, precision=HIGHEST, preferred_element_type=F32
    )[:1]

    def tell(n, carry):
        half = lax.div(n + 1, 2)
        k = jnp.where(lax.rem(n, 2) == 0, 8 - half, 8 + half)
        there = (lax.rem(z + k, NZ), y, t)
        remote(tot_me, tots.at[z], tot_send, tot_recv, there).start()
        remote(st_me, sts.at[z], st_send, st_recv, there).start()
        return carry

    lax.fori_loop(0, NZ - 1, tell, 0)

    ow_wait(1)
    oy_own(0, 1)
    oy_own(1, 1)
    mark("halo_wait")
    @pl.when(z == 0)
    def _():
        ext[:32, :] = jnp.zeros((32, 128), F32)

    @pl.when(z > 0)
    def _():
        halo = ext.at[pl.ds(0, 32), :]
        remote(halo, halo, halo_send, halo_recv, up).wait_recv()

    mark("conv")
    conv = jnp.zeros((TOK, 128), F32)
    for tap in range(31):
        conv = conv + taps[tap : tap + 1, :] * ext[2 + tap : 2 + tap + TOK, :]
    lane8, row8 = iota((8, 128), 1), iota((8, 128), 0)
    seq_of = lax.div(lane8, 64)
    pick_sum = jnp.where(row8 == seq_of, 1.0, 0.0).astype(BF16)
    pick_square = jnp.where(row8 == seq_of + 2, 1.0, 0.0).astype(BF16)
    me = 4 * x + y
    stats[me] = lax.dot_general(
        jnp.concatenate([pick_sum] * 3 + [pick_square] * 3, axis=1),
        jnp.concatenate([*thirds(conv), *thirds(conv * conv)], axis=1),
        NT,
        preferred_element_type=F32,
    )

    def stat_copy(k):
        other = lax.rem(me + k, 16)
        xx = lax.div(other, 4)
        return remote(
            stats.at[me],
            stats.at[me],
            stat_send,
            stat_recv,
            at(xx, other - 4 * xx, z, c),
        )

    def send_stat(k, carry):
        stat_copy(k).start()
        return carry

    lax.fori_loop(1, 16, send_stat, 0)

    ow_wait(3)
    oy_own(0, 3)
    oy_own(1, 3)

    mark("attention")
    queries_low, keys_low = queries.astype(BF16), keys.astype(BF16)
    for s in range(2):
        own = lax.dot_general(
            queries_low[32 * s : 32 * s + 32],
            keys_low[32 * s : 32 * s + 32],
            TN,
            preferred_element_type=F32,
        )
        scores[s] = jnp.where(xors[...] == 0, own, 0.0)
    lane_of = iota((64, TOK), 1)

    def level_scores(level, carry):
        factor = decay_sums(level)
        upper = jnp.bitwise_and(lax.shift_right_logical(lane_of, level), 1) == 1
        q_level = jnp.where(upper, queries * factor, 0.0).astype(BF16)
        k_level = jnp.where(upper, 0.0, keys * factor).astype(BF16)
        same = lax.shift_right_logical(xors[...], level + 1) == 0
        for s in range(2):
            pair = lax.dot_general(
                q_level[32 * s : 32 * s + 32],
                k_level[32 * s : 32 * s + 32],
                TN,
                preferred_element_type=F32,
            )
            scores[s] = scores[s] + jnp.where(same, pair, 0.0)
        return carry

    lax.fori_loop(0, 4, level_scores, 0)

    ow_wait(2)
    oy_own(0, 2)
    oy_own(1, 2)
    mark("attention2")
    lax.fori_loop(4, 8, level_scores, 0)
    heads = jnp.dot(scores[0].astype(BF16), v0, preferred_element_type=F32) + jnp.dot(
        scores[1].astype(BF16), v1, preferred_element_type=F32
    )
    q_start = (queries * decay_sums(8)).astype(BF16)

    mark("stat_wait")
    others = stats.at[pl.ds(0, 15)]
    remote(others, others, stat_send, stat_recv, up).wait_recv()
    mark("norm")
    total = stats[0]
    for k in range(1, 16):
        total = total + stats[k]
    picks = jnp.concatenate([pick_sum, pick_square], axis=1)
    moments = lax.dot_general(
        jnp.concatenate(thirds(total), axis=0),
        jnp.concatenate([picks] * 3, axis=0),
        TN,
        preferred_element_type=F32,
    ) * (1.0 / 1024.0)
    average, spread = moments[:, :128], moments[:, 128:]
    variance = jnp.maximum(spread - average * average, 0.0)
    normed = (conv - average) * lax.rsqrt(variance + 1e-05) * cgain
    conv_act = normed * sigmoid(normed)

    mark("state_wait")
    others = tots.at[pl.ds(0, NZ - 1)]
    remote(others, others, tot_send, tot_recv, up).wait_recv()
    others = sts.at[pl.ds(0, NZ - 1)]
    remote(others, others, st_send, st_recv, up).wait_recv()
    mark("heads")
    row16 = iota((NZ, 128), 0)
    known = jnp.where(row16 < z, tots[:, 0, :], 0.0)
    from_row, to_row = iota((NZ, NZ), 0), iota((NZ, NZ), 1)
    between = jnp.where(
        jnp.logical_and(to_row > from_row, to_row < z), 1.0, 0.0
    ).astype(F32)
    exponent = jnp.dot(between, known, precision=HIGHEST, preferred_element_type=F32)
    reach = jnp.where(row16 < z, jnp.exp(exponent), 0.0)
    reach = jnp.concatenate([reach, jnp.zeros((128 - NZ, 128), F32)], axis=0).T
    low32 = iota((32, 128), 1) < 64
    entering = jnp.zeros((32, 128), F32)
    for k in range(NZ - 1):
        factor = jnp.where(low32, reach[:32, k : k + 1], reach[32:64, k : k + 1])
        state = jnp.where(z > k, sts[k].astype(F32), 0.0)
        entering = entering + factor * state
    heads = (
        heads
        + lax.dot_general(
            q_start[:32],
            jnp.where(low32, entering, 0.0).astype(BF16),
            TN,
            preferred_element_type=F32,
        )
        + lax.dot_general(
            q_start[32:],
            jnp.where(low32, 0.0, entering).astype(BF16),
            TN,
            preferred_element_type=F32,
        )
    )
    same_head = lax.div(iota((128, 128), 0), 64) == lax.div(iota((128, 128), 1), 64)
    same_head = jnp.where(same_head, 1.0, 0.0).astype(BF16)
    mean_square = jnp.dot(
        jnp.concatenate(thirds(heads * heads), axis=1),
        jnp.concatenate([same_head] * 3, axis=0),
        preferred_element_type=F32,
    ) * (1.0 / 64.0)
    gla_act = (
        heads * lax.rsqrt(mean_square + 1e-06) * hgain * (gates * sigmoid(gates))
    )

    mark("act_send")
    act_me[0] = jnp.where(low_lanes, conv_act, roll64(gla_act)).astype(BF16)
    act_me[1] = jnp.where(low_lanes, roll64(conv_act), gla_act).astype(BF16)
    def act_cols(j):
        return pl.ds(pl.multiple_of(x * 256 + j * 128, 128), 128)

    for s in range(2):
        mine = (2 * c + s == y) & (y_half == c)
        copy = remote(
            act_me.at[s],
            acts.at[:, act_cols(y_low)],
            act_send,
            act_recv.at[y_low],
            at(x, 2 * c + s, z, y_half),
        )
        pl.when(jnp.logical_not(mine))(copy.start)

        @pl.when(mine)
        def _():
            acts[:, act_cols(y_low)] = act_me[s]

    mark("act_pass")
    oy_pass(0, 0)
    oy_pass(1, 3)
    oy_pass(0, 1)
    oy_pass(1, 2)
    for n, j in enumerate((y_low, 1 - y_low)):
        block = acts.at[:, act_cols(j)]
        arrived = remote(block, block, act_send, act_recv.at[j], partner)
        if n == 0:
            pl.when(y_half != c)(arrived.wait_recv)
        else:
            arrived.wait_recv()
        for step in (2, 1, 3):
            there = at(lax.rem(x + step, 4), y, z, c)
            remote(block, block, act2_send, act2_recv, there).start()

    mark("oy_rest")
    for ahead in (3, 2):
        oy_wait(0, ahead, y_down)
    for ahead in (0, 1):
        oy_wait(1, ahead, y_up)
    for ahead in (0, 3, 1, 2):
        oy_wait(2, ahead, y_far)
    mark("act_wait")
    others = acts.at[:, pl.ds(0, 768)]
    remote(others, others, act2_send, act2_recv, partner).wait_recv()
    mark("output")
    def output(half):
        whole = lax.dot_general(acts[...], ow[half], NT, preferred_element_type=F32)
        parts = [whole[:, 128 * yy : 128 * yy + 128] for yy in range(4)]
        tiles = []
        for kk in range(2):
            for even, odd in ((parts[0], parts[1]), (parts[2], parts[3])):
                if kk == 0:
                    tiles.append(jnp.where(low_lanes, even, roll64(odd)))
                else:
                    tiles.append(jnp.where(low_lanes, roll64(even), odd))
        return jnp.concatenate(tiles, axis=1)

    po_send[...] = output(1 - c).astype(BF16)
    trade = remote(po_send, po_recv, d2d_send.at[2], d2d_recv.at[2], partner)
    start(trade)
    residual = xg[rows(y * TOK, TOK), feature_cols(x, c)]
    result = residual.astype(F32) + output(c)
    mark("trade_wait")
    trade.wait_recv()
    out[...] = (result + po_recv[...].astype(F32)).astype(BF16)

    mark("drain")
    for copy, cond in finish:
        if cond is None:
            copy.wait_send()
        else:
            pl.when(cond)(copy.wait_send)

    def left(piece, semaphore, cond=None):
        copy = remote(piece, piece, semaphore, stat_recv, partner)
        if cond is None:
            copy.wait_send()
        else:
            pl.when(cond)(copy.wait_send)

    left(stats.at[pl.ds(0, 15)], stat_send)
    left(tots.at[pl.ds(0, NZ - 1)], tot_send)
    left(sts.at[pl.ds(0, NZ - 1)], st_send)
    left(xg.at[pl.ds(0, 192), :], oy_send)
    left(acts.at[:, pl.ds(0, 128)], act_send, y_half == c)
    left(acts.at[:, pl.ds(0, 256)], act_send, y_half != c)
    left(acts.at[:, pl.ds(0, 768)], act2_send)
    left(xg.at[pl.ds(0, 832), :], x_send, c == 0)
    left(xg.at[pl.ds(0, 128), :], x_send, c == 1)
    left(xg.at[pl.ds(0, 480), :], xd_send, c == 0)
    left(owsrc, own_send, c == 0)
    left(w.at[pl.ds(0, 3840), :], wz_send, c == 1)
    left(w.at[pl.ds(0, 2048), :], wd_send, c == 1)
    left(ow.at[0, pl.ds(0, 448), :], od_send, c == 1)
    left(owz.at[pl.ds(0, 15)], oz_send, c == 1)
    mark(None)


def shards(
    inputs,
    norm_gain,
    conv_in_a,
    conv_in_b,
    query_w,
    key_w,
    value_w,
    out_gate_w,
    pointwise_w,
    gla_out_w,
    forget_first_factor,
    decay_w,
    decay_bias,
    decay_extra,
    conv_kernel,
    conv_gain,
    head_gain,
):
    dma = pltpu.SemaphoreType.DMA
    vmem = pltpu.VMEM
    mixed = pl.pallas_call(
        body,
        out_shape=jax.ShapeDtypeStruct((TOK, 512), BF16),
        in_specs=[pl.BlockSpec(memory_space=pltpu.HBM)] * 17,
        out_specs=pl.BlockSpec(memory_space=vmem),
        scratch_shapes=[
            vmem((32, 128), F32),
            vmem((6, 64, 128), BF16),
            vmem((2, 64, 64), BF16),
            vmem((64, 128), BF16),
            vmem((64, 128), BF16),
            vmem((4, 128), F32),
            vmem((2, 32, TOK), F32),
            vmem((31, 128), F32),
            vmem((8, 128), F32),
            vmem((1, 64), F32),
            vmem((2, 64, 384), BF16),
            vmem((64, 256), BF16),
            vmem((128, 128), BF16),
            vmem((128, 128), F32),
            vmem((32, 128), F32),
            dma((17,)),
            vmem((4 * TOK, 4096), BF16),
            vmem((4096, 384), BF16),
            vmem((2, 512, 1024), BF16),
            vmem((NZ, 2, 64, 256), BF16),
            vmem((512, 512), F32),
            vmem((512, 512), BF16),
            vmem((512, 512), BF16),
            vmem((10, TOK, TOK), BF16),
            vmem((TOK, TOK), jnp.int32),
            vmem((2, TOK, TOK), F32),
            vmem((TOK + 32, 128), F32),
            vmem((2, 32, TOK), F32),
            vmem((16, 8, TOK), F32),
            vmem((1, 128), F32),
            vmem((NZ, 1, 128), F32),
            vmem((32, 128), BF16),
            vmem((NZ, 32, 128), BF16),
            vmem((2, TOK, 128), BF16),
            vmem((TOK, 1024), BF16),
            vmem((TOK, 512), BF16),
            vmem((TOK, 512), BF16),
            dma,
            dma,
            dma,
            dma,
            dma((64,)),
            dma((2,)),
            dma((4,)),
            dma,
            dma,
            dma,
            dma,
            dma,
            dma((NZ,)),
            dma,
            dma((4,)),
            dma,
            dma((3, 4)),
            dma((2,)),
            dma((2,)),
            dma((3,)),
            dma((3,)),
            dma,
            dma,
            dma,
            dma,
            dma,
            dma,
            dma,
            dma,
            dma,
            dma((2,)),
            dma,
            dma,
        ],
        compiler_params=pltpu.CompilerParams(
            collective_id=0, has_side_effects=True
        ),
        name="mixer",
    )(
        inputs[0],
        norm_gain.reshape(32, 128),
        conv_in_a,
        conv_in_b,
        query_w,
        key_w,
        value_w,
        out_gate_w,
        pointwise_w,
        gla_out_w,
        forget_first_factor.T,
        decay_w,
        decay_bias.reshape(4, 128),
        decay_extra[0].T.reshape(2, 32, TOK),
        conv_kernel,
        conv_gain.reshape(8, 128),
        head_gain.reshape(1, 64),
    )
    return mixed[None]


def solution(mesh):
    weights = P(("sp", "fs"), "tp")
    return jax.shard_map(
        shards,
        mesh=mesh,
        in_specs=(
            P("fs", "sp", "tp"),
            P(),
            weights,
            weights,
            weights,
            weights,
            weights,
            weights,
            weights,
            weights,
            P(),
            P(),
            P(),
            P("fs", "sp", "tp"),
            P(),
            P(),
            P(),
        ),
        out_specs=P("fs", "sp", "tp"),
        check_vma=False,
    )
```

```python
import functools
import heapq

import jax
import jax.numpy as jnp
from jax import lax
from jax.experimental import pallas as pl
from jax.experimental.pallas import tpu as pltpu
from jax.sharding import PartitionSpec as P

MESH = pl.DeviceIdType.MESH
F32 = jnp.float32
BF16 = jnp.bfloat16
HIGHEST = lax.Precision.HIGHEST
NZ = 16
TOK = 256
NT = (((1,), (1,)), ((), ()))
TN = (((0,), (0,)), ((), ()))


def remote(src, dst, send, recv, device):
    return pltpu.make_async_remote_copy(
        src_ref=src,
        dst_ref=dst,
        send_sem=send,
        recv_sem=recv,
        device_id=device,
        device_id_type=MESH,
    )


def wrap(value, size):
    return lax.rem(value + size, size)


def rows(start, size):
    return pl.ds(pl.multiple_of(start, size), size)


def iota(shape, dim):
    return lax.broadcasted_iota(jnp.int32, shape, dim)


def sigmoid(value):
    return 1.0 / (1.0 + jnp.exp(-value))


def thirds(value):
    first = value.astype(BF16)
    rest = value - first.astype(F32)
    second = rest.astype(BF16)
    return first, second, (rest - second.astype(F32)).astype(BF16)


def roll64(value):
    return pltpu.roll(value, 64, 1)


OFFSETS = (0, -1, 1, 2)
UNIT = (64, 64)
W_HOP, W_PART = 2.7, 0.45


def x_forwards(f, g, u):
    sends = []
    if g == 0:
        if f == 0:
            sends += [(0, 0, 1, 0), (0, 1, 2, 0)]
        elif f < 3 and u == f - 1:
            sends += [(0, u, 3, 0)]
        sends += [(1, 0, f, 1), (1, 1, f, 2)]
    elif g < 3 and u == g - 1:
        sends += [(1, u, f, 3)]
    return sends


def x_order():
    unit, latency, lead = 1.41, 2.5, 1.5
    free = {(axis, way): 0.0 for axis in range(2) for way in range(2)}
    waiting = {link: [] for link in free}
    events, actions, count = [], [], 0

    def left_over(f, g, u):
        return 0 if not x_forwards(f, g, u) else 1 if g else 2 + (u == f - 1)

    def feed(link, now):
        if waiting[link] and free[link] <= now + 1e-6:
            _, _, since, block, send = heapq.heappop(waiting[link])
            free[link] = now + unit
            actions.append((max(since, now - lead), len(actions), block, send))
            heapq.heappush(events, (now + unit, 0, link))
            _, _, ff, gg = send
            heapq.heappush(events, (now + unit + latency, 1, (block[0], ff, gg, block[3])))

    def arrive(now, block):
        nonlocal count
        half, f, g, u = block
        for send in x_forwards(f, g, u):
            link = ((send[0] + half) % 2, send[1])
            count += 1
            heapq.heappush(
                waiting[link], (-left_over(send[2], send[3], u), count, now, block, send)
            )
        for link in free:
            feed(link, now)

    for half in range(2):
        for u in range(2):
            arrive(0.0, (half, 0, 0, u))
    while events:
        now, kind, what = heapq.heappop(events)
        if kind:
            actions.append((now, -1, what, None))
            arrive(now, what)
        else:
            feed(what, now)
    return [action[2:] for action in sorted(actions, key=lambda entry: entry[:2])]


def body(
    xin_hbm,
    gain_hbm,
    a_hbm,
    b_hbm,
    q_hbm,
    k_hbm,
    v_hbm,
    gate_hbm,
    point_hbm,
    gla_hbm,
    low_hbm,
    dw_hbm,
    bias_hbm,
    extra_hbm,
    kernel_hbm,
    cgain_hbm,
    hgain_hbm,
    out,
    gain_in,
    tiles_in,
    narrow_in,
    low_in,
    dw_in,
    bias_in,
    exsrc,
    taps_in,
    cgain_in,
    hgain_in,
    wsrc,
    owsrc,
    dwt,
    bias,
    taps,
    in_sem,
    xg,
    w,
    ow,
    owz,
    acc_own,
    acc_send,
    acc_recv,
    mats,
    xors,
    scores,
    ext,
    exb,
    stats,
    tot_me,
    tots,
    st_me,
    sts,
    act_me,
    acts,
    po_send,
    po_recv,
    x_send,
    xd_send,
    xd_recv,
    own_send,
    ring_recv,
    wy_send,
    wy_recv,
    wz_send,
    wd_send,
    wd_recv,
    ox_recv,
    oz_send,
    oz_recv,
    od_send,
    od_recv,
    oy_send,
    oy_recv,
    ex_send,
    ex_recv,
    d2d_send,
    d2d_recv,
    halo_send,
    halo_recv,
    stat_send,
    stat_recv,
    tot_send,
    tot_recv,
    st_send,
    st_recv,
    act_send,
    act_recv,
    act2_send,
    act2_recv,
):
    scope = []

    def mark(name):
        if scope:
            scope.pop().__exit__(None, None, None)
        if name:
            scope.append(jax.named_scope(name))
            scope[0].__enter__()

    z = lax.axis_index("sp")
    y = lax.axis_index("fs")
    t = lax.axis_index("tp")
    x = lax.div(t, 2)
    c = t - 2 * x
    y_half = lax.div(y, 2)
    y_low = y - 2 * y_half
    z_class = lax.rem(lax.div(z, 2), 2)
    partner = (z, y, 2 * x + 1 - c)

    def at(xx, yy, zz, cc):
        return (zz, yy, 2 * xx + cc)

    mark("greet")
    barrier = pltpu.get_barrier_semaphore()

    def greet(zz, yy, tt):
        pl.semaphore_signal(barrier, inc=1, device_id=(zz, yy, tt), device_id_type=MESH)

    for step in (1, NZ - 1):
        greet(lax.rem(z + step, NZ), y, t)
    for step in range(1, 8):
        greet(z, y, lax.rem(t + step, 8))
    for step in range(1, 4):
        for cc in range(2):
            greet(z, lax.rem(y + step, 4), 2 * x + cc)

    group_pair = 2 * x + y_half

    def tile_of(index):
        return pl.ds(pl.multiple_of(index * 128, 128), 128)

    def feature_cols(xx, cc):
        return pl.ds(pl.multiple_of((2 * xx + cc) * 512, 512), 512)

    fetches = [
        pltpu.make_async_copy(source, target, in_sem.at[k])
        for k, (source, target) in enumerate(
            (
                (a_hbm, tiles_in.at[0]),
                (b_hbm, tiles_in.at[1]),
                (v_hbm, tiles_in.at[2]),
                (gate_hbm, tiles_in.at[3]),
                (point_hbm, tiles_in.at[4]),
                (gla_hbm, tiles_in.at[5]),
                (q_hbm, narrow_in.at[0]),
                (k_hbm, narrow_in.at[1]),
                (gain_hbm, gain_in),
                (low_hbm.at[:, tile_of(2 * z + y_half)], low_in),
                (xin_hbm, xg.at[rows(y * TOK, TOK), feature_cols(x, c)]),
                (extra_hbm, exsrc),
                (dw_hbm.at[:, tile_of(x)], dw_in),
                (bias_hbm, bias_in),
                (kernel_hbm.at[:, tile_of(group_pair)], taps_in),
                (cgain_hbm, cgain_in),
                (hgain_hbm, hgain_in),
            )
        )
    ]
    for fetch in fetches:
        fetch.start()

    mark("pack")
    low64 = iota((64, 128), 1) < 64
    lane64 = iota((64, 128), 1)
    y_even = y_low == 0

    def column(row_vector):
        return jnp.broadcast_to(row_vector, (128, 128)).T

    for fetch in fetches[:10]:
        fetch.wait()
    gain_all = column(gain_in[pl.ds(2 * z + y_half, 1), :])
    gain = jnp.where(y_even, gain_all[:64], gain_all[64:])

    def pair(k, scale):
        first = tiles_in[k].astype(F32) * scale
        second = tiles_in[k + 1].astype(F32) * scale
        return (
            jnp.where(low64, first, roll64(second)).astype(BF16),
            jnp.where(low64, roll64(first), second).astype(BF16),
        )

    for k in range(2):
        both = pair(2 * k, gain)
        for j in range(2):
            wsrc[j, :, 128 * k : 128 * k + 128] = both[j]
    both = pair(4, 1.0)
    for j in range(2):
        owsrc[:, 128 * j : 128 * j + 128] = both[j]
    narrow = jnp.concatenate([narrow_in[0], narrow_in[1]], axis=1).astype(F32)
    low_rows = low_in[...].astype(F32)
    low_rows = jnp.concatenate([low_rows, low_rows], axis=0).T
    low_rows = jnp.where(y_even, low_rows[:64], low_rows[64:])
    back32, back64 = pltpu.roll(narrow, 96, 1), roll64(narrow)
    mixed0 = jnp.where(low64, jnp.where(lane64 < 32, narrow, back32), low_rows)
    mixed1 = jnp.where(low64, jnp.where(lane64 < 32, back32, back64), low_rows)
    wsrc[0, :, 256:] = (mixed0 * gain).astype(BF16)
    wsrc[1, :, 256:] = (mixed1 * gain).astype(BF16)
    for fetch in fetches[10:12]:
        fetch.wait()
    mark("barrier_wait")
    pl.semaphore_wait(barrier, 2 + 7 + 6)

    finish = []

    def start(copy, cond=None):
        if cond is None:
            copy.start()
        else:
            pl.when(cond)(copy.start)
        finish.append((copy, cond))

    mark("first_sends")
    def w_at(zz, k):
        kind = lax.rem(lax.div(zz, 2), 2)
        begin = kind * 2048 + lax.div(zz, 4) * 512 + lax.rem(zz, 2) * 256 + k * 64
        return w.at[rows(begin, 64), :]

    for j in range(2):
        mine = jnp.logical_and(2 * c + j == y, c == 1)
        start(
            remote(
                wsrc.at[j], w_at(z, y), wy_send.at[j], wy_recv.at[y], at(x, 2 * c + j, z, 1)
            ),
            jnp.logical_not(mine),
        )

        @pl.when(mine)
        def _():
            w_at(z, y)[...] = wsrc[j]

    x_up, x_down = wrap(x + 1, 4), wrap(x - 1, 4)
    y_up, y_down = wrap(y + 1, 4), wrap(y - 1, 4)
    z_up, z_down = wrap(z + 1, NZ), wrap(z - 1, NZ)
    along_x = (at(x_up, y, z, 0), at(x_down, y, z, 0))
    along_y = (at(x, y_up, z, 0), at(x, y_down, z, 0))

    def x_rows(yy, half, u):
        begin = yy * TOK + 2 * UNIT[0] * half + UNIT[half] * u
        return pl.ds(pl.multiple_of(begin, 16), UNIT[half])

    def x_place(half, f, g, u):
        df, dg = OFFSETS[f], OFFSETS[g]
        xx, yy = (x + df, y + dg) if half == 0 else (x + dg, y + df)
        xx, yy = wrap(xx, 4), wrap(yy, 4)
        cols = pl.ds(pl.multiple_of(xx * 1024, 1024), 1024)
        if f == 0 and g == 0:
            cols = feature_cols(xx, c)
        return (
            xg.at[x_rows(yy, half, u), cols],
            xg.at[x_rows(yy, half, u), feature_cols(xx, 1)],
        )

    def x_send_on(block, send):
        place, _ = x_place(*block)
        half, u = block[0], block[3]
        which, way, ff, gg = send
        axis = along_x if (which + half) % 2 == 0 else along_y
        slot = 32 * half + 8 * ff + 2 * gg + u
        remote(place, place, x_send, ring_recv.at[slot], axis[way]).start()

    def x_wait(block):
        place, others = x_place(*block)
        half, f, g, u = block
        slot = 32 * half + 8 * f + 2 * g + u
        remote(place, place, x_send, ring_recv.at[slot], partner).wait_recv()
        remote(others, others, xd_send, xd_recv, partner).start()

    x_actions = x_order()
    x_first = [action for action in x_actions if action[0][1:3] == (0, 0)]
    for block, send in x_first[:8]:
        x_send_on(block, send)

    @pl.when(c == 0)
    def _():
        remote(owsrc, owz.at[z, 0], own_send, ox_recv, partner).start()

    @pl.when(c == 1)
    def _():
        owz[z, 1] = owsrc[...]

    for j in range(2):
        mine = jnp.logical_and(2 * c + j == y, y_half == c)
        start(
            remote(
                exsrc.at[j],
                exb.at[y_low],
                ex_send.at[j],
                ex_recv.at[y_low],
                at(x, 2 * c + j, z, y_half),
            ),
            jnp.logical_not(mine),
        )

        @pl.when(mine)
        def _():
            exb[y_low] = exsrc[j]

    up, down = (z_up, y, t), (z_down, y, t)

    ways = (up, down)

    def z_last(way, k):
        return 8 if (k in (0, 1, 4)) == (way == 0) else 7


    def w_on(way, d, k, origin):
        here = w_at(origin, k)
        if d < z_last(way, k):
            remote(here, here, wz_send, ring_recv.at[4 * origin + k], ways[way]).start()
        if d == 0 and way == 0:
            return

        @pl.when(lax.rem(lax.div(origin, 2), 2) == 0)
        def _():
            remote(here, here, wd_send, wd_recv, partner).start()

    def w_start(k):
        here = w_at(z, k)

        @pl.when(jnp.logical_not(jnp.logical_and(y == k, y_half == 1)))
        def _():
            remote(here, here, wz_send, wy_recv.at[k], up).wait_recv()

        w_on(0, 0, k, z)
        w_on(1, 0, k, z)

    def w_event(way, d, k):
        origin = wrap(z - d if way == 0 else z + d, NZ)
        here = w_at(origin, k)
        remote(here, here, wz_send, ring_recv.at[4 * origin + k], up).wait_recv()
        w_on(way, d, k, origin)

    def ow_cols(xx):
        return pl.ds(pl.multiple_of(xx * 256, 256), 256)

    def ow_at(zz):
        k = lax.rem(zz, 4)
        half = lax.div(k, 2)
        return ow.at[half, rows(y * 128 + (k - 2 * half) * 64, 64), ow_cols(x)]

    def ow_on(way, d, cc, origin):
        here = owz.at[origin, cc]
        if d < z_last(way, 4 + cc):
            remote(here, here, oz_send, oz_recv.at[origin, cc], ways[way]).start()

    def ow_give(n, carry):
        turn = lax.div(n, 4)
        ahead = jnp.where(turn == 2, 3, jnp.where(turn == 3, 2, turn))
        column = lax.rem(x + ahead, 4)
        origin = 4 * column + lax.rem(n, 4)
        behind = lax.rem(4 - ahead, 4)
        place = ow_at(origin)

        def give(cc):
            remote(
                owz.at[origin, cc], place, od_send, od_recv.at[behind], at(column, y, z, cc)
            ).start()

        give(0)
        pl.when(column != x)(functools.partial(give, 1))

        @pl.when(column == x)
        def _():
            place[...] = owz[origin, 1]

        return carry

    def ow_start():
        for cc in (1, 0):
            if cc == 0:
                here = owz.at[z, 0]
                remote(here, here, oz_send, ox_recv, partner).wait_recv()
            ow_on(0, 0, cc, z)
            ow_on(1, 0, cc, z)

    def ow_event(way, d, k):
        origin = wrap(z - d if way == 0 else z + d, NZ)
        here = owz.at[origin, k - 4]
        remote(here, here, oz_send, oz_recv.at[origin, k - 4], up).wait_recv()
        ow_on(way, d, k - 4, origin)

    mark("params")
    for fetch in fetches[12:]:
        fetch.wait()
    dw_all = dw_in[...].astype(F32)
    dw_all = jnp.concatenate([dw_all, dw_all], axis=0).T
    dwt[...] = dw_all.astype(BF16)
    bias[...] = column(bias_in[pl.ds(x, 1), :])
    low31 = iota((31, 128), 1) < 64
    tap_rows = taps_in[...]
    tap_back = roll64(tap_rows)
    taps[:31, :] = jnp.where(low31 == y_even, tap_rows, tap_back)
    cgain_row = cgain_in[pl.ds(group_pair, 1), :]
    cgain = jnp.where(low31[:1] == y_even, cgain_row, roll64(cgain_row))
    hgain = jnp.concatenate([hgain_in[...], hgain_in[...]], axis=1)

    mark("constants")
    lane = iota((TOK, TOK), 1)
    row = iota((TOK, TOK), 0)
    xors[...] = jnp.bitwise_xor(row, lane)
    one = jnp.ones((TOK, TOK), F32)
    nil = jnp.zeros((TOK, TOK), F32)

    def level_matrix(level, carry):
        half = lax.shift_left(jnp.int32(1), level)
        base = lane - jnp.bitwise_and(lane, 2 * half - 1)
        middle = base + half - 1
        low = jnp.minimum(lane, middle)
        high = jnp.maximum(lane, middle)
        mats[level] = jnp.where(
            jnp.logical_and(row > low, row <= high), one, nil
        ).astype(BF16)
        return carry

    lax.fori_loop(0, 8, level_matrix, 0)
    mats[8] = jnp.where(row <= lane, one, nil).astype(BF16)
    mats[9] = jnp.where(row > lane, one, nil).astype(BF16)

    z_agenda = []
    for way in range(2):
        for d in range(1, 9):
            for k in range(6):
                if d > z_last(way, k):
                    continue
                call = ow_event if k >= 4 else w_event
                z_agenda.append((W_HOP * d + W_PART * k, call, (way, d, k)))
    z_agenda.sort(key=lambda entry: entry[0])
    mark("gather")

    @pl.when(c == 0)
    def _():
        for n, (block, send) in enumerate(x_actions):
            if n % 30 == 0:
                mark(f"x{n}")
            if send is None:
                x_wait(block)
            elif (block, send) not in x_first[:8]:
                x_send_on(block, send)
        mark("w_arrive")
        everything = w.at[pl.ds(0, 2048), :]
        remote(everything, everything, wd_send, wd_recv, partner).wait_recv()
        mark(None)

    @pl.when(c == 1)
    def _():
        for block, send in x_first[8:]:
            x_send_on(block, send)
        for k in range(4):
            w_start(k)
        ow_start()
        for n, (_, call, event) in enumerate(z_agenda):
            if n % 24 == 0:
                mark(f"z{n}")
            call(*event)
        lax.fori_loop(0, 16, ow_give, 0)
        mark("x_arrive")
        everything = xg.at[pl.ds(0, 480), :]
        remote(everything, everything, xd_send, xd_recv, partner).wait_recv()
        mark(None)

    y_next = (at(x, y_up, z, c), at(x, y_down, z, c))
    y_from = (y_down, y_up)
    y_far = wrap(y + 2, 4)

    def oy_at(yy, ahead):
        return ow.at[:, rows(yy * 128, 128), ow_cols(lax.rem(x + ahead, 4))]

    def oy_own(way, ahead):
        here = oy_at(y, ahead)
        remote(here, here, oy_send, oy_recv.at[way, ahead], y_next[way]).start()

    def oy_wait(way, ahead, yy):
        here = oy_at(yy, ahead)
        remote(here, here, oy_send, oy_recv.at[way, ahead], partner).wait_recv()

    def oy_pass(way, ahead):
        oy_wait(way, ahead, y_from[way])
        here = oy_at(y_from[way], ahead)
        remote(here, here, oy_send, oy_recv.at[2, ahead], y_next[way]).start()

    mark("project")
    def swap_part(n):
        part = pl.ds(128, 384) if n == 0 else pl.ds(0, 128)
        return remote(
            acc_send.at[:, part], acc_recv.at[:, part], d2d_send.at[n], d2d_recv.at[n], partner
        )

    def project(half, target, n):
        begin, size = (128, 256) if n == 0 else (0, 128)
        for s in range(2):
            at_rows = pl.ds(s * TOK, TOK)
            blocks = [
                xg[rows((2 * half + s) * TOK, TOK), feature_cols(k, c)] for k in range(4)
            ]
            total = jnp.zeros((TOK, size), F32)
            for k in range(4):
                total = total + jnp.dot(
                    blocks[k],
                    w[rows(c * 2048 + 512 * k, 512), begin : begin + size],
                    preferred_element_type=F32,
                )
            target[at_rows, begin : begin + size] = total.astype(target.dtype)
            if n:
                continue
            squares = jnp.zeros((TOK, 128), F32)
            for k in range(16):
                piece = blocks[k // 4][:, 128 * (k % 4) : 128 * (k % 4) + 128].astype(F32)
                squares = squares + piece * piece
            target[at_rows, 384:] = squares.astype(target.dtype)

    def ow_wait(ahead):
        unit = ow.at[0, pl.ds(0, 64), :]
        copy = remote(unit, unit, od_send, od_recv.at[ahead], partner)
        if ahead:
            copy.wait_recv()
        else:
            pl.when(c == 0)(copy.wait_recv)

    project(1 - c, acc_send, 0)
    start(swap_part(0))
    ow_wait(0)
    oy_own(0, 0)
    oy_own(1, 0)
    mark("project2")
    project(c, acc_own, 0)
    mark("project3")
    project(1 - c, acc_send, 1)
    start(swap_part(1))
    mark("swap_wait")
    swap_part(0).wait_recv()

    low_lanes = iota((TOK, 128), 1) < 64

    def scaled(s):
        at_rows = pl.ds(s * TOK, TOK)
        both = acc_own[at_rows, 128:] + acc_recv[at_rows, 128:].astype(F32)
        mean = jnp.sum(both[:, 256:], axis=1, keepdims=True) * (1.0 / 4096.0)
        factor = lax.rsqrt(mean + 1e-06)
        return factor, (both[:, :256] * factor).astype(BF16).astype(F32)

    (factor0, p0), (factor1, p1) = scaled(0), scaled(1)

    mark("gating")
    project(c, acc_own, 1)
    swap_part(1).wait_recv()
    first, second = (
        ((acc_own[part, :128] + acc_recv[part, :128].astype(F32)) * factor).astype(BF16).astype(F32)
        for part, factor in ((pl.ds(0, TOK), factor0), (pl.ds(TOK, TOK), factor1))
    )
    left = jnp.where(low_lanes, first, roll64(second))
    right = jnp.where(low_lanes, roll64(first), second)
    ext[32:, :] = (left * sigmoid(right)).astype(BF16).astype(F32)
    start(
        remote(
            ext.at[pl.ds(TOK, 32), :], ext.at[pl.ds(0, 32), :], halo_send, halo_recv, up
        ),
        z < NZ - 1,
    )
    mark("decay")
    v0, v1 = p0[:, :128], p1[:, :128]
    gates = jnp.where(low_lanes, roll64(v0), v1)
    zero = jnp.zeros((TOK, 128), F32)
    v0 = jnp.where(low_lanes, v0, zero).astype(BF16)
    v1 = jnp.where(low_lanes, zero, roll64(v1)).astype(BF16)
    qt0, qt1 = p0[:, 128:].T, p1[:, 128:].T
    queries = jnp.concatenate([qt0[:32], qt1[:32]], axis=0) * (32.0 ** (-0.5))
    keys = jnp.concatenate([qt0[32:64], qt1[32:64]], axis=0)
    for s in range(2):
        local = jnp.logical_and(y_half == c, y_low == s)

        @pl.when(jnp.logical_not(local))
        def _():
            remote(exb.at[s], exb.at[s], ex_send.at[s], ex_recv.at[s], up).wait_recv()

    decays = []
    for s, qt in enumerate((qt0, qt1)):
        pre = (
            jnp.dot(
                dwt[rows(32 * y, 32), :][:, :64],
                qt[64:].astype(BF16),
                preferred_element_type=F32,
            )
            + bias[rows(32 * y, 32), :][:, :1]
        )
        log_sig = jnp.minimum(pre, 0.0) - jnp.log1p(jnp.exp(-jnp.abs(pre)))
        decays.append(log_sig * (1.0 / 16.0) + exb[s])
    decay = jnp.concatenate(decays, axis=0)
    parts = jnp.concatenate(thirds(decay), axis=0)

    def decay_sums(which):
        sums = jnp.dot(parts, mats[which], preferred_element_type=F32)
        return jnp.exp(sums[:64] + sums[64:128] + sums[128:])

    tail_keys = (keys * decay_sums(9)).astype(BF16)
    st_me[...] = (
        jnp.dot(tail_keys[:32], v0, preferred_element_type=F32)
        + jnp.dot(tail_keys[32:], v1, preferred_element_type=F32)
    ).astype(BF16)
    wide = jnp.concatenate([decay, jnp.zeros((64, TOK), F32)], axis=0)
    tot_me[...] = lax.dot_general(
        jnp.ones((8, TOK), F32), wide, NT, precision=HIGHEST, preferred_element_type=F32
    )[:1]

    def tell(n, carry):
        half = lax.div(n + 1, 2)
        k = jnp.where(lax.rem(n, 2) == 0, 8 - half, 8 + half)
        there = (lax.rem(z + k, NZ), y, t)
        remote(tot_me, tots.at[z], tot_send, tot_recv, there).start()
        remote(st_me, sts.at[z], st_send, st_recv, there).start()
        return carry

    lax.fori_loop(0, NZ - 1, tell, 0)

    ow_wait(1)
    oy_own(0, 1)
    oy_own(1, 1)
    mark("halo_wait")
    @pl.when(z == 0)
    def _():
        ext[:32, :] = jnp.zeros((32, 128), F32)

    @pl.when(z > 0)
    def _():
        halo = ext.at[pl.ds(0, 32), :]
        remote(halo, halo, halo_send, halo_recv, up).wait_recv()

    mark("conv")
    conv = jnp.zeros((TOK, 128), F32)
    for tap in range(31):
        conv = conv + taps[tap : tap + 1, :] * ext[2 + tap : 2 + tap + TOK, :]
    lane8, row8 = iota((8, 128), 1), iota((8, 128), 0)
    seq_of = lax.div(lane8, 64)
    pick_sum = jnp.where(row8 == seq_of, 1.0, 0.0).astype(BF16)
    pick_square = jnp.where(row8 == seq_of + 2, 1.0, 0.0).astype(BF16)
    me = 4 * x + y
    stats[me] = lax.dot_general(
        jnp.concatenate([pick_sum] * 3 + [pick_square] * 3, axis=1),
        jnp.concatenate([*thirds(conv), *thirds(conv * conv)], axis=1),
        NT,
        preferred_element_type=F32,
    )

    def stat_copy(k):
        other = lax.rem(me + k, 16)
        xx = lax.div(other, 4)
        return remote(
            stats.at[me],
            stats.at[me],
            stat_send,
            stat_recv,
            at(xx, other - 4 * xx, z, c),
        )

    def send_stat(k, carry):
        stat_copy(k).start()
        return carry

    lax.fori_loop(1, 16, send_stat, 0)

    ow_wait(3)
    oy_own(0, 3)
    oy_own(1, 3)

    mark("attention")
    queries_low, keys_low = queries.astype(BF16), keys.astype(BF16)
    for s in range(2):
        own = lax.dot_general(
            queries_low[32 * s : 32 * s + 32],
            keys_low[32 * s : 32 * s + 32],
            TN,
            preferred_element_type=F32,
        )
        scores[s] = jnp.where(xors[...] == 0, own, 0.0)
    lane_of = iota((64, TOK), 1)

    def level_scores(level, carry):
        factor = decay_sums(level)
        upper = jnp.bitwise_and(lax.shift_right_logical(lane_of, level), 1) == 1
        q_level = jnp.where(upper, queries * factor, 0.0).astype(BF16)
        k_level = jnp.where(upper, 0.0, keys * factor).astype(BF16)
        same = lax.shift_right_logical(xors[...], level + 1) == 0
        for s in range(2):
            pair = lax.dot_general(
                q_level[32 * s : 32 * s + 32],
                k_level[32 * s : 32 * s + 32],
                TN,
                preferred_element_type=F32,
            )
            scores[s] = scores[s] + jnp.where(same, pair, 0.0)
        return carry

    lax.fori_loop(0, 4, level_scores, 0)

    ow_wait(2)
    oy_own(0, 2)
    oy_own(1, 2)
    mark("attention2")
    lax.fori_loop(4, 8, level_scores, 0)
    heads = jnp.dot(scores[0].astype(BF16), v0, preferred_element_type=F32) + jnp.dot(
        scores[1].astype(BF16), v1, preferred_element_type=F32
    )
    q_start = (queries * decay_sums(8)).astype(BF16)

    mark("stat_wait")
    others = stats.at[pl.ds(0, 15)]
    remote(others, others, stat_send, stat_recv, up).wait_recv()
    mark("norm")
    total = stats[0]
    for k in range(1, 16):
        total = total + stats[k]
    picks = jnp.concatenate([pick_sum, pick_square], axis=1)
    moments = lax.dot_general(
        jnp.concatenate(thirds(total), axis=0),
        jnp.concatenate([picks] * 3, axis=0),
        TN,
        preferred_element_type=F32,
    ) * (1.0 / 1024.0)
    average, spread = moments[:, :128], moments[:, 128:]
    variance = jnp.maximum(spread - average * average, 0.0)
    normed = (conv - average) * lax.rsqrt(variance + 1e-05) * cgain
    conv_act = normed * sigmoid(normed)

    mark("state_wait")
    others = tots.at[pl.ds(0, NZ - 1)]
    remote(others, others, tot_send, tot_recv, up).wait_recv()
    others = sts.at[pl.ds(0, NZ - 1)]
    remote(others, others, st_send, st_recv, up).wait_recv()
    mark("heads")
    row16 = iota((NZ, 128), 0)
    known = jnp.where(row16 < z, tots[:, 0, :], 0.0)
    from_row, to_row = iota((NZ, NZ), 0), iota((NZ, NZ), 1)
    between = jnp.where(
        jnp.logical_and(to_row > from_row, to_row < z), 1.0, 0.0
    ).astype(F32)
    exponent = jnp.dot(between, known, precision=HIGHEST, preferred_element_type=F32)
    reach = jnp.where(row16 < z, jnp.exp(exponent), 0.0)
    reach = jnp.concatenate([reach, jnp.zeros((128 - NZ, 128), F32)], axis=0).T
    low32 = iota((32, 128), 1) < 64
    entering = jnp.zeros((32, 128), F32)
    for k in range(NZ - 1):
        factor = jnp.where(low32, reach[:32, k : k + 1], reach[32:64, k : k + 1])
        state = jnp.where(z > k, sts[k].astype(F32), 0.0)
        entering = entering + factor * state
    heads = (
        heads
        + lax.dot_general(
            q_start[:32],
            jnp.where(low32, entering, 0.0).astype(BF16),
            TN,
            preferred_element_type=F32,
        )
        + lax.dot_general(
            q_start[32:],
            jnp.where(low32, 0.0, entering).astype(BF16),
            TN,
            preferred_element_type=F32,
        )
    )
    same_head = lax.div(iota((128, 128), 0), 64) == lax.div(iota((128, 128), 1), 64)
    same_head = jnp.where(same_head, 1.0, 0.0).astype(BF16)
    mean_square = jnp.dot(
        jnp.concatenate(thirds(heads * heads), axis=1),
        jnp.concatenate([same_head] * 3, axis=0),
        preferred_element_type=F32,
    ) * (1.0 / 64.0)
    gla_act = (
        heads * lax.rsqrt(mean_square + 1e-06) * hgain * (gates * sigmoid(gates))
    )

    mark("act_send")
    act_me[0] = jnp.where(low_lanes, conv_act, roll64(gla_act)).astype(BF16)
    act_me[1] = jnp.where(low_lanes, roll64(conv_act), gla_act).astype(BF16)
    def act_cols(j):
        return pl.ds(pl.multiple_of(x * 256 + j * 128, 128), 128)

    for s in range(2):
        mine = (2 * c + s == y) & (y_half == c)
        copy = remote(
            act_me.at[s],
            acts.at[:, act_cols(y_low)],
            act_send,
            act_recv.at[y_low],
            at(x, 2 * c + s, z, y_half),
        )
        pl.when(jnp.logical_not(mine))(copy.start)

        @pl.when(mine)
        def _():
            acts[:, act_cols(y_low)] = act_me[s]

    mark("act_pass")
    oy_pass(0, 0)
    oy_pass(1, 3)
    oy_pass(0, 1)
    oy_pass(1, 2)
    for n, j in enumerate((y_low, 1 - y_low)):
        block = acts.at[:, act_cols(j)]
        arrived = remote(block, block, act_send, act_recv.at[j], partner)
        if n == 0:
            pl.when(y_half != c)(arrived.wait_recv)
        else:
            arrived.wait_recv()
        for step in (2, 1, 3):
            there = at(lax.rem(x + step, 4), y, z, c)
            remote(block, block, act2_send, act2_recv, there).start()

    mark("oy_rest")
    for ahead in (3, 2):
        oy_wait(0, ahead, y_down)
    for ahead in (0, 1):
        oy_wait(1, ahead, y_up)
    for ahead in (0, 3, 1, 2):
        oy_wait(2, ahead, y_far)
    mark("act_wait")
    others = acts.at[:, pl.ds(0, 768)]
    remote(others, others, act2_send, act2_recv, partner).wait_recv()
    mark("output")
    def output(half):
        whole = lax.dot_general(acts[...], ow[half], NT, preferred_element_type=F32)
        parts = [whole[:, 128 * yy : 128 * yy + 128] for yy in range(4)]
        tiles = []
        for kk in range(2):
            for even, odd in ((parts[0], parts[1]), (parts[2], parts[3])):
                if kk == 0:
                    tiles.append(jnp.where(low_lanes, even, roll64(odd)))
                else:
                    tiles.append(jnp.where(low_lanes, roll64(even), odd))
        return jnp.concatenate(tiles, axis=1)

    po_send[...] = output(1 - c).astype(BF16)
    trade = remote(po_send, po_recv, d2d_send.at[2], d2d_recv.at[2], partner)
    start(trade)
    residual = xg[rows(y * TOK, TOK), feature_cols(x, c)]
    result = residual.astype(F32) + output(c)
    mark("trade_wait")
    trade.wait_recv()
    out[...] = (result + po_recv[...].astype(F32)).astype(BF16)

    mark("drain")
    for copy, cond in finish:
        if cond is None:
            copy.wait_send()
        else:
            pl.when(cond)(copy.wait_send)

    def left(piece, semaphore, cond=None):
        copy = remote(piece, piece, semaphore, stat_recv, partner)
        if cond is None:
            copy.wait_send()
        else:
            pl.when(cond)(copy.wait_send)

    left(stats.at[pl.ds(0, 15)], stat_send)
    left(tots.at[pl.ds(0, NZ - 1)], tot_send)
    left(sts.at[pl.ds(0, NZ - 1)], st_send)
    left(xg.at[pl.ds(0, 192), :], oy_send)
    left(acts.at[:, pl.ds(0, 128)], act_send, y_half == c)
    left(acts.at[:, pl.ds(0, 256)], act_send, y_half != c)
    left(acts.at[:, pl.ds(0, 768)], act2_send)
    left(xg.at[pl.ds(0, 832), :], x_send, c == 0)
    left(xg.at[pl.ds(0, 128), :], x_send, c == 1)
    left(xg.at[pl.ds(0, 480), :], xd_send, c == 0)
    left(owsrc, own_send, c == 0)
    left(w.at[pl.ds(0, 3840), :], wz_send, c == 1)
    left(w.at[pl.ds(0, 2048), :], wd_send, c == 1)
    left(ow.at[0, pl.ds(0, 448), :], od_send, c == 1)
    left(owz.at[pl.ds(0, 15)], oz_send, c == 1)
    mark(None)


def shards(
    inputs,
    norm_gain,
    conv_in_a,
    conv_in_b,
    query_w,
    key_w,
    value_w,
    out_gate_w,
    pointwise_w,
    gla_out_w,
    forget_first_factor,
    decay_w,
    decay_bias,
    decay_extra,
    conv_kernel,
    conv_gain,
    head_gain,
):
    dma = pltpu.SemaphoreType.DMA
    vmem = pltpu.VMEM
    mixed = pl.pallas_call(
        body,
        out_shape=jax.ShapeDtypeStruct((TOK, 512), BF16),
        in_specs=[pl.BlockSpec(memory_space=pltpu.HBM)] * 17,
        out_specs=pl.BlockSpec(memory_space=vmem),
        scratch_shapes=[
            vmem((32, 128), F32),
            vmem((6, 64, 128), BF16),
            vmem((2, 64, 64), BF16),
            vmem((64, 128), BF16),
            vmem((64, 128), BF16),
            vmem((4, 128), F32),
            vmem((2, 32, TOK), F32),
            vmem((31, 128), F32),
            vmem((8, 128), F32),
            vmem((1, 64), F32),
            vmem((2, 64, 384), BF16),
            vmem((64, 256), BF16),
            vmem((128, 128), BF16),
            vmem((128, 128), F32),
            vmem((32, 128), F32),
            dma((17,)),
            vmem((4 * TOK, 4096), BF16),
            vmem((4096, 384), BF16),
            vmem((2, 512, 1024), BF16),
            vmem((NZ, 2, 64, 256), BF16),
            vmem((512, 512), F32),
            vmem((512, 512), BF16),
            vmem((512, 512), BF16),
            vmem((10, TOK, TOK), BF16),
            vmem((TOK, TOK), jnp.int32),
            vmem((2, TOK, TOK), F32),
            vmem((TOK + 32, 128), F32),
            vmem((2, 32, TOK), F32),
            vmem((16, 8, TOK), F32),
            vmem((1, 128), F32),
            vmem((NZ, 1, 128), F32),
            vmem((32, 128), BF16),
            vmem((NZ, 32, 128), BF16),
            vmem((2, TOK, 128), BF16),
            vmem((TOK, 1024), BF16),
            vmem((TOK, 512), BF16),
            vmem((TOK, 512), BF16),
            dma,
            dma,
            dma,
            dma,
            dma((64,)),
            dma((2,)),
            dma((4,)),
            dma,
            dma,
            dma,
            dma,
            dma,
            dma((NZ, 2)),
            dma,
            dma((4,)),
            dma,
            dma((3, 4)),
            dma((2,)),
            dma((2,)),
            dma((3,)),
            dma((3,)),
            dma,
            dma,
            dma,
            dma,
            dma,
            dma,
            dma,
            dma,
            dma,
            dma((2,)),
            dma,
            dma,
        ],
        compiler_params=pltpu.CompilerParams(
            collective_id=0, has_side_effects=True
        ),
        name="mixer",
    )(
        inputs[0],
        norm_gain.reshape(32, 128),
        conv_in_a,
        conv_in_b,
        query_w,
        key_w,
        value_w,
        out_gate_w,
        pointwise_w,
        gla_out_w,
        forget_first_factor.T,
        decay_w,
        decay_bias.reshape(4, 128),
        decay_extra[0].T.reshape(2, 32, TOK),
        conv_kernel,
        conv_gain.reshape(8, 128),
        head_gain.reshape(1, 64),
    )
    return mixed[None]


def solution(mesh):
    weights = P(("sp", "fs"), "tp")
    return jax.shard_map(
        shards,
        mesh=mesh,
        in_specs=(
            P("fs", "sp", "tp"),
            P(),
            weights,
            weights,
            weights,
            weights,
            weights,
            weights,
            weights,
            weights,
            P(),
            P(),
            P(),
            P("fs", "sp", "tp"),
            P(),
            P(),
            P(),
        ),
        out_specs=P("fs", "sp", "tp"),
        check_vma=False,
    )
```

```python
import functools
import heapq

import jax
import jax.numpy as jnp
from jax import lax
from jax.experimental import pallas as pl
from jax.experimental.pallas import tpu as pltpu
from jax.sharding import PartitionSpec as P

MESH = pl.DeviceIdType.MESH
F32 = jnp.float32
BF16 = jnp.bfloat16
HIGHEST = lax.Precision.HIGHEST
NZ = 16
TOK = 256
NT = (((1,), (1,)), ((), ()))
TN = (((0,), (0,)), ((), ()))


def remote(src, dst, send, recv, device):
    return pltpu.make_async_remote_copy(
        src_ref=src,
        dst_ref=dst,
        send_sem=send,
        recv_sem=recv,
        device_id=device,
        device_id_type=MESH,
    )


def wrap(value, size):
    return lax.rem(value + size, size)


def rows(start, size):
    return pl.ds(pl.multiple_of(start, size), size)


def iota(shape, dim):
    return lax.broadcasted_iota(jnp.int32, shape, dim)


def sigmoid(value):
    return 1.0 / (1.0 + jnp.exp(-value))


def thirds(value):
    first = value.astype(BF16)
    rest = value - first.astype(F32)
    second = rest.astype(BF16)
    return first, second, (rest - second.astype(F32)).astype(BF16)


def roll64(value):
    return pltpu.roll(value, 64, 1)


OFFSETS = (0, -1, 1, 2)
UNIT = (64, 64)
W_HOP, W_PART = 2.7, 0.45


def x_forwards(f, g, u):
    sends = []
    if g == 0:
        if f == 0:
            sends += [(0, 0, 1, 0), (0, 1, 2, 0)]
        elif f < 3 and u == f - 1:
            sends += [(0, u, 3, 0)]
        sends += [(1, 0, f, 1), (1, 1, f, 2)]
    elif g < 3 and u == g - 1:
        sends += [(1, u, f, 3)]
    return sends


def x_order():
    unit, latency, lead = 1.41, 2.5, 1.5
    free = {(axis, way): 0.0 for axis in range(2) for way in range(2)}
    waiting = {link: [] for link in free}
    events, actions, count = [], [], 0

    def left_over(f, g, u):
        return 0 if not x_forwards(f, g, u) else 1 if g else 2 + (u == f - 1)

    def feed(link, now):
        if waiting[link] and free[link] <= now + 1e-6:
            _, _, since, block, send = heapq.heappop(waiting[link])
            free[link] = now + unit
            actions.append((max(since, now - lead), len(actions), block, send))
            heapq.heappush(events, (now + unit, 0, link))
            _, _, ff, gg = send
            heapq.heappush(events, (now + unit + latency, 1, (block[0], ff, gg, block[3])))

    def arrive(now, block):
        nonlocal count
        half, f, g, u = block
        for send in x_forwards(f, g, u):
            link = ((send[0] + half) % 2, send[1])
            count += 1
            heapq.heappush(
                waiting[link], (-left_over(send[2], send[3], u), count, now, block, send)
            )
        for link in free:
            feed(link, now)

    for half in range(2):
        for u in range(2):
            arrive(0.0, (half, 0, 0, u))
    while events:
        now, kind, what = heapq.heappop(events)
        if kind:
            actions.append((now, -1, what, None))
            arrive(now, what)
        else:
            feed(what, now)
    return [action[2:] for action in sorted(actions, key=lambda entry: entry[:2])]


def body(
    xin_hbm,
    gain_hbm,
    a_hbm,
    b_hbm,
    q_hbm,
    k_hbm,
    v_hbm,
    gate_hbm,
    point_hbm,
    gla_hbm,
    low_hbm,
    dw_hbm,
    bias_hbm,
    extra_hbm,
    kernel_hbm,
    cgain_hbm,
    hgain_hbm,
    out,
    gain_in,
    tiles_in,
    narrow_in,
    low_in,
    dw_in,
    bias_in,
    exsrc,
    taps_in,
    cgain_in,
    hgain_in,
    wsrc,
    owsrc,
    dwt,
    bias,
    taps,
    in_sem,
    xg,
    w,
    ow,
    owz,
    acc_own,
    acc_send,
    acc_recv,
    mats,
    xors,
    scores,
    ext,
    exb,
    stats,
    tot_me,
    tots,
    st_me,
    sts,
    act_me,
    acts,
    po_send,
    po_recv,
    x_send,
    xd_send,
    xd_recv,
    own_send,
    ring_recv,
    wy_send,
    wy_recv,
    wz_send,
    wd_send,
    wd_recv,
    ox_recv,
    oz_send,
    oz_recv,
    od_send,
    od_recv,
    oy_send,
    oy_recv,
    ex_send,
    ex_recv,
    d2d_send,
    d2d_recv,
    halo_send,
    halo_recv,
    stat_send,
    stat_recv,
    tot_send,
    tot_recv,
    st_send,
    st_recv,
    act_send,
    act_recv,
    act2_send,
    act2_recv,
):
    scope = []

    def mark(name):
        if scope:
            scope.pop().__exit__(None, None, None)
        if name:
            scope.append(jax.named_scope(name))
            scope[0].__enter__()

    z = lax.axis_index("sp")
    y = lax.axis_index("fs")
    t = lax.axis_index("tp")
    x = lax.div(t, 2)
    c = t - 2 * x
    y_half = lax.div(y, 2)
    y_low = y - 2 * y_half
    z_class = lax.rem(lax.div(z, 2), 2)
    partner = (z, y, 2 * x + 1 - c)

    def at(xx, yy, zz, cc):
        return (zz, yy, 2 * xx + cc)

    mark("greet")
    barrier = pltpu.get_barrier_semaphore()

    def greet(zz, yy, tt):
        pl.semaphore_signal(barrier, inc=1, device_id=(zz, yy, tt), device_id_type=MESH)

    for step in (1, NZ - 1):
        greet(lax.rem(z + step, NZ), y, t)
    for step in range(1, 8):
        greet(z, y, lax.rem(t + step, 8))
    for step in range(1, 4):
        for cc in range(2):
            greet(z, lax.rem(y + step, 4), 2 * x + cc)

    group_pair = 2 * x + y_half

    def tile_of(index):
        return pl.ds(pl.multiple_of(index * 128, 128), 128)

    def feature_cols(xx, cc):
        return pl.ds(pl.multiple_of((2 * xx + cc) * 512, 512), 512)

    fetches = [
        pltpu.make_async_copy(source, target, in_sem.at[k])
        for k, (source, target) in enumerate(
            (
                (a_hbm, tiles_in.at[0]),
                (b_hbm, tiles_in.at[1]),
                (v_hbm, tiles_in.at[2]),
                (gate_hbm, tiles_in.at[3]),
                (point_hbm, tiles_in.at[4]),
                (gla_hbm, tiles_in.at[5]),
                (q_hbm, narrow_in.at[0]),
                (k_hbm, narrow_in.at[1]),
                (gain_hbm, gain_in),
                (low_hbm.at[:, tile_of(2 * z + y_half)], low_in),
                (xin_hbm, xg.at[rows(y * TOK, TOK), feature_cols(x, c)]),
                (extra_hbm, exsrc),
                (dw_hbm.at[:, tile_of(x)], dw_in),
                (bias_hbm, bias_in),
                (kernel_hbm.at[:, tile_of(group_pair)], taps_in),
                (cgain_hbm, cgain_in),
                (hgain_hbm, hgain_in),
            )
        )
    ]
    for fetch in fetches:
        fetch.start()

    mark("pack")
    low64 = iota((64, 128), 1) < 64
    lane64 = iota((64, 128), 1)
    y_even = y_low == 0

    def column(row_vector):
        return jnp.broadcast_to(row_vector, (128, 128)).T

    for fetch in fetches[:10]:
        fetch.wait()
    gain_all = column(gain_in[pl.ds(2 * z + y_half, 1), :])
    gain = jnp.where(y_even, gain_all[:64], gain_all[64:])

    def pair(k, scale):
        first = tiles_in[k].astype(F32) * scale
        second = tiles_in[k + 1].astype(F32) * scale
        return (
            jnp.where(low64, first, roll64(second)).astype(BF16),
            jnp.where(low64, roll64(first), second).astype(BF16),
        )

    for k in range(2):
        both = pair(2 * k, gain)
        for j in range(2):
            wsrc[j, :, 128 * k : 128 * k + 128] = both[j]
    both = pair(4, 1.0)
    for j in range(2):
        owsrc[:, 128 * j : 128 * j + 128] = both[j]
    narrow = jnp.concatenate([narrow_in[0], narrow_in[1]], axis=1).astype(F32)
    low_rows = low_in[...].astype(F32)
    low_rows = jnp.concatenate([low_rows, low_rows], axis=0).T
    low_rows = jnp.where(y_even, low_rows[:64], low_rows[64:])
    back32, back64 = pltpu.roll(narrow, 96, 1), roll64(narrow)
    mixed0 = jnp.where(low64, jnp.where(lane64 < 32, narrow, back32), low_rows)
    mixed1 = jnp.where(low64, jnp.where(lane64 < 32, back32, back64), low_rows)
    wsrc[0, :, 256:] = (mixed0 * gain).astype(BF16)
    wsrc[1, :, 256:] = (mixed1 * gain).astype(BF16)
    for fetch in fetches[10:12]:
        fetch.wait()
    mark("barrier_wait")
    pl.semaphore_wait(barrier, 2 + 7 + 6)

    finish = []

    def start(copy, cond=None):
        if cond is None:
            copy.start()
        else:
            pl.when(cond)(copy.start)
        finish.append((copy, cond))

    mark("first_sends")
    def w_at(zz, k):
        kind = lax.rem(lax.div(zz, 2), 2)
        begin = kind * 2048 + lax.div(zz, 4) * 512 + lax.rem(zz, 2) * 256 + k * 64
        return w.at[rows(begin, 64), :]

    for j in range(2):
        mine = jnp.logical_and(2 * c + j == y, c == 1)
        start(
            remote(
                wsrc.at[j], w_at(z, y), wy_send.at[j], wy_recv.at[y], at(x, 2 * c + j, z, 1)
            ),
            jnp.logical_not(mine),
        )

        @pl.when(mine)
        def _():
            w_at(z, y)[...] = wsrc[j]

    x_up, x_down = wrap(x + 1, 4), wrap(x - 1, 4)
    y_up, y_down = wrap(y + 1, 4), wrap(y - 1, 4)
    z_up, z_down = wrap(z + 1, NZ), wrap(z - 1, NZ)
    along_x = (at(x_up, y, z, 0), at(x_down, y, z, 0))
    along_y = (at(x, y_up, z, 0), at(x, y_down, z, 0))

    def x_rows(yy, half, u):
        begin = yy * TOK + 2 * UNIT[0] * half + UNIT[half] * u
        return pl.ds(pl.multiple_of(begin, 16), UNIT[half])

    def x_place(half, f, g, u):
        df, dg = OFFSETS[f], OFFSETS[g]
        xx, yy = (x + df, y + dg) if half == 0 else (x + dg, y + df)
        xx, yy = wrap(xx, 4), wrap(yy, 4)
        cols = pl.ds(pl.multiple_of(xx * 1024, 1024), 1024)
        if f == 0 and g == 0:
            cols = feature_cols(xx, c)
        return (
            xg.at[x_rows(yy, half, u), cols],
            xg.at[x_rows(yy, half, u), feature_cols(xx, 1)],
        )

    def x_send_on(block, send):
        place, _ = x_place(*block)
        half, u = block[0], block[3]
        which, way, ff, gg = send
        axis = along_x if (which + half) % 2 == 0 else along_y
        slot = 32 * half + 8 * ff + 2 * gg + u
        remote(place, place, x_send, ring_recv.at[slot], axis[way]).start()

    def x_wait(block):
        place, others = x_place(*block)
        half, f, g, u = block
        slot = 32 * half + 8 * f + 2 * g + u
        remote(place, place, x_send, ring_recv.at[slot], partner).wait_recv()
        remote(others, others, xd_send, xd_recv, partner).start()

    x_actions = x_order()
    x_first = [action for action in x_actions if action[0][1:3] == (0, 0)]
    for block, send in x_first[:8]:
        x_send_on(block, send)

    @pl.when(c == 0)
    def _():
        remote(owsrc, owz.at[z, 0], own_send, ox_recv, partner).start()

    @pl.when(c == 1)
    def _():
        owz[z, 1] = owsrc[...]

    for j in range(2):
        mine = jnp.logical_and(2 * c + j == y, y_half == c)
        start(
            remote(
                exsrc.at[j],
                exb.at[y_low],
                ex_send.at[j],
                ex_recv.at[y_low],
                at(x, 2 * c + j, z, y_half),
            ),
            jnp.logical_not(mine),
        )

        @pl.when(mine)
        def _():
            exb[y_low] = exsrc[j]

    up, down = (z_up, y, t), (z_down, y, t)

    ways = (up, down)

    def z_last(way, k):
        return 8 if (k in (0, 1, 4)) == (way == 0) else 7


    def w_on(way, d, k, origin):
        here = w_at(origin, k)
        if d < z_last(way, k):
            remote(here, here, wz_send, ring_recv.at[4 * origin + k], ways[way]).start()
        if d == 0 and way == 0:
            return

        @pl.when(lax.rem(lax.div(origin, 2), 2) == 0)
        def _():
            remote(here, here, wd_send, wd_recv, partner).start()

    def w_start(k):
        here = w_at(z, k)

        @pl.when(jnp.logical_not(jnp.logical_and(y == k, y_half == 1)))
        def _():
            remote(here, here, wz_send, wy_recv.at[k], up).wait_recv()

        w_on(0, 0, k, z)
        w_on(1, 0, k, z)

    def w_event(way, d, k):
        origin = wrap(z - d if way == 0 else z + d, NZ)
        here = w_at(origin, k)
        remote(here, here, wz_send, ring_recv.at[4 * origin + k], up).wait_recv()
        w_on(way, d, k, origin)

    def ow_cols(xx):
        return pl.ds(pl.multiple_of(xx * 256, 256), 256)

    def ow_at(zz):
        k = lax.rem(zz, 4)
        half = lax.div(k, 2)
        return ow.at[half, rows(y * 128 + (k - 2 * half) * 64, 64), ow_cols(x)]

    def ow_on(way, d, cc, origin):
        here = owz.at[origin, cc]
        if d < z_last(way, 4 + cc):
            remote(here, here, oz_send, oz_recv.at[origin, cc], ways[way]).start()

    def ow_give(n, carry):
        turn = lax.div(n, 4)
        ahead = jnp.where(turn == 2, 3, jnp.where(turn == 3, 2, turn))
        column = lax.rem(x + ahead, 4)
        origin = 4 * column + lax.rem(n, 4)
        behind = lax.rem(4 - ahead, 4)
        place = ow_at(origin)

        def give(cc):
            remote(
                owz.at[origin, cc], place, od_send, od_recv.at[behind], at(column, y, z, cc)
            ).start()

        give(0)
        pl.when(column != x)(functools.partial(give, 1))

        @pl.when(column == x)
        def _():
            place[...] = owz[origin, 1]

        return carry

    def ow_start():
        for cc in (1, 0):
            if cc == 0:
                here = owz.at[z, 0]
                remote(here, here, oz_send, ox_recv, partner).wait_recv()
            ow_on(0, 0, cc, z)
            ow_on(1, 0, cc, z)

    def ow_event(way, d, k):
        origin = wrap(z - d if way == 0 else z + d, NZ)
        here = owz.at[origin, k - 4]
        remote(here, here, oz_send, oz_recv.at[origin, k - 4], up).wait_recv()
        ow_on(way, d, k - 4, origin)

    mark("params")
    for fetch in fetches[12:]:
        fetch.wait()
    dw_all = dw_in[...].astype(F32)
    dw_all = jnp.concatenate([dw_all, dw_all], axis=0).T
    dwt[...] = dw_all.astype(BF16)
    bias[...] = column(bias_in[pl.ds(x, 1), :])
    low31 = iota((31, 128), 1) < 64
    tap_rows = taps_in[...]
    tap_back = roll64(tap_rows)
    taps[:31, :] = jnp.where(low31 == y_even, tap_rows, tap_back)
    cgain_row = cgain_in[pl.ds(group_pair, 1), :]
    cgain = jnp.where(low31[:1] == y_even, cgain_row, roll64(cgain_row))
    hgain = jnp.concatenate([hgain_in[...], hgain_in[...]], axis=1)

    mark("constants")
    lane = iota((TOK, TOK), 1)
    row = iota((TOK, TOK), 0)
    xors[...] = jnp.bitwise_xor(row, lane)
    one = jnp.ones((TOK, TOK), F32)
    nil = jnp.zeros((TOK, TOK), F32)

    def level_matrix(level, carry):
        half = lax.shift_left(jnp.int32(1), level)
        base = lane - jnp.bitwise_and(lane, 2 * half - 1)
        middle = base + half - 1
        low = jnp.minimum(lane, middle)
        high = jnp.maximum(lane, middle)
        mats[level] = jnp.where(
            jnp.logical_and(row > low, row <= high), one, nil
        ).astype(BF16)
        return carry

    lax.fori_loop(0, 8, level_matrix, 0)
    mats[8] = jnp.where(row <= lane, one, nil).astype(BF16)
    mats[9] = jnp.where(row > lane, one, nil).astype(BF16)

    z_agenda = []
    for way in range(2):
        for d in range(1, 9):
            for k in range(6):
                if d > z_last(way, k):
                    continue
                call = ow_event if k >= 4 else w_event
                z_agenda.append((W_HOP * d + W_PART * k, call, (way, d, k)))
    z_agenda.sort(key=lambda entry: entry[0])
    mark("gather")

    @pl.when(c == 0)
    def _():
        for n, (block, send) in enumerate(x_actions):
            if n % 30 == 0:
                mark(f"x{n}")
            if send is None:
                x_wait(block)
            elif (block, send) not in x_first[:8]:
                x_send_on(block, send)
        mark("w_arrive")
        everything = w.at[pl.ds(0, 2048), :]
        remote(everything, everything, wd_send, wd_recv, partner).wait_recv()
        mark(None)

    @pl.when(c == 1)
    def _():
        for block, send in x_first[8:]:
            x_send_on(block, send)
        for k in range(4):
            w_start(k)
        ow_start()
        for n, (_, call, event) in enumerate(z_agenda):
            if n % 24 == 0:
                mark(f"z{n}")
            call(*event)
        lax.fori_loop(0, 16, ow_give, 0)
        mark("x_arrive")
        everything = xg.at[pl.ds(0, 480), :]
        remote(everything, everything, xd_send, xd_recv, partner).wait_recv()
        mark(None)

    y_next = (at(x, y_up, z, c), at(x, y_down, z, c))
    y_from = (y_down, y_up)
    y_far = wrap(y + 2, 4)

    def oy_at(yy, ahead):
        return ow.at[:, rows(yy * 128, 128), ow_cols(lax.rem(x + ahead, 4))]

    def oy_own(way, ahead):
        here = oy_at(y, ahead)
        remote(here, here, oy_send, oy_recv.at[way, ahead], y_next[way]).start()

    def oy_wait(way, ahead, yy):
        here = oy_at(yy, ahead)
        remote(here, here, oy_send, oy_recv.at[way, ahead], partner).wait_recv()

    def oy_pass(way, ahead):
        oy_wait(way, ahead, y_from[way])
        here = oy_at(y_from[way], ahead)
        remote(here, here, oy_send, oy_recv.at[2, ahead], y_next[way]).start()

    mark("project")
    def swap_part(n):
        part = pl.ds(128, 384) if n == 0 else pl.ds(0, 128)
        return remote(
            acc_send.at[:, part], acc_recv.at[:, part], d2d_send.at[n], d2d_recv.at[n], partner
        )

    def project(half, target, n):
        begin, size = (128, 256) if n == 0 else (0, 128)
        for s in range(2):
            at_rows = pl.ds(s * TOK, TOK)
            blocks = [
                xg[rows((2 * half + s) * TOK, TOK), feature_cols(k, c)] for k in range(4)
            ]
            total = jnp.zeros((TOK, size), F32)
            for k in range(4):
                total = total + jnp.dot(
                    blocks[k],
                    w[rows(c * 2048 + 512 * k, 512), begin : begin + size],
                    preferred_element_type=F32,
                )
            target[at_rows, begin : begin + size] = total.astype(target.dtype)
            if n:
                continue
            squares = jnp.zeros((TOK, 128), F32)
            for k in range(16):
                piece = blocks[k // 4][:, 128 * (k % 4) : 128 * (k % 4) + 128].astype(F32)
                squares = squares + piece * piece
            target[at_rows, 384:] = squares.astype(target.dtype)

    def ow_wait(ahead):
        unit = ow.at[0, pl.ds(0, 64), :]
        copy = remote(unit, unit, od_send, od_recv.at[ahead], partner)
        if ahead:
            copy.wait_recv()
        else:
            pl.when(c == 0)(copy.wait_recv)

    project(1 - c, acc_send, 0)
    start(swap_part(0))
    ow_wait(0)
    oy_own(0, 0)
    oy_own(1, 0)
    mark("project2")
    project(c, acc_own, 0)
    mark("project3")
    project(1 - c, acc_send, 1)
    start(swap_part(1))
    mark("swap_wait")
    swap_part(0).wait_recv()

    low_lanes = iota((TOK, 128), 1) < 64

    def scaled(s):
        at_rows = pl.ds(s * TOK, TOK)
        both = acc_own[at_rows, 128:] + acc_recv[at_rows, 128:].astype(F32)
        mean = jnp.sum(both[:, 256:], axis=1, keepdims=True) * (1.0 / 4096.0)
        factor = lax.rsqrt(mean + 1e-06)
        return factor, (both[:, :256] * factor).astype(BF16).astype(F32)

    (factor0, p0), (factor1, p1) = scaled(0), scaled(1)

    mark("gating")
    project(c, acc_own, 1)
    swap_part(1).wait_recv()
    first, second = (
        ((acc_own[part, :128] + acc_recv[part, :128].astype(F32)) * factor).astype(BF16).astype(F32)
        for part, factor in ((pl.ds(0, TOK), factor0), (pl.ds(TOK, TOK), factor1))
    )
    left = jnp.where(low_lanes, first, roll64(second))
    right = jnp.where(low_lanes, roll64(first), second)
    ext[32:, :] = (left * sigmoid(right)).astype(BF16).astype(F32)
    start(
        remote(
            ext.at[pl.ds(TOK, 32), :], ext.at[pl.ds(0, 32), :], halo_send, halo_recv, up
        ),
        z < NZ - 1,
    )
    mark("decay")
    v0, v1 = p0[:, :128], p1[:, :128]
    gates = jnp.where(low_lanes, roll64(v0), v1)
    zero = jnp.zeros((TOK, 128), F32)
    v0 = jnp.where(low_lanes, v0, zero).astype(BF16)
    v1 = jnp.where(low_lanes, zero, roll64(v1)).astype(BF16)
    qt0, qt1 = p0[:, 128:].T, p1[:, 128:].T
    queries = jnp.concatenate([qt0[:32], qt1[:32]], axis=0) * (32.0 ** (-0.5))
    keys = jnp.concatenate([qt0[32:64], qt1[32:64]], axis=0)
    for s in range(2):
        local = jnp.logical_and(y_half == c, y_low == s)

        @pl.when(jnp.logical_not(local))
        def _():
            remote(exb.at[s], exb.at[s], ex_send.at[s], ex_recv.at[s], up).wait_recv()

    decays = []
    for s, qt in enumerate((qt0, qt1)):
        pre = (
            jnp.dot(
                dwt[rows(32 * y, 32), :][:, :64],
                qt[64:].astype(BF16),
                preferred_element_type=F32,
            )
            + bias[rows(32 * y, 32), :][:, :1]
        )
        log_sig = jnp.minimum(pre, 0.0) - jnp.log1p(jnp.exp(-jnp.abs(pre)))
        decays.append(log_sig * (1.0 / 16.0) + exb[s])
    decay = jnp.concatenate(decays, axis=0)
    parts = jnp.concatenate(thirds(decay), axis=0)

    def decay_sums(which):
        sums = jnp.dot(parts, mats[which], preferred_element_type=F32)
        return jnp.exp(sums[:64] + sums[64:128] + sums[128:])

    tail_keys = (keys * decay_sums(9)).astype(BF16)
    st_me[...] = (
        jnp.dot(tail_keys[:32], v0, preferred_element_type=F32)
        + jnp.dot(tail_keys[32:], v1, preferred_element_type=F32)
    ).astype(BF16)
    wide = jnp.concatenate([decay, jnp.zeros((64, TOK), F32)], axis=0)
    tot_me[...] = lax.dot_general(
        jnp.ones((8, TOK), F32), wide, NT, precision=HIGHEST, preferred_element_type=F32
    )[:1]

    def tell(n, carry):
        half = lax.div(n + 1, 2)
        k = jnp.where(lax.rem(n, 2) == 0, 8 - half, 8 + half)
        there = (lax.rem(z + k, NZ), y, t)
        remote(tot_me, tots.at[z], tot_send, tot_recv, there).start()
        remote(st_me, sts.at[z], st_send, st_recv, there).start()
        return carry

    lax.fori_loop(0, NZ - 1, tell, 0)

    ow_wait(1)
    oy_own(0, 1)
    oy_own(1, 1)
    mark("halo_wait")
    @pl.when(z == 0)
    def _():
        ext[:32, :] = jnp.zeros((32, 128), F32)

    @pl.when(z > 0)
    def _():
        halo = ext.at[pl.ds(0, 32), :]
        remote(halo, halo, halo_send, halo_recv, up).wait_recv()

    mark("conv")
    conv = jnp.zeros((TOK, 128), F32)
    for tap in range(31):
        conv = conv + taps[tap : tap + 1, :] * ext[2 + tap : 2 + tap + TOK, :]
    lane8, row8 = iota((8, 128), 1), iota((8, 128), 0)
    seq_of = lax.div(lane8, 64)
    pick_sum = jnp.where(row8 == seq_of, 1.0, 0.0).astype(BF16)
    pick_square = jnp.where(row8 == seq_of + 2, 1.0, 0.0).astype(BF16)
    me = 4 * x + y
    stats[me] = lax.dot_general(
        jnp.concatenate([pick_sum] * 3 + [pick_square] * 3, axis=1),
        jnp.concatenate([*thirds(conv), *thirds(conv * conv)], axis=1),
        NT,
        preferred_element_type=F32,
    )

    def stat_copy(k):
        other = lax.rem(me + k, 16)
        xx = lax.div(other, 4)
        return remote(
            stats.at[me],
            stats.at[me],
            stat_send,
            stat_recv,
            at(xx, other - 4 * xx, z, c),
        )

    def send_stat(k, carry):
        stat_copy(k).start()
        return carry

    lax.fori_loop(1, 16, send_stat, 0)

    ow_wait(3)
    oy_own(0, 3)
    oy_own(1, 3)

    mark("attention")
    queries_low, keys_low = queries.astype(BF16), keys.astype(BF16)
    for s in range(2):
        own = lax.dot_general(
            queries_low[32 * s : 32 * s + 32],
            keys_low[32 * s : 32 * s + 32],
            TN,
            preferred_element_type=F32,
        )
        scores[s] = jnp.where(xors[...] == 0, own, 0.0)
    lane_of = iota((64, TOK), 1)

    def level_scores(level, carry):
        factor = decay_sums(level)
        upper = jnp.bitwise_and(lax.shift_right_logical(lane_of, level), 1) == 1
        q_level = jnp.where(upper, queries * factor, 0.0).astype(BF16)
        k_level = jnp.where(upper, 0.0, keys * factor).astype(BF16)
        same = lax.shift_right_logical(xors[...], level + 1) == 0
        for s in range(2):
            pair = lax.dot_general(
                q_level[32 * s : 32 * s + 32],
                k_level[32 * s : 32 * s + 32],
                TN,
                preferred_element_type=F32,
            )
            scores[s] = scores[s] + jnp.where(same, pair, 0.0)
        return carry

    lax.fori_loop(0, 4, level_scores, 0)

    ow_wait(2)
    oy_own(0, 2)
    oy_own(1, 2)
    mark("attention2")
    lax.fori_loop(4, 8, level_scores, 0)
    heads = jnp.dot(scores[0].astype(BF16), v0, preferred_element_type=F32) + jnp.dot(
        scores[1].astype(BF16), v1, preferred_element_type=F32
    )
    q_start = (queries * decay_sums(8)).astype(BF16)

    mark("stat_wait")
    others = stats.at[pl.ds(0, 15)]
    remote(others, others, stat_send, stat_recv, up).wait_recv()
    mark("norm")
    total = stats[0]
    for k in range(1, 16):
        total = total + stats[k]
    picks = jnp.concatenate([pick_sum, pick_square], axis=1)
    moments = lax.dot_general(
        jnp.concatenate(thirds(total), axis=0),
        jnp.concatenate([picks] * 3, axis=0),
        TN,
        preferred_element_type=F32,
    ) * (1.0 / 1024.0)
    average, spread = moments[:, :128], moments[:, 128:]
    variance = jnp.maximum(spread - average * average, 0.0)
    normed = (conv - average) * lax.rsqrt(variance + 1e-05) * cgain
    conv_act = normed * sigmoid(normed)

    mark("state_wait")
    others = tots.at[pl.ds(0, NZ - 1)]
    remote(others, others, tot_send, tot_recv, up).wait_recv()
    others = sts.at[pl.ds(0, NZ - 1)]
    remote(others, others, st_send, st_recv, up).wait_recv()
    mark("heads")
    row16 = iota((NZ, 128), 0)
    known = jnp.where(row16 < z, tots[:, 0, :], 0.0)
    from_row, to_row = iota((NZ, NZ), 0), iota((NZ, NZ), 1)
    between = jnp.where(
        jnp.logical_and(to_row > from_row, to_row < z), 1.0, 0.0
    ).astype(F32)
    exponent = jnp.dot(between, known, precision=HIGHEST, preferred_element_type=F32)
    reach = jnp.where(row16 < z, jnp.exp(exponent), 0.0)
    reach = jnp.concatenate([reach, jnp.zeros((128 - NZ, 128), F32)], axis=0).T
    low32 = iota((32, 128), 1) < 64
    entering = jnp.zeros((32, 128), F32)
    for k in range(NZ - 1):
        factor = jnp.where(low32, reach[:32, k : k + 1], reach[32:64, k : k + 1])
        state = jnp.where(z > k, sts[k].astype(F32), 0.0)
        entering = entering + factor * state
    heads = (
        heads
        + lax.dot_general(
            q_start[:32],
            jnp.where(low32, entering, 0.0).astype(BF16),
            TN,
            preferred_element_type=F32,
        )
        + lax.dot_general(
            q_start[32:],
            jnp.where(low32, 0.0, entering).astype(BF16),
            TN,
            preferred_element_type=F32,
        )
    )
    same_head = lax.div(iota((128, 128), 0), 64) == lax.div(iota((128, 128), 1), 64)
    same_head = jnp.where(same_head, 1.0, 0.0).astype(BF16)
    mean_square = jnp.dot(
        jnp.concatenate(thirds(heads * heads), axis=1),
        jnp.concatenate([same_head] * 3, axis=0),
        preferred_element_type=F32,
    ) * (1.0 / 64.0)
    gla_act = (
        heads * lax.rsqrt(mean_square + 1e-06) * hgain * (gates * sigmoid(gates))
    )

    mark("act_send")
    act_me[0] = jnp.where(low_lanes, conv_act, roll64(gla_act)).astype(BF16)
    act_me[1] = jnp.where(low_lanes, roll64(conv_act), gla_act).astype(BF16)
    def act_cols(j):
        return pl.ds(pl.multiple_of(x * 256 + j * 128, 128), 128)

    for s in range(2):
        mine = (2 * c + s == y) & (y_half == c)
        copy = remote(
            act_me.at[s],
            acts.at[:, act_cols(y_low)],
            act_send,
            act_recv.at[y_low],
            at(x, 2 * c + s, z, y_half),
        )
        pl.when(jnp.logical_not(mine))(copy.start)

        @pl.when(mine)
        def _():
            acts[:, act_cols(y_low)] = act_me[s]

    mark("act_pass")
    def act_on(source, j):
        block = acts.at[:, act_cols(j)]
        for step in (2, 1, 3):
            there = at(lax.rem(x + step, 4), y, z, c)
            remote(source, block, act2_send, act2_recv, there).start()

    def act_arrived(j):
        block = acts.at[:, act_cols(j)]
        remote(block, block, act_send, act_recv.at[j], partner).wait_recv()
        act_on(block, j)

    pl.when(y_half == c)(lambda: act_on(act_me.at[y_low], y_low))
    oy_pass(0, 0)
    oy_pass(1, 3)
    oy_pass(0, 1)
    oy_pass(1, 2)
    pl.when(y_half != c)(lambda: act_arrived(y_low))
    act_arrived(1 - y_low)

    mark("oy_rest")
    for ahead in (3, 2):
        oy_wait(0, ahead, y_down)
    for ahead in (0, 1):
        oy_wait(1, ahead, y_up)
    for ahead in (0, 3, 1, 2):
        oy_wait(2, ahead, y_far)
    mark("act_wait")
    others = acts.at[:, pl.ds(0, 768)]
    remote(others, others, act2_send, act2_recv, partner).wait_recv()
    mark("output")
    def output(half):
        whole = lax.dot_general(acts[...], ow[half], NT, preferred_element_type=F32)
        parts = [whole[:, 128 * yy : 128 * yy + 128] for yy in range(4)]
        tiles = []
        for kk in range(2):
            for even, odd in ((parts[0], parts[1]), (parts[2], parts[3])):
                if kk == 0:
                    tiles.append(jnp.where(low_lanes, even, roll64(odd)))
                else:
                    tiles.append(jnp.where(low_lanes, roll64(even), odd))
        return jnp.concatenate(tiles, axis=1)

    po_send[...] = output(1 - c).astype(BF16)
    trade = remote(po_send, po_recv, d2d_send.at[2], d2d_recv.at[2], partner)
    start(trade)
    residual = xg[rows(y * TOK, TOK), feature_cols(x, c)]
    result = residual.astype(F32) + output(c)
    mark("trade_wait")
    trade.wait_recv()
    out[...] = (result + po_recv[...].astype(F32)).astype(BF16)

    mark("drain")
    for copy, cond in finish:
        if cond is None:
            copy.wait_send()
        else:
            pl.when(cond)(copy.wait_send)

    def left(piece, semaphore, cond=None):
        copy = remote(piece, piece, semaphore, stat_recv, partner)
        if cond is None:
            copy.wait_send()
        else:
            pl.when(cond)(copy.wait_send)

    left(stats.at[pl.ds(0, 15)], stat_send)
    left(tots.at[pl.ds(0, NZ - 1)], tot_send)
    left(sts.at[pl.ds(0, NZ - 1)], st_send)
    left(xg.at[pl.ds(0, 192), :], oy_send)
    left(acts.at[:, pl.ds(0, 128)], act_send, y_half == c)
    left(acts.at[:, pl.ds(0, 256)], act_send, y_half != c)
    left(acts.at[:, pl.ds(0, 768)], act2_send)
    left(xg.at[pl.ds(0, 832), :], x_send, c == 0)
    left(xg.at[pl.ds(0, 128), :], x_send, c == 1)
    left(xg.at[pl.ds(0, 480), :], xd_send, c == 0)
    left(owsrc, own_send, c == 0)
    left(w.at[pl.ds(0, 3840), :], wz_send, c == 1)
    left(w.at[pl.ds(0, 2048), :], wd_send, c == 1)
    left(ow.at[0, pl.ds(0, 448), :], od_send, c == 1)
    left(owz.at[pl.ds(0, 15)], oz_send, c == 1)
    mark(None)


def shards(
    inputs,
    norm_gain,
    conv_in_a,
    conv_in_b,
    query_w,
    key_w,
    value_w,
    out_gate_w,
    pointwise_w,
    gla_out_w,
    forget_first_factor,
    decay_w,
    decay_bias,
    decay_extra,
    conv_kernel,
    conv_gain,
    head_gain,
):
    dma = pltpu.SemaphoreType.DMA
    vmem = pltpu.VMEM
    mixed = pl.pallas_call(
        body,
        out_shape=jax.ShapeDtypeStruct((TOK, 512), BF16),
        in_specs=[pl.BlockSpec(memory_space=pltpu.HBM)] * 17,
        out_specs=pl.BlockSpec(memory_space=vmem),
        scratch_shapes=[
            vmem((32, 128), F32),
            vmem((6, 64, 128), BF16),
            vmem((2, 64, 64), BF16),
            vmem((64, 128), BF16),
            vmem((64, 128), BF16),
            vmem((4, 128), F32),
            vmem((2, 32, TOK), F32),
            vmem((31, 128), F32),
            vmem((8, 128), F32),
            vmem((1, 64), F32),
            vmem((2, 64, 384), BF16),
            vmem((64, 256), BF16),
            vmem((128, 128), BF16),
            vmem((128, 128), F32),
            vmem((32, 128), F32),
            dma((17,)),
            vmem((4 * TOK, 4096), BF16),
            vmem((4096, 384), BF16),
            vmem((2, 512, 1024), BF16),
            vmem((NZ, 2, 64, 256), BF16),
            vmem((512, 512), F32),
            vmem((512, 512), BF16),
            vmem((512, 512), BF16),
            vmem((10, TOK, TOK), BF16),
            vmem((TOK, TOK), jnp.int32),
            vmem((2, TOK, TOK), F32),
            vmem((TOK + 32, 128), F32),
            vmem((2, 32, TOK), F32),
            vmem((16, 8, TOK), F32),
            vmem((1, 128), F32),
            vmem((NZ, 1, 128), F32),
            vmem((32, 128), BF16),
            vmem((NZ, 32, 128), BF16),
            vmem((2, TOK, 128), BF16),
            vmem((TOK, 1024), BF16),
            vmem((TOK, 512), BF16),
            vmem((TOK, 512), BF16),
            dma,
            dma,
            dma,
            dma,
            dma((64,)),
            dma((2,)),
            dma((4,)),
            dma,
            dma,
            dma,
            dma,
            dma,
            dma((NZ, 2)),
            dma,
            dma((4,)),
            dma,
            dma((3, 4)),
            dma((2,)),
            dma((2,)),
            dma((3,)),
            dma((3,)),
            dma,
            dma,
            dma,
            dma,
            dma,
            dma,
            dma,
            dma,
            dma,
            dma((2,)),
            dma,
            dma,
        ],
        compiler_params=pltpu.CompilerParams(
            collective_id=0, has_side_effects=True
        ),
        name="mixer",
    )(
        inputs[0],
        norm_gain.reshape(32, 128),
        conv_in_a,
        conv_in_b,
        query_w,
        key_w,
        value_w,
        out_gate_w,
        pointwise_w,
        gla_out_w,
        forget_first_factor.T,
        decay_w,
        decay_bias.reshape(4, 128),
        decay_extra[0].T.reshape(2, 32, TOK),
        conv_kernel,
        conv_gain.reshape(8, 128),
        head_gain.reshape(1, 64),
    )
    return mixed[None]


def solution(mesh):
    weights = P(("sp", "fs"), "tp")
    return jax.shard_map(
        shards,
        mesh=mesh,
        in_specs=(
            P("fs", "sp", "tp"),
            P(),
            weights,
            weights,
            weights,
            weights,
            weights,
            weights,
            weights,
            weights,
            P(),
            P(),
            P(),
            P("fs", "sp", "tp"),
            P(),
            P(),
            P(),
        ),
        out_specs=P("fs", "sp", "tp"),
        check_vma=False,
    )
```
